256 devices in a mesh: sp: 16 (over y, x), tp: 16 (over z, core).
Axes of the slice: x: 4, y: 4, z: 8, core: 2. Of those that a mesh axis runs over, the one named last changes fastest.
Arguments:
- layer_input: bfloat16 [8192, 2048], P(('sp', 'tp')), may hold values from -6 to 6
- receptance: bfloat16 [8192, 2048], P('sp', 'tp'), may hold values from -6 to 6
- keys: bfloat16 [8192, 2048], P('sp', 'tp'), may hold values from -6 to 6
- values: bfloat16 [8192, 2048], P('sp', 'tp'), may hold values from -6 to 6
- erase_preact: bfloat16 [8192, 2048], P('sp', 'tp'), may hold values from -12 to 5
- decay_preact: bfloat16 [8192, 2048], P('sp', 'tp'), may hold values from -40 to 3
- decay_spike: float32 [8192, 32], P('sp', 'tp'), may hold values from -2 to 0
- head_norm_gain: bfloat16 [2048], P('tp'), may hold values from 0.099609375 to 1.8984375
- output_weight: bfloat16 [2048, 2048], P('tp'), may hold values from -0.125 to 0.125
- expert_norm_gain: bfloat16 [2048], replicated, may hold values from 0.099609375 to 1.8984375
- routes: int32 [8192, 2], P(('sp', 'tp')), may hold values from 0 to 31, all different within a row; in each aligned block of 32 rows (0 to 31, 32 to 63, ...) at most 3 rows name the same one
- routing_weight: float32 [8192, 2], P(('sp', 'tp')), may hold values from 0.3 to 1.5
- expert_gate_weight: bfloat16 [32, 2048, 4096], P('sp', None, 'tp'), may hold values from -0.125 to 0.125
- expert_up_weight: bfloat16 [32, 2048, 4096], P('sp', None, 'tp'), may hold values from -0.125 to 0.125
- expert_down_weight: bfloat16 [32, 4096, 2048], P('sp', 'tp'), may hold values from -0.09375 to 0.09375
- shared_gate_weight: bfloat16 [2048, 4096], P(None, 'tp'), may hold values from -0.125 to 0.125
- shared_up_weight: bfloat16 [2048, 4096], P(None, 'tp'), may hold values from -0.125 to 0.125
- shared_down_weight: bfloat16 [4096, 2048], P('tp'), may hold values from -0.09375 to 0.09375
Outputs:
- layer_out: bfloat16 [8192, 2048], P(('sp', 'tp'))
The draws below stay inside these ranges and needn't reach their ends.
Inputs may be any that keep to these rules, and one draw needn't show every extreme that they name: `routes`: in each aligned block of 32 rows no expert is named by more than 3 rows.
All inputs are finite; a program needn't handle non-finite values.
Results may differ from the reference program's by a relative error of at most 0.02.
Values may be sent and summed in bfloat16 or wider, within the bound.
A program may use at most 128 MiB of HBM per device.

```python
import math
import jax
import jax.numpy as jnp
import numpy as np
from jax import lax

D = 2048
HEAD = 64
HEADS = 32
TOK_DEV = 512
TOKENS = 8192
ROWS_DEV = 32
EXPERTS = 32
TOP_K = 2
FFE = 4096
SH = 4096
CAP = 3
N_SP = 16
N_TP = 16


def slow_heads(key):
    slow_count = HEADS // 2
    order = jax.random.permutation(jax.random.fold_in(key, 41), HEADS)
    return order < slow_count


def rough_noise(key, array_shape):
    return 0.8 * jax.random.truncated_normal(key, -3.0, 3.0, array_shape, jnp.float32)


def draw_keys(key, part):
    noise = jax.random.normal(jax.random.fold_in(key, 79), (TOKENS, D), jnp.float32)
    common = jax.random.normal(jax.random.fold_in(key, 73), (1, D), jnp.float32)
    return jnp.clip(common + noise, -6.0, 6.0).astype(jnp.bfloat16)


def draw_decay_preact(key, part):
    slow = slow_heads(key)
    fast_rate = jax.random.uniform(jax.random.fold_in(key, 43), (HEADS,), jnp.float32, 0.01, 0.033)
    head_rate = jnp.where(slow, 0.1 / TOKENS, fast_rate)
    head_base = jnp.repeat(jnp.log(head_rate) + 0.5, HEAD)[None, :]
    stretch = jax.random.uniform(jax.random.fold_in(key, 47), (TOKENS // TOK_DEV, 1), jnp.float32, -0.7, 0.7)
    per_block = jnp.repeat(stretch, TOK_DEV, axis=0)
    noise = rough_noise(jax.random.fold_in(key, 53), (TOKENS, D))
    return (head_base + per_block + noise).astype(jnp.bfloat16)


def draw_erase_preact(key, part):
    slow = slow_heads(key)
    fast_base = jax.random.uniform(jax.random.fold_in(key, 59), (HEADS,), jnp.float32, 2.0, 2.6)
    head_base = jnp.repeat(jnp.where(slow, -7.0, fast_base), HEAD)[None, :]
    noise = rough_noise(jax.random.fold_in(key, 61), (TOKENS, D))
    return jnp.clip(head_base + noise, -12.0, 5.0).astype(jnp.bfloat16)


def draw_decay_spike(key, part):
    where_hit = jax.random.randint(jax.random.fold_in(key, 67), (3,), 0, TOKENS)
    depth = jnp.log(jax.random.uniform(jax.random.fold_in(key, 71), (3, HEADS), jnp.float32, 0.5, 0.8))
    hits = (jnp.arange(TOKENS, dtype=jnp.int32)[:, None] == where_hit[None, :]).astype(jnp.float32)
    return jnp.dot(hits, depth)


def levels(rng, shape, split, low, largest):
    def one(dim, blocks):
        steps = jax.random.uniform(jax.random.fold_in(jax.random.fold_in(rng, 6), dim), (blocks,), jnp.float32, low / len(split), largest / len(split))
        return jnp.repeat(jnp.exp(steps), shape[dim] // blocks).reshape((-1,) + (1,) * (len(shape) - dim - 1))

    factor_of = one(*split[0])
    for cut in split[1:]:
        factor_of = factor_of * one(*cut)
    return factor_of


def routed_block(key, own, number, rows, amount, top, bound, skew):
    sequence = jax.random.permutation(key, amount)
    packed, ordinary = shares(amount, rows * top, bound, skew, True), shares(amount, rows * top, bound, skew, False)
    places = jnp.arange(amount)

    def named(sizes, turn):
        used = int((sizes > 0).sum())
        fixed = max(1, used // 4)
        shifted = fixed + (places - fixed + turn * (used - fixed)) % max(1, amount - fixed)
        return jnp.zeros((amount,), jnp.int32).at[sequence[jnp.where(places < fixed, places, shifted)]].set(jnp.asarray(sizes, jnp.int32))

    sizes = jnp.where(number % 4 == 0, named(packed, number // 4), named(ordinary, number - number // 4 - 1))
    mixed = jax.random.permutation(jax.random.fold_in(own, 3), amount)
    giver, taker = mixed[0:amount // 2 * 2:2], mixed[1:amount // 2 * 2:2]
    margin = jnp.minimum(sizes[giver] - 1, bound - sizes[taker]) // 2
    margin = jnp.where((giver == sequence[0]) | (taker == sequence[0]) | (sizes[taker] == 0), 0, jnp.maximum(margin, 0))
    shifted = jax.random.randint(jax.random.fold_in(own, 4), (amount // 2,), 0, 1 << 20) % (margin + 1)
    sizes = sizes.at[giver].add(-shifted).at[taker].add(shifted)
    members = jnp.searchsorted(jnp.cumsum(sizes), jnp.arange(rows * top), side="right").astype(jnp.int32)
    table = members.reshape(top, rows).T
    table = table[jax.random.permutation(jax.random.fold_in(own, 1), rows)]
    turn = jax.random.randint(jax.random.fold_in(own, 2), (rows, 1), 0, top)
    return jnp.take_along_axis(table, (jnp.arange(top)[None, :] + turn) % top, axis=1)


def shares(number_of, total, bound, skew, full):
    loads = [(1 << 20) // math.isqrt(standing ** skew) + 1 for standing in range(1, number_of + 1)]
    largest = bound if full else min(bound, max(-(-total // number_of), total * loads[0] // sum(loads)))
    least = 1 if total - largest >= number_of - 1 else 0
    given, surplus = [largest] + [least] * (number_of - 1), total - largest - least * (number_of - 1)
    while surplus > 0:
        free = [i for i in range(1, number_of) if given[i] < largest] or [i for i in range(1, number_of) if given[i] < bound]
        pool, remaining = sum([loads[i] for i in free]), surplus
        for i in free:
            extra = min(bound - given[i], max(1, remaining * loads[i] // pool), surplus)
            given[i] = given[i] + extra
            surplus = surplus - extra
    return np.array(given)


def bell_draw(rng, dims, scale, reach, cuts=(), kind=jnp.bfloat16):
    factor_of = levels(rng, dims, cuts, -0.22, 0.18) if cuts else 1.0
    drawn = jax.random.normal(rng, dims, jnp.float32) * scale * factor_of
    return jnp.minimum(jnp.maximum(drawn, -reach), reach).astype(kind)


def setup_inputs(seed: int = 0) -> dict:
    key_list = jax.random.split(jax.random.key(seed), 19)
    layer_input = bell_draw(key_list[0], (TOKENS, D), 1.0, 6.0, ((0, 256),))
    receptance = bell_draw(key_list[1], (TOKENS, D), 1.0, 6.0, ((0, 16), (1, 16)))
    keys = draw_keys(jax.random.fold_in(key_list[18], 71), 0)
    values = bell_draw(key_list[3], (TOKENS, D), 1.0, 6.0, ((0, 16), (1, 16)))
    erase_preact = draw_erase_preact(jax.random.fold_in(key_list[18], 71), 0)
    decay_preact = draw_decay_preact(jax.random.fold_in(key_list[18], 71), 0)
    decay_spike = draw_decay_spike(jax.random.fold_in(key_list[18], 71), 0)
    head_norm_gain = jnp.clip(1.0 + 0.18 * jax.random.normal(key_list[7], (D,), jnp.float32), 0.099609375, 1.8984375).astype(jnp.bfloat16)
    output_weight = bell_draw(key_list[8], (D, D), D ** -0.5, 0.125, ((0, 16),))
    expert_norm_gain = jnp.clip(1.0 + 0.18 * jax.random.normal(key_list[9], (D,), jnp.float32), 0.099609375, 1.8984375).astype(jnp.bfloat16)
    routes_keys = jax.random.split(jax.random.fold_in(key_list[10], 1), TOKENS // ROWS_DEV)
    routes_turns = jax.random.permutation(jax.random.fold_in(key_list[10], 3), TOKENS // ROWS_DEV)
    routes = jax.vmap(lambda own, number: routed_block(jax.random.fold_in(key_list[10], 2), own, number, ROWS_DEV, EXPERTS, TOP_K, CAP, 2))(routes_keys, routes_turns).reshape((TOKENS, TOP_K))
    routing_weight = jnp.clip(0.3 + 1.2 * jax.random.uniform(key_list[11], (TOKENS, TOP_K), jnp.float32) ** levels(key_list[11], (TOKENS, TOP_K), ((0, 256),), -0.2, 0.2), 0.3, 1.5)
    expert_gate_weight = bell_draw(key_list[12], (EXPERTS, D, FFE), D ** -0.5, 0.125, ((0, 16), (2, 16)))
    expert_up_weight = bell_draw(key_list[13], (EXPERTS, D, FFE), D ** -0.5, 0.125, ((0, 16), (2, 16)))
    expert_down_weight = bell_draw(key_list[14], (EXPERTS, FFE, D), FFE ** -0.5, 0.09375, ((0, 16), (1, 16)))
    shared_gate_weight = bell_draw(key_list[15], (D, SH), D ** -0.5, 0.125, ((1, 16),))
    shared_up_weight = bell_draw(key_list[16], (D, SH), D ** -0.5, 0.125, ((1, 16),))
    shared_down_weight = bell_draw(key_list[17], (SH, D), SH ** -0.5, 0.09375, ((0, 16),))
    return dict(layer_input=layer_input, receptance=receptance, keys=keys, values=values, erase_preact=erase_preact, decay_preact=decay_preact, decay_spike=decay_spike, head_norm_gain=head_norm_gain, output_weight=output_weight, expert_norm_gain=expert_norm_gain, routes=routes, routing_weight=routing_weight, expert_gate_weight=expert_gate_weight, expert_up_weight=expert_up_weight, expert_down_weight=expert_down_weight, shared_gate_weight=shared_gate_weight, shared_up_weight=shared_up_weight, shared_down_weight=shared_down_weight)


highest = lax.Precision.HIGHEST
GN_EPS = 0.00064
RMS_EPS = 1e-06

def each_head(array):
    return array.astype(jnp.float32).reshape(array.shape[0], HEADS, HEAD)

def recurrence(decay_factor, unit_keys, beta, key_rows, value_rows, read_rows):

    def advance(state_now, inputs):
        decay_t, unit_t, beta_t, key_t, value_t, read_t = inputs
        removed = jnp.einsum('hij,hj->hi', state_now, unit_t, precision=highest)
        state_now = state_now * decay_t[:, None, :] - removed[:, :, None] * beta_t[:, None, :] + value_t[:, :, None] * key_t[:, None, :]
        return (state_now, jnp.einsum('hij,hj->hi', state_now, read_t, precision=highest))
    start_state = jnp.zeros((HEADS, HEAD, HEAD), jnp.float32)
    _, outputs = lax.scan(advance, start_state, (decay_factor, unit_keys, beta, key_rows, value_rows, read_rows))
    return outputs

def grouped_down(hidden, down, groups):
    group_cols = hidden.shape[1] // groups

    def add_group(running, group_idx):
        first_col = (group_idx * group_cols).astype(jnp.int32)
        hidden_part = lax.dynamic_slice_in_dim(hidden, first_col, group_cols, 1)
        down_part = lax.dynamic_slice_in_dim(down, first_col, group_cols, 0)
        partial_value = jnp.dot(hidden_part, down_part, preferred_element_type=jnp.float32).astype(jnp.bfloat16)
        partial_value = lax.optimization_barrier(partial_value)
        return (running + partial_value.astype(jnp.float32), None)
    running, _ = lax.scan(add_group, jnp.zeros((hidden.shape[0], down.shape[1]), jnp.float32), jnp.arange(groups, dtype=jnp.int32))
    return running

def reference(layer_input, receptance, keys, values, erase_preact, decay_preact, decay_spike, head_norm_gain, output_weight, expert_norm_gain, routes, routing_weight, expert_gate_weight, expert_up_weight, expert_down_weight, shared_gate_weight, shared_up_weight, shared_down_weight):
    key_rows = each_head(keys)
    unit_keys = key_rows * lax.rsqrt(lax.optimization_barrier(jnp.sum(key_rows * key_rows, axis=-1, keepdims=True)) + 1e-06)
    beta = unit_keys * jax.nn.sigmoid(each_head(erase_preact))
    decay_factor = jnp.exp(-jnp.exp(-jax.nn.softplus(-each_head(decay_preact)) - 0.5) + decay_spike.astype(jnp.float32)[:, :, None])
    value_rows = each_head(values)
    read_rows = each_head(receptance)
    forward = recurrence(decay_factor, unit_keys, beta, key_rows, value_rows, read_rows)
    flipped = [array[::-1] for array in (decay_factor, unit_keys, beta, key_rows, value_rows, read_rows)]
    backward = recurrence(*flipped)[::-1]
    mix = forward + backward
    center = lax.optimization_barrier(jnp.mean(mix, axis=-1, keepdims=True))
    spread = lax.optimization_barrier(jnp.mean(jnp.square(mix - center), axis=-1, keepdims=True))
    mixed = ((mix - center) * lax.rsqrt(spread + GN_EPS)).reshape(TOKENS, D) * head_norm_gain.astype(jnp.float32)
    mixed = mixed.astype(jnp.bfloat16)
    residual = layer_input.astype(jnp.float32) + jnp.dot(mixed, output_weight, preferred_element_type=jnp.float32)
    normed = residual * lax.rsqrt(lax.optimization_barrier(jnp.mean(residual * residual, axis=-1, keepdims=True)) + RMS_EPS)
    normed = (normed * expert_norm_gain.astype(jnp.float32)).astype(jnp.bfloat16)
    shared_hidden = (jax.nn.silu(jnp.dot(normed, shared_gate_weight, preferred_element_type=jnp.float32)) * jnp.dot(normed, shared_up_weight, preferred_element_type=jnp.float32)).astype(jnp.bfloat16)
    shared = grouped_down(shared_hidden, shared_down_weight, N_TP)
    entries = routes.reshape(-1).astype(jnp.int32)
    entry_weight = routing_weight.reshape(-1).astype(jnp.float32)
    entry_owner = jnp.arange(TOKENS * TOP_K, dtype=jnp.int32) // TOP_K
    most_rows = N_SP * N_TP * CAP

    def one_expert(running, expert):
        chosen = entries == expert
        position = jnp.cumsum(chosen.astype(jnp.int32)) - 1
        target = jnp.where(chosen, position, most_rows).astype(jnp.int32)
        owners = jnp.full((most_rows,), TOKENS, jnp.int32).at[target].set(entry_owner, mode='drop')
        weights = jnp.zeros((most_rows,), jnp.float32).at[target].set(entry_weight, mode='drop')
        picked = jnp.take(normed, jnp.minimum(owners, TOKENS - 1).astype(jnp.int32), axis=0)
        gate_value = jnp.dot(picked, expert_gate_weight[expert], preferred_element_type=jnp.float32)
        up_value = jnp.dot(picked, expert_up_weight[expert], preferred_element_type=jnp.float32)
        hidden = (jax.nn.silu(gate_value) * up_value).astype(jnp.bfloat16)
        routed = grouped_down(hidden, expert_down_weight[expert], N_TP).astype(jnp.bfloat16)
        routed = lax.optimization_barrier(routed)
        running = running.at[owners].add(weights[:, None] * routed.astype(jnp.float32), mode='drop')
        return (running, None)
    routed_sum, _ = lax.scan(one_expert, jnp.zeros((TOKENS, D), jnp.float32), jnp.arange(EXPERTS, dtype=jnp.int32))
    return (residual + shared + routed_sum).astype(jnp.bfloat16)
```

```python
import functools

import jax
import jax.numpy as jnp
from jax import lax
from jax.experimental import pallas as pl
from jax.experimental.pallas import tpu as pltpu
from jax.sharding import PartitionSpec as P

SP = "sp"
TP = "tp"
BLOCK = 64
LANES = 128
GN_EPS = 0.00064
RMS_EPS = 1e-06
f32 = jnp.float32
bf16 = jnp.bfloat16
VMEM = pl.BlockSpec(memory_space=pltpu.VMEM)
NN = (((1,), (0,)), ((), ()))
NT = (((1,), (1,)), ((), ()))
TN = (((0,), (0,)), ((), ()))


def iota(shape, dim):
    return lax.broadcasted_iota(jnp.int32, shape, dim)


def halves(array):
    high = array.astype(bf16)
    return high, (array - high.astype(f32)).astype(bf16)


def raw_dot(left, right, dims):
    return lax.dot_general(left, right, dims, preferred_element_type=f32)


def both_heads(rows):
    lane = iota(rows.shape, 1)
    zero = jnp.zeros_like(rows)
    return jnp.concatenate(
        [jnp.where(lane < BLOCK, rows, zero), jnp.where(lane < BLOCK, zero, rows)], axis=0
    )


def fine_dot(left, right, dims, spread=False):
    left_high, left_low = halves(left)
    right_high, right_low = halves(right)
    if spread:
        right_high, right_low = both_heads(right_high), both_heads(right_low)
    if dims == TN:
        return raw_dot(
            jnp.concatenate([left_high, left_high, left_low], axis=0),
            jnp.concatenate([right_high, right_low, right_high], axis=0),
            TN,
        )
    count = left.shape[0]
    both = raw_dot(jnp.concatenate([left_high, left_low], axis=0), right_high, dims)
    return both[:count] + both[count:] + raw_dot(left_high, right_low, dims)


def exact_right_dot(left, right, dims):
    left_high, left_low = halves(left)
    count = left.shape[0]
    both = raw_dot(jnp.concatenate([left_high, left_low], axis=0), right, dims)
    return both[:count] + both[count:]


def head_sum(rows):
    ones = (iota((LANES, LANES), 0) // BLOCK == iota((LANES, LANES), 1) // BLOCK).astype(bf16)
    return exact_right_dot(rows, ones, NN)


def block_sums(log_decay):
    high = log_decay.astype(bf16)
    rest = log_decay - high.astype(f32)
    middle = rest.astype(bf16)
    low = (rest - middle.astype(f32)).astype(bf16)
    count = log_decay.shape[0]
    ones = (iota((count, count), 0) >= iota((count, count), 1)).astype(bf16)
    width = log_decay.shape[1]
    sums = raw_dot(ones, jnp.concatenate([high, middle, low], axis=1), NN)
    return sums[:, :width] + sums[:, width : 2 * width] + sums[:, 2 * width :]


def inverse(strict):
    row, lane = iota(strict.shape, 0), iota(strict.shape, 1) % BLOCK

    def within(size):
        return row // size == lane // size

    def product(left, right):
        return fine_dot(left, right, NN, spread=True)

    small = jnp.where(within(8), strict, 0.0)
    start = jnp.where(row == lane, 1.0, 0.0) - small
    square = product(small, small)
    both = product(jnp.concatenate([start, square], axis=0), square)
    result = start + both[:BLOCK]
    result = result + product(result, both[BLOCK:])
    for size in (8, 16, 32):
        edge = jnp.where(within(2 * size) & ~within(size), strict, 0.0)
        result = result - product(product(result, edge), result)
    return result


def one_way(unit, beta, key_rows, value_spread, read, left_unit, left_read, right, edge, lower):
    row, lane = iota((BLOCK, LANES), 0), iota((BLOCK, LANES), 1) % BLOCK
    strict = row > lane if lower else row < lane
    upto = row >= lane if lower else row <= lane
    unit_mid, read_mid = unit * left_unit, read * left_read
    beta_mid, key_mid = beta * right, key_rows * right
    left_high, left_low = halves(jnp.concatenate([unit_mid, read_mid], axis=0))
    beta_parts, key_parts = halves(beta_mid), halves(key_mid)
    right_high, right_low = [
        jnp.concatenate([both_heads(b), both_heads(k)], axis=0)
        for b, k in zip(beta_parts, key_parts)
    ]
    both = raw_dot(jnp.concatenate([left_high, left_low], axis=0), right_high, NT)
    pairs = both[: 2 * BLOCK] + both[2 * BLOCK :] + raw_dot(left_high, right_low, NT)
    erase_beta = jnp.where(strict, pairs[:BLOCK, :LANES], 0.0)
    erase_key = jnp.where(strict, pairs[:BLOCK, LANES:], 0.0)
    read_beta = jnp.where(upto, pairs[BLOCK:, :LANES], 0.0)
    read_key = jnp.where(upto, pairs[BLOCK:, LANES:], 0.0)
    keyed = exact_right_dot(jnp.concatenate([erase_key, read_key], axis=0), value_spread, NN)
    solver = inverse(erase_beta)
    lead = fine_dot(solver, unit_mid * edge, NN, spread=True)
    own = fine_dot(solver, -keyed[:BLOCK], NN, spread=True)
    solved = jnp.concatenate([lead, own], axis=1)
    parts = halves(solved)
    spread_parts = [
        jnp.concatenate([both_heads(p[:, :LANES]), both_heads(p[:, LANES:])], axis=1) for p in parts
    ]
    read_high, read_low = halves(read_beta)
    both = raw_dot(jnp.concatenate([read_high, read_low], axis=0), spread_parts[0], NN)
    applied = both[:BLOCK] + both[BLOCK:] + raw_dot(read_high, spread_parts[1], NN)
    readout = read_mid * edge - applied[:, :LANES]
    local = applied[:, LANES:] + keyed[BLOCK:]
    return solved, beta_mid * edge, key_mid * edge, readout, local


def mixer_kernel(
    read_ref,
    key_ref,
    value_ref,
    erase_ref,
    decay_ref,
    spike_ref,
    local_ref,
    readout_ref,
    prefix_ref,
    start_ref,
    whole_ref,
    move_ref,
    carry_ref,
    *,
    together,
):
    tokens = key_ref.shape[0]
    block_count = tokens // BLOCK
    lane = iota((BLOCK, LANES), 1)
    same_head = iota((LANES, LANES), 0) // BLOCK == iota((LANES, LANES), 1) // BLOCK
    diagonal = iota((LANES, LANES), 0) == iota((LANES, LANES), 1)

    def one_block(block):
        at = pl.ds(pl.multiple_of(block * BLOCK, BLOCK), BLOCK)
        key_rows = key_ref[at, :].astype(f32)
        read = read_ref[at, :].astype(f32)
        value = value_ref[at, :]
        unit = key_rows * lax.rsqrt(head_sum(key_rows * key_rows) + 1e-06)
        beta = unit * jax.nn.sigmoid(erase_ref[at, :].astype(f32))
        decay_in = decay_ref[at, :].astype(f32)
        spike = jnp.where(lane < BLOCK, spike_ref[at, 0:1], spike_ref[at, 1:2])
        log_decay = -jnp.exp(-jax.nn.softplus(-decay_in) - 0.5) + spike
        upto = block_sums(log_decay)
        total = upto[BLOCK - 1 :, :]
        middle = 0.5 * total
        ahead = upto - log_decay
        before, after = jnp.exp(ahead - middle), jnp.exp(upto - middle)
        until, since = jnp.exp(middle - upto), jnp.exp(middle - ahead)
        edge = jnp.exp(middle)
        value_spread = both_heads(value)
        ways = (
            one_way(unit, beta, key_rows, value_spread, read, before, after, until, edge, True),
            one_way(unit, beta, key_rows, value_spread, read, until, since, before, edge, False),
        )
        local_ref[at, :] = ways[0][4] + ways[1][4]
        over = jnp.exp(total)
        for way, (solved, beta_end, key_end, readout, _) in enumerate(ways):
            readout_ref[at, way * LANES : (way + 1) * LANES] = readout
            moved = fine_dot(solved, beta_end, TN)
            key_high, key_low = halves(key_end)
            keyed = raw_dot(
                jnp.concatenate([value, value], axis=0),
                jnp.concatenate([key_high, key_low], axis=0),
                TN,
            )
            move_ref[way, block] = jnp.where(
                same_head, jnp.where(diagonal, over, 0.0) - moved[:LANES], 0.0
            )
            carry = jnp.where(same_head, moved[LANES:] + keyed, 0.0)
            carry_ref[way, block] = carry[:BLOCK] + carry[BLOCK:]

    def step(index, _):
        for k in range(together):
            one_block(index * together + k)
        return 0

    lax.fori_loop(0, block_count // together, step, 0)
    identity = jnp.where(iota((BLOCK, LANES), 0) == iota((BLOCK, LANES), 1) % BLOCK, 1.0, 0.0)
    running = [jnp.concatenate([identity, jnp.zeros_like(identity)], axis=0)] * 2
    for k in range(block_count):
        for way in range(2):
            block = k if way == 0 else block_count - 1 - k
            now = running[way]
            prefix_ref[way, block] = now[:BLOCK]
            start_ref[way, block] = now[BLOCK:]
            after = fine_dot(now, move_ref[way, block], NN)
            running[way] = jnp.concatenate(
                [after[:BLOCK], after[BLOCK:] + carry_ref[way, block]], axis=0
            )
    for way in range(2):
        whole_ref[way] = running[way].astype(bf16)


def mixer_terms(read, keys, values, erase, decay, spike):
    tokens = keys.shape[0]
    block_count = tokens // BLOCK
    shape = jax.ShapeDtypeStruct
    return pl.pallas_call(
        functools.partial(mixer_kernel, together=2),
        name="mixer_terms",
        out_shape=(
            shape((tokens, LANES), f32),
            shape((tokens, 2 * LANES), f32),
            shape((2, block_count, BLOCK, LANES), f32),
            shape((2, block_count, BLOCK, LANES), f32),
            shape((2, 2 * BLOCK, LANES), bf16),
        ),
        in_specs=[VMEM] * 6,
        out_specs=[VMEM] * 5,
        scratch_shapes=[
            pltpu.VMEM((2, block_count, LANES, LANES), f32),
            pltpu.VMEM((2, block_count, BLOCK, LANES), f32),
        ],
    )(read, keys, values, erase, decay, spike)


def finish_kernel(place_ref, got_ref, local_ref, readout_ref, prefix_ref, start_ref, gain_ref, mixed_ref):
    place = place_ref[0]
    count = got_ref.shape[0]
    block_count = prefix_ref.shape[1]
    entry = [jnp.zeros((BLOCK, LANES), f32)] * 2
    for k in range(count - 1):
        for way in range(2):
            j = k if way == 0 else count - 1 - k
            passed = j < place if way == 0 else j > place
            moved = exact_right_dot(entry[way], both_heads(got_ref[j, :BLOCK, :]), NN)
            entry[way] = jnp.where(passed, moved + got_ref[j, BLOCK:, :].astype(f32), entry[way])
    entry_halves = [halves(e) for e in entry]
    gain = gain_ref[...].astype(f32)
    for block in range(block_count):
        parts = []
        for way in range(2):
            high, low = entry_halves[way]
            prefix = prefix_ref[way, block]
            prefix_high, prefix_low = [both_heads(p) for p in halves(prefix)]
            both = raw_dot(jnp.concatenate([high, low], axis=0), prefix_high, NN)
            state = both[:BLOCK] + both[BLOCK:] + raw_dot(high, prefix_low, NN)
            parts.append([both_heads(p) for p in halves(state + start_ref[way, block])])
        state_high, state_low = [jnp.concatenate([parts[0][k], parts[1][k]], axis=1) for k in (0, 1)]
        at = slice(block * BLOCK, (block + 1) * BLOCK)
        read_high, read_low = halves(readout_ref[at, :])
        both = raw_dot(jnp.concatenate([read_high, read_low], axis=0), state_high, NT)
        mix = local_ref[at, :] + both[:BLOCK] + both[BLOCK:] + raw_dot(read_high, state_low, NT)
        center = mix - head_sum(mix) * (1.0 / BLOCK)
        spread = head_sum(center * center) * (1.0 / BLOCK)
        mixed_ref[at, :] = (center * lax.rsqrt(spread + GN_EPS) * gain).astype(bf16)


def finish_mix(place, got, local, readout, prefix, start, gain):
    return pl.pallas_call(
        finish_kernel,
        name="finish_mix",
        out_shape=jax.ShapeDtypeStruct(local.shape, bf16),
        in_specs=[pl.BlockSpec(memory_space=pltpu.SMEM)] + [VMEM] * 6,
        out_specs=VMEM,
    )(place, got, local, readout, prefix, start, gain)


def push_kernel(x_ref, o_ref, send_sem, recv_sem, *, axis, count, source, target):
    me = lax.axis_index(axis)
    barrier = pltpu.get_barrier_semaphore()
    for k in range(1, count):
        pl.semaphore_signal(barrier, inc=1, device_id={axis: lax.rem(me + k, count)})
    pl.semaphore_wait(barrier, count - 1)
    copies = []
    for k in range(1, count):
        peer = lax.rem(me + k, count)
        copy = pltpu.make_async_remote_copy(
            src_ref=source(x_ref, me, peer, count),
            dst_ref=target(o_ref, me),
            send_sem=send_sem.at[k],
            recv_sem=recv_sem.at[k],
            device_id={axis: peer},
        )
        copy.start()
        copies.append(copy)
    target(o_ref, me)[...] = source(x_ref, me, me, count)[...]
    for copy in copies:
        copy.wait()


def push(x, out_shape, axis, count, source, target, number, name):
    return pl.pallas_call(
        functools.partial(push_kernel, axis=axis, count=count, source=source, target=target),
        name=name,
        out_shape=jax.ShapeDtypeStruct(out_shape, x.dtype),
        in_specs=[VMEM],
        out_specs=VMEM,
        scratch_shapes=[pltpu.SemaphoreType.DMA((count,)), pltpu.SemaphoreType.DMA((count,))],
        compiler_params=pltpu.CompilerParams(collective_id=number, has_side_effects=True),
    )(x)


def way_for(x_ref, me, peer, count):
    return x_ref.at[(me + count - peer) // (count + 1)]


def slot_of_peer(x_ref, me, peer, count):
    return x_ref.at[peer]


def at_slot(o_ref, me):
    return o_ref.at[me]


def at_lanes(o_ref, me):
    return o_ref.at[:, pl.ds(pl.multiple_of(me * LANES, LANES), LANES)]


def expert_kernel(x_ref, gate_ref, up_ref, down_ref, *rest):
    o_ref = rest[-1]
    groups, rows, width = x_ref.shape
    x = x_ref[...].reshape(groups * rows, width)
    gate = raw_dot(x, gate_ref[0], NN)
    up = raw_dot(x, up_ref[0], NN)
    hidden = (gate / (1.0 + jnp.exp(-gate)) * up).astype(bf16)
    o_ref[...] = raw_dot(hidden, down_ref[0], NN).astype(bf16).reshape(groups, rows, width)


def expert_rows(slab, gate, up, down, rows, first, into, name):
    groups, _, width = slab.shape
    steps, _, hidden = gate.shape
    specs = [
        pl.BlockSpec((groups, rows, width), lambda e: (0, first + e, 0)),
        pl.BlockSpec((1, width, hidden), lambda e: (e, 0, 0)),
        pl.BlockSpec((1, width, hidden), lambda e: (e, 0, 0)),
        pl.BlockSpec((1, hidden, width), lambda e: (e, 0, 0)),
    ]
    arrays = [slab, gate, up, down]
    aliases = {}
    if into is not None:
        specs.append(pl.BlockSpec(memory_space=pl.ANY))
        arrays.append(into)
        aliases = {4: 0}
    return pl.pallas_call(
        expert_kernel,
        name=name,
        grid=(steps,),
        out_shape=jax.ShapeDtypeStruct(slab.shape, bf16),
        in_specs=specs,
        out_specs=pl.BlockSpec((groups, rows, width), lambda e: (0, first + e, 0)),
        input_output_aliases=aliases,
        compiler_params=pltpu.CompilerParams(vmem_limit_bytes=56 * 1024 * 1024),
    )(*arrays)


def body(
    layer_input,
    receptance,
    keys,
    values,
    erase_preact,
    decay_preact,
    decay_spike,
    head_norm_gain,
    output_weight,
    expert_norm_gain,
    routes,
    routing_weight,
    expert_gate_weight,
    expert_up_weight,
    expert_down_weight,
    shared_gate_weight,
    shared_up_weight,
    shared_down_weight,
):
    sp_count, tp_count = lax.axis_size(SP), lax.axis_size(TP)
    local, readout, prefix, start, whole = mixer_terms(
        receptance, keys, values, erase_preact, decay_preact, decay_spike
    )
    got = push(whole, (sp_count,) + whole.shape[1:], SP, sp_count, way_for, at_slot, 0, "states")
    place = lax.axis_index(SP).astype(jnp.int32).reshape(1)
    mixed = finish_mix(place, got, local, readout, prefix, start, head_norm_gain.reshape(1, -1))
    row_count, model_width = layer_input.shape
    token_major = push(
        mixed.reshape(tp_count, row_count, LANES),
        (row_count, model_width),
        TP,
        tp_count,
        slot_of_peer,
        at_lanes,
        1,
        "heads",
    )
    projected = jnp.dot(
        token_major,
        lax.all_gather(output_weight, TP, axis=0, tiled=True),
        preferred_element_type=f32,
    )
    residual = layer_input.astype(f32) + projected
    normed = residual * lax.rsqrt(jnp.mean(residual * residual, axis=-1, keepdims=True) + RMS_EPS)
    normed = (normed * expert_norm_gain.astype(f32)).astype(bf16)

    top_count = routes.shape[1]
    expert_local = expert_gate_weight.shape[0]
    capacity = 3
    room = 8
    slot_total = sp_count * room
    entries = routes.reshape(-1)
    entry_count = entries.shape[0]
    expert_hot = (entries[:, None] == jnp.arange(expert_local * sp_count)[None, :]).astype(jnp.int32)
    rank_in = jnp.sum((jnp.cumsum(expert_hot, axis=0) - 1) * expert_hot, axis=1)
    slot_of = entries // expert_local * room + entries % expert_local * capacity + rank_in
    slot_hot = slot_of[:, None] == jnp.arange(slot_total)[None, :]
    placing = jnp.sum(
        slot_hot.reshape(row_count, top_count, slot_total).astype(f32), axis=1
    ).astype(bf16)
    weighting = jnp.sum(
        jnp.where(slot_hot, routing_weight.reshape(-1, 1), 0.0).reshape(
            row_count, top_count, slot_total
        ),
        axis=1,
    )
    outgoing = lax.dot_general(placing, normed, TN, preferred_element_type=f32).astype(bf16)
    arrived = push(
        outgoing.reshape(sp_count, room, model_width),
        (sp_count, room, model_width),
        SP,
        sp_count,
        slot_of_peer,
        at_slot,
        2,
        "to_experts",
    ).reshape(slot_total, model_width)
    used = sp_count * capacity
    packed_row = jnp.arange(expert_local * used)
    from_slot = (
        packed_row % used // capacity * room
        + packed_row // used * capacity
        + packed_row % capacity
    )
    packing = (from_slot[:, None] == jnp.arange(slot_total)[None, :]).astype(bf16)
    packed = jnp.dot(packing, arrived, preferred_element_type=f32).astype(bf16)
    own_block = jnp.concatenate([packed, normed], axis=0)
    block_rows = own_block.shape[0]
    slab = lax.all_gather(own_block, TP, axis=0, tiled=True)
    slab = slab.reshape(tp_count, block_rows, model_width)
    outs = expert_rows(
        slab, expert_gate_weight, expert_up_weight, expert_down_weight, used, 0, None, "routed"
    )
    outs = expert_rows(
        slab,
        shared_gate_weight[None],
        shared_up_weight[None],
        shared_down_weight[None],
        row_count,
        expert_local * used // row_count,
        outs,
        "shared",
    )
    summed = lax.psum_scatter(
        outs.reshape(tp_count * block_rows, model_width), TP, scatter_dimension=0, tiled=True
    )
    unpacked = lax.dot_general(
        packing, summed[: expert_local * used], TN, preferred_element_type=f32
    ).astype(bf16)
    returned = push(
        unpacked.reshape(sp_count, room, model_width),
        (sp_count, room, model_width),
        SP,
        sp_count,
        slot_of_peer,
        at_slot,
        3,
        "to_tokens",
    ).reshape(slot_total, model_width)
    weight_high, weight_rest = halves(weighting)
    routed = jnp.dot(weight_high, returned, preferred_element_type=f32) + jnp.dot(
        weight_rest, returned, preferred_element_type=f32
    )
    return (residual + summed[expert_local * used :].astype(f32) + routed).astype(bf16)


def solution(mesh):
    both = (SP, TP)
    in_specs = (
        P(both, None),
        P(SP, TP),
        P(SP, TP),
        P(SP, TP),
        P(SP, TP),
        P(SP, TP),
        P(SP, TP),
        P(TP),
        P(TP, None),
        P(),
        P(both, None),
        P(both, None),
        P(SP, None, TP),
        P(SP, None, TP),
        P(SP, TP, None),
        P(None, TP),
        P(None, TP),
        P(TP, None),
    )
    return jax.shard_map(
        body, mesh=mesh, in_specs=in_specs, out_specs=P(both, None), check_vma=False
    )
```

```python
import functools

import jax
import jax.numpy as jnp
from jax import lax
from jax.experimental import pallas as pl
from jax.experimental.pallas import tpu as pltpu
from jax.sharding import PartitionSpec as P

SP = "sp"
TP = "tp"
BLOCK = 64
LANES = 128
GN_EPS = 0.00064
RMS_EPS = 1e-06
f32 = jnp.float32
bf16 = jnp.bfloat16
VMEM = pl.BlockSpec(memory_space=pltpu.VMEM)
NN = (((1,), (0,)), ((), ()))
NT = (((1,), (1,)), ((), ()))
TN = (((0,), (0,)), ((), ()))


def iota(shape, dim):
    return lax.broadcasted_iota(jnp.int32, shape, dim)


def halves(array):
    high = array.astype(bf16)
    return high, (array - high.astype(f32)).astype(bf16)


def raw_dot(left, right, dims):
    return lax.dot_general(left, right, dims, preferred_element_type=f32)


def both_heads(rows):
    lane = iota(rows.shape, 1)
    zero = jnp.zeros_like(rows)
    return jnp.concatenate(
        [jnp.where(lane < BLOCK, rows, zero), jnp.where(lane < BLOCK, zero, rows)], axis=0
    )


def fine_dot(left, right, dims, spread=False):
    left_high, left_low = halves(left)
    right_high, right_low = halves(right)
    if spread:
        right_high, right_low = both_heads(right_high), both_heads(right_low)
    if dims == TN:
        return raw_dot(
            jnp.concatenate([left_high, left_high, left_low], axis=0),
            jnp.concatenate([right_high, right_low, right_high], axis=0),
            TN,
        )
    count = left.shape[0]
    both = raw_dot(jnp.concatenate([left_high, left_low], axis=0), right_high, dims)
    return both[:count] + both[count:] + raw_dot(left_high, right_low, dims)


def exact_right_dot(left, right, dims):
    left_high, left_low = halves(left)
    count = left.shape[0]
    both = raw_dot(jnp.concatenate([left_high, left_low], axis=0), right, dims)
    return both[:count] + both[count:]


def head_sum(rows):
    ones = (iota((LANES, LANES), 0) // BLOCK == iota((LANES, LANES), 1) // BLOCK).astype(bf16)
    return exact_right_dot(rows, ones, NN)


def block_sums(log_decay):
    high = log_decay.astype(bf16)
    rest = log_decay - high.astype(f32)
    middle = rest.astype(bf16)
    low = (rest - middle.astype(f32)).astype(bf16)
    count = log_decay.shape[0]
    ones = (iota((count, count), 0) >= iota((count, count), 1)).astype(bf16)
    width = log_decay.shape[1]
    sums = raw_dot(ones, jnp.concatenate([high, middle, low], axis=1), NN)
    return sums[:, :width] + sums[:, width : 2 * width] + sums[:, 2 * width :]


def inverse(strict):
    row, lane = iota(strict.shape, 0), iota(strict.shape, 1) % BLOCK

    def within(size):
        return row // size == lane // size

    def product(left, right):
        return fine_dot(left, right, NN, spread=True)

    small = jnp.where(within(8), strict, 0.0)
    start = jnp.where(row == lane, 1.0, 0.0) - small
    square = product(small, small)
    both = product(jnp.concatenate([start, square], axis=0), square)
    result = start + both[:BLOCK]
    result = result + product(result, both[BLOCK:])
    for size in (8, 16, 32):
        edge = jnp.where(within(2 * size) & ~within(size), strict, 0.0)
        result = result - product(product(result, edge), result)
    return result


def one_way(unit, beta, key_rows, value_spread, read, left_unit, left_read, right, edge, lower):
    row, lane = iota((BLOCK, LANES), 0), iota((BLOCK, LANES), 1) % BLOCK
    strict = row > lane if lower else row < lane
    upto = row >= lane if lower else row <= lane
    unit_mid, read_mid = unit * left_unit, read * left_read
    beta_mid, key_mid = beta * right, key_rows * right
    left_high, left_low = halves(jnp.concatenate([unit_mid, read_mid], axis=0))
    beta_parts, key_parts = halves(beta_mid), halves(key_mid)
    right_high, right_low = [
        jnp.concatenate([both_heads(b), both_heads(k)], axis=0)
        for b, k in zip(beta_parts, key_parts)
    ]
    both = raw_dot(jnp.concatenate([left_high, left_low], axis=0), right_high, NT)
    pairs = both[: 2 * BLOCK] + both[2 * BLOCK :] + raw_dot(left_high, right_low, NT)
    erase_beta = jnp.where(strict, pairs[:BLOCK, :LANES], 0.0)
    erase_key = jnp.where(strict, pairs[:BLOCK, LANES:], 0.0)
    read_beta = jnp.where(upto, pairs[BLOCK:, :LANES], 0.0)
    read_key = jnp.where(upto, pairs[BLOCK:, LANES:], 0.0)
    keyed = exact_right_dot(jnp.concatenate([erase_key, read_key], axis=0), value_spread, NN)
    solver = inverse(erase_beta)
    lead = fine_dot(solver, unit_mid * edge, NN, spread=True)
    own = fine_dot(solver, -keyed[:BLOCK], NN, spread=True)
    solved = jnp.concatenate([lead, own], axis=1)
    parts = halves(solved)
    spread_parts = [
        jnp.concatenate([both_heads(p[:, :LANES]), both_heads(p[:, LANES:])], axis=1) for p in parts
    ]
    read_high, read_low = halves(read_beta)
    both = raw_dot(jnp.concatenate([read_high, read_low], axis=0), spread_parts[0], NN)
    applied = both[:BLOCK] + both[BLOCK:] + raw_dot(read_high, spread_parts[1], NN)
    readout = read_mid * edge - applied[:, :LANES]
    local = applied[:, LANES:] + keyed[BLOCK:]
    return solved, beta_mid * edge, key_mid * edge, readout, local


def mixer_kernel(
    read_ref,
    key_ref,
    value_ref,
    erase_ref,
    decay_ref,
    spike_ref,
    local_ref,
    readout_ref,
    prefix_ref,
    start_ref,
    whole_ref,
    move_ref,
    carry_ref,
    *,
    together,
):
    tokens = key_ref.shape[0]
    block_count = tokens // BLOCK
    lane = iota((BLOCK, LANES), 1)
    same_head = iota((LANES, LANES), 0) // BLOCK == iota((LANES, LANES), 1) // BLOCK
    diagonal = iota((LANES, LANES), 0) == iota((LANES, LANES), 1)

    def one_block(block):
        at = pl.ds(pl.multiple_of(block * BLOCK, BLOCK), BLOCK)
        key_rows = key_ref[at, :].astype(f32)
        read = read_ref[at, :].astype(f32)
        value = value_ref[at, :]
        unit = key_rows * lax.rsqrt(head_sum(key_rows * key_rows) + 1e-06)
        beta = unit * jax.nn.sigmoid(erase_ref[at, :].astype(f32))
        decay_in = decay_ref[at, :].astype(f32)
        spike = jnp.where(lane < BLOCK, spike_ref[at, 0:1], spike_ref[at, 1:2])
        log_decay = -jnp.exp(-jax.nn.softplus(-decay_in) - 0.5) + spike
        upto = block_sums(log_decay)
        total = upto[BLOCK - 1 :, :]
        middle = 0.5 * total
        ahead = upto - log_decay
        before, after = jnp.exp(ahead - middle), jnp.exp(upto - middle)
        until, since = jnp.exp(middle - upto), jnp.exp(middle - ahead)
        edge = jnp.exp(middle)
        value_spread = both_heads(value)
        ways = (
            one_way(unit, beta, key_rows, value_spread, read, before, after, until, edge, True),
            one_way(unit, beta, key_rows, value_spread, read, until, since, before, edge, False),
        )
        local_ref[at, :] = ways[0][4] + ways[1][4]
        over = jnp.exp(total)
        for way, (solved, beta_end, key_end, readout, _) in enumerate(ways):
            readout_ref[at, way * LANES : (way + 1) * LANES] = readout
            moved = fine_dot(solved, beta_end, TN)
            key_high, key_low = halves(key_end)
            keyed = raw_dot(
                jnp.concatenate([value, value], axis=0),
                jnp.concatenate([key_high, key_low], axis=0),
                TN,
            )
            move_ref[way, block] = jnp.where(
                same_head, jnp.where(diagonal, over, 0.0) - moved[:LANES], 0.0
            )
            carry = jnp.where(same_head, moved[LANES:] + keyed, 0.0)
            carry_ref[way, block] = carry[:BLOCK] + carry[BLOCK:]

    def step(index, _):
        for k in range(together):
            one_block(index * together + k)
        return 0

    lax.fori_loop(0, block_count // together, step, 0)
    identity = jnp.where(iota((BLOCK, LANES), 0) == iota((BLOCK, LANES), 1) % BLOCK, 1.0, 0.0)
    running = [jnp.concatenate([identity, jnp.zeros_like(identity)], axis=0)] * 2
    for k in range(block_count):
        for way in range(2):
            block = k if way == 0 else block_count - 1 - k
            now = running[way]
            prefix_ref[way, block] = now[:BLOCK]
            start_ref[way, block] = now[BLOCK:]
            after = fine_dot(now, move_ref[way, block], NN)
            running[way] = jnp.concatenate(
                [after[:BLOCK], after[BLOCK:] + carry_ref[way, block]], axis=0
            )
    for way in range(2):
        whole_ref[way] = running[way].astype(bf16)


def mixer_terms(read, keys, values, erase, decay, spike):
    tokens = keys.shape[0]
    block_count = tokens // BLOCK
    shape = jax.ShapeDtypeStruct
    return pl.pallas_call(
        functools.partial(mixer_kernel, together=2),
        name="mixer_terms",
        out_shape=(
            shape((tokens, LANES), f32),
            shape((tokens, 2 * LANES), f32),
            shape((2, block_count, BLOCK, LANES), f32),
            shape((2, block_count, BLOCK, LANES), f32),
            shape((2, 2 * BLOCK, LANES), bf16),
        ),
        in_specs=[VMEM] * 6,
        out_specs=[VMEM] * 5,
        scratch_shapes=[
            pltpu.VMEM((2, block_count, LANES, LANES), f32),
            pltpu.VMEM((2, block_count, BLOCK, LANES), f32),
        ],
    )(read, keys, values, erase, decay, spike)


def finish_kernel(place_ref, got_ref, local_ref, readout_ref, prefix_ref, start_ref, gain_ref, mixed_ref):
    place = place_ref[0]
    count = got_ref.shape[0]
    block_count = prefix_ref.shape[1]
    entry = [jnp.zeros((BLOCK, LANES), f32)] * 2
    for k in range(count - 1):
        for way in range(2):
            j = k if way == 0 else count - 1 - k
            passed = j < place if way == 0 else j > place
            moved = exact_right_dot(entry[way], both_heads(got_ref[j, :BLOCK, :]), NN)
            entry[way] = jnp.where(passed, moved + got_ref[j, BLOCK:, :].astype(f32), entry[way])
    entry_halves = [halves(e) for e in entry]
    gain = gain_ref[...].astype(f32)
    for block in range(block_count):
        parts = []
        for way in range(2):
            high, low = entry_halves[way]
            prefix = prefix_ref[way, block]
            prefix_high, prefix_low = [both_heads(p) for p in halves(prefix)]
            both = raw_dot(jnp.concatenate([high, low], axis=0), prefix_high, NN)
            state = both[:BLOCK] + both[BLOCK:] + raw_dot(high, prefix_low, NN)
            parts.append([both_heads(p) for p in halves(state + start_ref[way, block])])
        state_high, state_low = [jnp.concatenate([parts[0][k], parts[1][k]], axis=1) for k in (0, 1)]
        at = slice(block * BLOCK, (block + 1) * BLOCK)
        read_high, read_low = halves(readout_ref[at, :])
        both = raw_dot(jnp.concatenate([read_high, read_low], axis=0), state_high, NT)
        mix = local_ref[at, :] + both[:BLOCK] + both[BLOCK:] + raw_dot(read_high, state_low, NT)
        center = mix - head_sum(mix) * (1.0 / BLOCK)
        spread = head_sum(center * center) * (1.0 / BLOCK)
        mixed_ref[at, :] = (center * lax.rsqrt(spread + GN_EPS) * gain).astype(bf16)


def finish_mix(place, got, local, readout, prefix, start, gain):
    return pl.pallas_call(
        finish_kernel,
        name="finish_mix",
        out_shape=jax.ShapeDtypeStruct(local.shape, bf16),
        in_specs=[pl.BlockSpec(memory_space=pltpu.SMEM)] + [VMEM] * 6,
        out_specs=VMEM,
    )(place, got, local, readout, prefix, start, gain)


def push_kernel(x_ref, o_ref, send_sem, recv_sem, *, axis, count, source, target):
    me = lax.axis_index(axis)
    barrier = pltpu.get_barrier_semaphore()
    for k in range(1, count):
        pl.semaphore_signal(barrier, inc=1, device_id={axis: lax.rem(me + k, count)})
    pl.semaphore_wait(barrier, count - 1)
    copies = []
    for k in range(1, count):
        peer = lax.rem(me + k, count)
        copy = pltpu.make_async_remote_copy(
            src_ref=source(x_ref, me, peer, count),
            dst_ref=target(o_ref, me),
            send_sem=send_sem.at[k],
            recv_sem=recv_sem.at[k],
            device_id={axis: peer},
        )
        copy.start()
        copies.append(copy)
    target(o_ref, me)[...] = source(x_ref, me, me, count)[...]
    for copy in copies:
        copy.wait()


def push(x, out_shape, axis, count, source, target, number, name):
    return pl.pallas_call(
        functools.partial(push_kernel, axis=axis, count=count, source=source, target=target),
        name=name,
        out_shape=jax.ShapeDtypeStruct(out_shape, x.dtype),
        in_specs=[VMEM],
        out_specs=VMEM,
        scratch_shapes=[pltpu.SemaphoreType.DMA((count,)), pltpu.SemaphoreType.DMA((count,))],
        compiler_params=pltpu.CompilerParams(collective_id=number, has_side_effects=True),
    )(x)


def way_for(x_ref, me, peer, count):
    return x_ref.at[(me + count - peer) // (count + 1)]


def slot_of_peer(x_ref, me, peer, count):
    return x_ref.at[peer]


def at_slot(o_ref, me):
    return o_ref.at[me]


def at_lanes(o_ref, me):
    return o_ref.at[:, pl.ds(pl.multiple_of(me * LANES, LANES), LANES)]


def ring_kernel(
    x_ref,
    expert_gate,
    expert_up,
    expert_down,
    shared_gate,
    shared_up,
    shared_down,
    o_ref,
    blocks,
    partial,
    other,
    right_in,
    left_in,
    gate,
    up,
    down,
    weight_sem,
    gather_send,
    gather_recv,
    pass_send,
    pass_recv,
    pair_send,
    pair_recv,
    sum_send,
    sum_recv,
    *,
    axis,
    chips,
    used,
):
    me = lax.axis_index(axis)
    chip, core = me // 2, lax.rem(me, 2)
    rows, width = x_ref.shape
    half = rows // 2
    far = chips // 2
    steps = chips - 1
    local_experts = expert_gate.shape[0]
    hidden = shared_gate.shape[1]
    ways = ((1, 0), (-1, 1))

    def chip_at(distance):
        return lax.rem(chip + distance + chips, chips)

    def slot(distance, which):
        return chip_at(distance) * 2 + which

    ahead, behind, twin = slot(1, core), slot(-1, core), chip * 2 + 1 - core

    weight_copies = []
    for k, (pair, single, into) in enumerate(
        ((expert_gate, shared_gate, gate), (expert_up, shared_up, up), (expert_down, shared_down, down))
    ):
        weight_copies.append(
            pltpu.make_async_copy(pair, into.at[pl.ds(0, local_experts)], weight_sem.at[2 * k])
        )
        weight_copies.append(
            pltpu.make_async_copy(single, into.at[local_experts], weight_sem.at[2 * k + 1])
        )
    for copy in weight_copies:
        copy.start()

    barrier = pltpu.get_barrier_semaphore()
    for peer in (ahead, behind, twin):
        pl.semaphore_signal(barrier, inc=1, device_id={axis: peer})
    pl.semaphore_wait(barrier, 3)

    def part(which):
        return pl.ds(which * half, half)

    def half_of(way, step):
        return step % 2 if way == 0 else 1 - step % 2

    def remote(source, target, send, recv, peer):
        return pltpu.make_async_remote_copy(
            src_ref=source, dst_ref=target, send_sem=send, recv_sem=recv, device_id={axis: peer}
        )

    sent = []

    def start(copy):
        copy.start()
        sent.append(copy)

    def gather_copy(way, step):
        sign = ways[way][0]
        at = slot(-sign * (step // 2), core)
        piece = part(half_of(way, step))
        source = x_ref.at[piece] if step < 2 else blocks.at[at, piece]
        return remote(
            source,
            blocks.at[at, piece],
            gather_send.at[way, step],
            gather_recv.at[way, step],
            ahead if way == 0 else behind,
        )

    def pass_copy(way, step):
        sign = ways[way][0]
        at = slot(-sign * (step // 2 + 1), core)
        piece = part(half_of(way, step))
        return remote(
            blocks.at[at, piece],
            blocks.at[at, piece],
            pass_send.at[way, step],
            pass_recv.at[way, step],
            twin,
        )

    own_copy = remote(
        x_ref, blocks.at[me], pass_send.at[0, steps], pass_recv.at[0, steps], twin
    )
    for step in (0, 1):
        for way in (0, 1):
            start(gather_copy(way, step))
    start(own_copy)
    blocks[me] = x_ref[...]

    def experts_on(distance):
        first = chip_at(distance) * 2

        def one(k, _):
            which = lax.rem(k + local_experts, local_experts + 1)
            begin = pl.multiple_of(
                used * (k // 2) + (rows - used) * ((2 - k) // 2), 16
            )
            at = pl.ds(begin, used)
            x = blocks[pl.ds(first, 2), at, :].reshape(2 * used, width)
            gated = raw_dot(x, gate[which], NN)
            lifted = raw_dot(x, up[which], NN)
            inner = (gated / (1.0 + jnp.exp(-gated)) * lifted).astype(bf16)
            partial[pl.ds(first, 2), at, :] = (
                raw_dot(inner, down[which], NN).astype(bf16).reshape(2, used, width)
            )
            return 0

        lax.fori_loop(0, local_experts + 1, one, 0)

    def pair_copy(distance):
        at = slot(distance, 1 - core)
        index = chip_at(distance)
        return remote(
            partial.at[at], other.at[index], pair_send.at[index], pair_recv.at[index], twin
        )

    for copy in weight_copies:
        copy.wait()
    own_copy.wait_recv()
    experts_on(0)
    waiting = [0]
    for step in range(steps):
        for way in (0, 1):
            gather_copy(way, step).wait_recv()
            if step + 2 < steps:
                start(gather_copy(way, step + 2))
            start(pass_copy(way, step))
        for distance in waiting:
            start(pair_copy(distance))
        waiting = []
        if step % 2 == 1:
            for way in (0, 1):
                for s in (step - 1, step):
                    pass_copy(way, s).wait_recv()
            distance = (step + 1) // 2

            def both(k, _):
                experts_on(distance * (2 * k - 1))
                return 0

            lax.fori_loop(0, 2, both, 0)
            waiting = [-distance, distance]
    for way in (0, 1):
        pass_copy(way, steps - 1).wait_recv()
    experts_on(far)
    for distance in (far,):
        start(pair_copy(distance))

    def sum_distance(step):
        return far - (step + 1) // 2

    inbox = (right_in, left_in)

    def sum_copy(way, step):
        sign = ways[way][0]
        at = slot(sign * sum_distance(step), core)
        return remote(
            partial.at[at, part(sum_half_of(way, step))],
            inbox[way].at[step],
            sum_send.at[way, step],
            sum_recv.at[way, step],
            ahead if way == 0 else behind,
        )

    def sum_half_of(way, step):
        return step % 2 if way == 0 else 1 - step % 2

    met = set()

    def meet(distance):
        key = distance % chips
        if key not in met:
            met.add(key)
            pair_copy(distance).wait_recv()

    for step in range(steps):
        for way in (0, 1):
            sign = ways[way][0]
            distance = sign * sum_distance(step)
            meet(distance)
            at, piece = slot(distance, core), part(sum_half_of(way, step))
            total = partial[at, piece, :].astype(f32) + other[chip_at(distance), piece, :].astype(f32)
            if step >= 2:
                sum_copy(way, step - 2).wait_recv()
                total = total + inbox[way][step - 2].astype(f32)
            partial[at, piece, :] = total.astype(bf16)
        for way in (0, 1):
            start(sum_copy(way, step))
    meet(0)
    for which in (0, 1):
        piece = part(which)
        total = partial[me, piece, :].astype(f32) + other[chip, piece, :].astype(f32)
        for way in (0, 1):
            step = steps - 2 if sum_half_of(way, steps - 2) == which else steps - 1
            sum_copy(way, step).wait_recv()
            total = total + inbox[way][step].astype(f32)
        o_ref[piece, :] = total.astype(bf16)
    for copy in sent:
        copy.wait_send()


def experts_over(x, weights, axis, devices, used, number, name):
    rows, width = x.shape
    hidden = weights[3].shape[1]
    local_experts = weights[0].shape[0]
    chips = devices // 2
    steps = chips - 1
    dma = pltpu.SemaphoreType.DMA
    anywhere = pl.BlockSpec(memory_space=pl.ANY)
    return pl.pallas_call(
        functools.partial(ring_kernel, axis=axis, chips=chips, used=used),
        name=name,
        out_shape=jax.ShapeDtypeStruct((rows, width), bf16),
        in_specs=[VMEM] + [anywhere] * 6,
        out_specs=VMEM,
        scratch_shapes=[
            pltpu.VMEM((devices, rows, width), bf16),
            pltpu.VMEM((devices, rows, width), bf16),
            pltpu.VMEM((chips, rows, width), bf16),
            pltpu.VMEM((steps, rows // 2, width), bf16),
            pltpu.VMEM((steps, rows // 2, width), bf16),
            pltpu.VMEM((local_experts + 1, width, hidden), bf16),
            pltpu.VMEM((local_experts + 1, width, hidden), bf16),
            pltpu.VMEM((local_experts + 1, hidden, width), bf16),
            dma((6,)),
            dma((2, steps)),
            dma((2, steps)),
            dma((2, steps + 1)),
            dma((2, steps + 1)),
            dma((chips,)),
            dma((chips,)),
            dma((2, steps)),
            dma((2, steps)),
        ],
        compiler_params=pltpu.CompilerParams(
            collective_id=number, has_side_effects=True, vmem_limit_bytes=58 * 1024 * 1024
        ),
    )(x, *weights)


def body(
    layer_input,
    receptance,
    keys,
    values,
    erase_preact,
    decay_preact,
    decay_spike,
    head_norm_gain,
    output_weight,
    expert_norm_gain,
    routes,
    routing_weight,
    expert_gate_weight,
    expert_up_weight,
    expert_down_weight,
    shared_gate_weight,
    shared_up_weight,
    shared_down_weight,
):
    sp_count, tp_count = lax.axis_size(SP), lax.axis_size(TP)
    local, readout, prefix, start, whole = mixer_terms(
        receptance, keys, values, erase_preact, decay_preact, decay_spike
    )
    got = push(whole, (sp_count,) + whole.shape[1:], SP, sp_count, way_for, at_slot, 0, "states")
    place = lax.axis_index(SP).astype(jnp.int32).reshape(1)
    mixed = finish_mix(place, got, local, readout, prefix, start, head_norm_gain.reshape(1, -1))
    row_count, model_width = layer_input.shape
    token_major = push(
        mixed.reshape(tp_count, row_count, LANES),
        (row_count, model_width),
        TP,
        tp_count,
        slot_of_peer,
        at_lanes,
        1,
        "heads",
    )
    projected = jnp.dot(
        token_major,
        lax.all_gather(output_weight, TP, axis=0, tiled=True),
        preferred_element_type=f32,
    )
    residual = layer_input.astype(f32) + projected
    normed = residual * lax.rsqrt(jnp.mean(residual * residual, axis=-1, keepdims=True) + RMS_EPS)
    normed = (normed * expert_norm_gain.astype(f32)).astype(bf16)

    top_count = routes.shape[1]
    expert_local = expert_gate_weight.shape[0]
    capacity = 3
    room = 8
    slot_total = sp_count * room
    entries = routes.reshape(-1)
    entry_count = entries.shape[0]
    expert_hot = (entries[:, None] == jnp.arange(expert_local * sp_count)[None, :]).astype(jnp.int32)
    rank_in = jnp.sum((jnp.cumsum(expert_hot, axis=0) - 1) * expert_hot, axis=1)
    slot_of = entries // expert_local * room + entries % expert_local * capacity + rank_in
    slot_hot = slot_of[:, None] == jnp.arange(slot_total)[None, :]
    placing = jnp.sum(
        slot_hot.reshape(row_count, top_count, slot_total).astype(f32), axis=1
    ).astype(bf16)
    weighting = jnp.sum(
        jnp.where(slot_hot, routing_weight.reshape(-1, 1), 0.0).reshape(
            row_count, top_count, slot_total
        ),
        axis=1,
    )
    outgoing = lax.dot_general(placing, normed, TN, preferred_element_type=f32).astype(bf16)
    arrived = push(
        outgoing.reshape(sp_count, room, model_width),
        (sp_count, room, model_width),
        SP,
        sp_count,
        slot_of_peer,
        at_slot,
        2,
        "to_experts",
    ).reshape(slot_total, model_width)
    used = sp_count * capacity
    packed_row = jnp.arange(expert_local * used)
    from_slot = (
        packed_row % used // capacity * room
        + packed_row // used * capacity
        + packed_row % capacity
    )
    packing = (from_slot[:, None] == jnp.arange(slot_total)[None, :]).astype(bf16)
    packed = jnp.dot(packing, arrived, preferred_element_type=f32).astype(bf16)
    own_block = jnp.concatenate([packed, normed], axis=0)
    summed = experts_over(
        own_block,
        (
            expert_gate_weight,
            expert_up_weight,
            expert_down_weight,
            shared_gate_weight,
            shared_up_weight,
            shared_down_weight,
        ),
        TP,
        tp_count,
        used,
        4,
        "experts",
    )
    unpacked = lax.dot_general(
        packing, summed[: expert_local * used], TN, preferred_element_type=f32
    ).astype(bf16)
    returned = push(
        unpacked.reshape(sp_count, room, model_width),
        (sp_count, room, model_width),
        SP,
        sp_count,
        slot_of_peer,
        at_slot,
        3,
        "to_tokens",
    ).reshape(slot_total, model_width)
    weight_high, weight_rest = halves(weighting)
    routed = jnp.dot(weight_high, returned, preferred_element_type=f32) + jnp.dot(
        weight_rest, returned, preferred_element_type=f32
    )
    return (residual + summed[expert_local * used :].astype(f32) + routed).astype(bf16)


def solution(mesh):
    both = (SP, TP)
    in_specs = (
        P(both, None),
        P(SP, TP),
        P(SP, TP),
        P(SP, TP),
        P(SP, TP),
        P(SP, TP),
        P(SP, TP),
        P(TP),
        P(TP, None),
        P(),
        P(both, None),
        P(both, None),
        P(SP, None, TP),
        P(SP, None, TP),
        P(SP, TP, None),
        P(None, TP),
        P(None, TP),
        P(TP, None),
    )
    return jax.shard_map(
        body, mesh=mesh, in_specs=in_specs, out_specs=P(both, None), check_vma=False
    )
```

```python
import functools

import jax
import jax.numpy as jnp
from jax import lax
from jax.experimental import pallas as pl
from jax.experimental.pallas import tpu as pltpu
from jax.sharding import PartitionSpec as P

SP = "sp"
TP = "tp"
BLOCK = 64
LANES = 128
GN_EPS = 0.00064
RMS_EPS = 1e-06
f32 = jnp.float32
bf16 = jnp.bfloat16
VMEM = pl.BlockSpec(memory_space=pltpu.VMEM)
NN = (((1,), (0,)), ((), ()))
NT = (((1,), (1,)), ((), ()))
TN = (((0,), (0,)), ((), ()))


def iota(shape, dim):
    return lax.broadcasted_iota(jnp.int32, shape, dim)


def halves(array):
    high = array.astype(bf16)
    return high, (array - high.astype(f32)).astype(bf16)


def raw_dot(left, right, dims):
    return lax.dot_general(left, right, dims, preferred_element_type=f32)


def head_mask(count, dtype):
    first = (iota((count, LANES), 1) < BLOCK).astype(f32)
    return first.astype(dtype), (1.0 - first).astype(dtype)


def both_heads(rows):
    first, second = head_mask(rows.shape[0], rows.dtype)
    return jnp.concatenate([rows * first, rows * second], axis=0)


def fine_dot(left, right, dims, spread=False):
    left_high, left_low = halves(left)
    right_high, right_low = halves(right)
    if spread:
        right_high, right_low = both_heads(right_high), both_heads(right_low)
    if dims == TN:
        return raw_dot(
            jnp.concatenate([left_high, left_high, left_low], axis=0),
            jnp.concatenate([right_high, right_low, right_high], axis=0),
            TN,
        )
    count = left.shape[0]
    both = raw_dot(jnp.concatenate([left_high, left_low], axis=0), right_high, dims)
    return both[:count] + both[count:] + raw_dot(left_high, right_low, dims)


def exact_right_dot(left, right, dims):
    left_high, left_low = halves(left)
    count = left.shape[0]
    both = raw_dot(jnp.concatenate([left_high, left_low], axis=0), right, dims)
    return both[:count] + both[count:]


def head_sum(rows):
    ones = (iota((LANES, LANES), 0) // BLOCK == iota((LANES, LANES), 1) // BLOCK).astype(bf16)
    return exact_right_dot(rows, ones, NN)


def block_sums(log_decay):
    high = log_decay.astype(bf16)
    rest = log_decay - high.astype(f32)
    middle = rest.astype(bf16)
    low = (rest - middle.astype(f32)).astype(bf16)
    count = log_decay.shape[0]
    ones = (iota((count, count), 0) >= iota((count, count), 1)).astype(bf16)
    width = log_decay.shape[1]
    sums = raw_dot(ones, jnp.concatenate([high, middle, low], axis=1), NN)
    return sums[:, :width] + sums[:, width : 2 * width] + sums[:, 2 * width :]


def inverses(stricts):
    row, lane = iota((BLOCK, LANES), 0), iota((BLOCK, LANES), 1) % BLOCK

    def within(size):
        return row // size == lane // size

    def products(lefts, rights):
        return [fine_dot(left, right, NN, spread=True) for left, right in zip(lefts, rights)]

    smalls = [jnp.where(within(8), strict, 0.0) for strict in stricts]
    starts = [jnp.where(row == lane, 1.0, 0.0) - small for small in smalls]
    squares = products(smalls, smalls)
    boths = products([jnp.concatenate(p, axis=0) for p in zip(starts, squares)], squares)
    results = [start + both[:BLOCK] for start, both in zip(starts, boths)]
    more = products(results, [both[BLOCK:] for both in boths])
    results = [r + m for r, m in zip(results, more)]
    for size in (8, 16, 32):
        keep = within(2 * size) & ~within(size)
        edges = products(results, [jnp.where(keep, strict, 0.0) for strict in stricts])
        more = products(edges, results)
        results = [r - m for r, m in zip(results, more)]
    return results


def block_terms(chains):
    row, lane = iota((BLOCK, LANES), 0), iota((BLOCK, LANES), 1) % BLOCK
    scaled, pairs = [], []
    for unit, beta, key_rows, _, read, left_unit, left_read, right, _, _ in chains:
        scaled.append((unit * left_unit, read * left_read, beta * right, key_rows * right))
    for unit_mid, read_mid, beta_mid, key_mid in scaled:
        left_high, left_low = halves(jnp.concatenate([unit_mid, read_mid], axis=0))
        right_high, right_low = [
            jnp.concatenate([both_heads(b), both_heads(k)], axis=0)
            for b, k in zip(halves(beta_mid), halves(key_mid))
        ]
        both = raw_dot(jnp.concatenate([left_high, left_low], axis=0), right_high, NT)
        pairs.append(both[: 2 * BLOCK] + both[2 * BLOCK :] + raw_dot(left_high, right_low, NT))
    erase_betas, keyeds, read_betas = [], [], []
    for pair, chain in zip(pairs, chains):
        strict = row > lane if chain[-1] else row < lane
        upto = row >= lane if chain[-1] else row <= lane
        erase_betas.append(jnp.where(strict, pair[:BLOCK, :LANES], 0.0))
        erase_key = jnp.where(strict, pair[:BLOCK, LANES:], 0.0)
        read_betas.append(jnp.where(upto, pair[BLOCK:, :LANES], 0.0))
        read_key = jnp.where(upto, pair[BLOCK:, LANES:], 0.0)
        keyeds.append(
            exact_right_dot(jnp.concatenate([erase_key, read_key], axis=0), chain[3], NN)
        )
    solvers = inverses(erase_betas)
    solved = []
    for solver, (unit_mid, _, _, _), keyed, chain in zip(solvers, scaled, keyeds, chains):
        solver_high, solver_low = halves(solver)
        right_high, right_low = [
            jnp.concatenate([both_heads(u), both_heads(k)], axis=1)
            for u, k in zip(halves(unit_mid * chain[8]), halves(-keyed[:BLOCK]))
        ]
        both = raw_dot(jnp.concatenate([solver_high, solver_low], axis=0), right_high, NN)
        solved.append(both[:BLOCK] + both[BLOCK:] + raw_dot(solver_high, right_low, NN))
    terms = []
    for found, read_beta, keyed, scale, chain in zip(solved, read_betas, keyeds, scaled, chains):
        spread_parts = [
            jnp.concatenate([both_heads(p[:, :LANES]), both_heads(p[:, LANES:])], axis=1)
            for p in halves(found)
        ]
        read_high, read_low = halves(read_beta)
        both = raw_dot(jnp.concatenate([read_high, read_low], axis=0), spread_parts[0], NN)
        applied = both[:BLOCK] + both[BLOCK:] + raw_dot(read_high, spread_parts[1], NN)
        readout = scale[1] * chain[8] - applied[:, :LANES]
        local = applied[:, LANES:] + keyed[BLOCK:]
        terms.append((found, scale[2] * chain[8], scale[3] * chain[8], readout, local))
    return terms


def mixer_kernel(
    read_ref,
    key_ref,
    value_ref,
    erase_ref,
    decay_ref,
    spike_ref,
    local_ref,
    readout_ref,
    prefix_ref,
    start_ref,
    got_ref,
    move_ref,
    carry_ref,
    whole_ref,
    send_sem,
    recv_sem,
    *,
    together,
):
    barrier, expected = meet_peers(SP, got_ref.shape[0], [])
    tokens = key_ref.shape[0]
    block_count = tokens // BLOCK
    lane = iota((BLOCK, LANES), 1)
    same_head = iota((LANES, LANES), 0) // BLOCK == iota((LANES, LANES), 1) // BLOCK
    diagonal = iota((LANES, LANES), 0) == iota((LANES, LANES), 1)

    def some_blocks(blocks):
        chains, totals, values = [], [], []
        places = [pl.ds(pl.multiple_of(block * BLOCK, BLOCK), BLOCK) for block in blocks]
        for at in places:
            key_rows = key_ref[at, :].astype(f32)
            read = read_ref[at, :].astype(f32)
            value = value_ref[at, :]
            unit = key_rows * lax.rsqrt(head_sum(key_rows * key_rows) + 1e-06)
            beta = unit * jax.nn.sigmoid(erase_ref[at, :].astype(f32))
            decay_in = decay_ref[at, :].astype(f32)
            spike = jnp.where(lane < BLOCK, spike_ref[at, 0:1], spike_ref[at, 1:2])
            log_decay = -jnp.exp(-jax.nn.softplus(-decay_in) - 0.5) + spike
            upto = block_sums(log_decay)
            total = upto[BLOCK - 1 :, :]
            middle = 0.5 * total
            ahead = upto - log_decay
            before, after = jnp.exp(ahead - middle), jnp.exp(upto - middle)
            until, since = jnp.exp(middle - upto), jnp.exp(middle - ahead)
            edge = jnp.exp(middle)
            shared = (unit, beta, key_rows, both_heads(value), read)
            chains.append(shared + (before, after, until, edge, True))
            chains.append(shared + (until, since, before, edge, False))
            totals.append(total)
            values.append(value)
        terms = block_terms(chains)
        for k, at in enumerate(places):
            local_ref[at, :] = terms[2 * k][4] + terms[2 * k + 1][4]
        for k, (solved, beta_end, key_end, readout, _) in enumerate(terms):
            way, at, value = k % 2, places[k // 2], values[k // 2]
            readout_ref[at, way * LANES : (way + 1) * LANES] = readout
            moved = fine_dot(solved, beta_end, TN)
            key_high, key_low = halves(key_end)
            keyed = raw_dot(
                jnp.concatenate([value, value], axis=0),
                jnp.concatenate([key_high, key_low], axis=0),
                TN,
            )
            move_ref[way, blocks[k // 2]] = jnp.where(
                same_head, jnp.where(diagonal, jnp.exp(totals[k // 2]), 0.0) - moved[:LANES], 0.0
            )
            carry = jnp.where(same_head, moved[LANES:] + keyed, 0.0)
            carry_ref[way, blocks[k // 2]] = carry[:BLOCK] + carry[BLOCK:]

    def step(index, _):
        some_blocks([index * together + k for k in range(together)])
        return 0

    lax.fori_loop(0, block_count // together, step, 0)
    identity = jnp.where(iota((BLOCK, LANES), 0) == iota((BLOCK, LANES), 1) % BLOCK, 1.0, 0.0)
    running = [jnp.concatenate([identity, jnp.zeros_like(identity)], axis=0)] * 2
    for k in range(block_count):
        for way in range(2):
            block = k if way == 0 else block_count - 1 - k
            now = running[way]
            prefix_ref[way, block] = now[:BLOCK]
            start_ref[way, block] = now[BLOCK:]
            after = fine_dot(now, move_ref[way, block], NN)
            running[way] = jnp.concatenate(
                [after[:BLOCK], after[BLOCK:] + carry_ref[way, block]], axis=0
            )
    for way in range(2):
        whole_ref[way] = running[way].astype(bf16)
    pl.semaphore_wait(barrier, expected)
    me, count = lax.axis_index(SP), got_ref.shape[0]
    states = Push(
        SP,
        lambda peer: whole_ref.at[(me + count - peer) // (count + 1)],
        got_ref,
        (send_sem, recv_sem),
    )
    states.begin()
    states.arrive()
    states.leave()


def mixer_terms(read, keys, values, erase, decay, spike, sp_count, number):
    tokens = keys.shape[0]
    block_count = tokens // BLOCK
    shape = jax.ShapeDtypeStruct
    return pl.pallas_call(
        functools.partial(mixer_kernel, together=4),
        name="mixer_terms",
        out_shape=(
            shape((tokens, LANES), f32),
            shape((tokens, 2 * LANES), f32),
            shape((2, block_count, BLOCK, LANES), f32),
            shape((2, block_count, BLOCK, LANES), f32),
            shape((sp_count, 2 * BLOCK, LANES), bf16),
        ),
        in_specs=[VMEM] * 6,
        out_specs=[VMEM] * 5,
        scratch_shapes=[
            pltpu.VMEM((2, block_count, LANES, LANES), f32),
            pltpu.VMEM((2, block_count, BLOCK, LANES), f32),
            pltpu.VMEM((2, 2 * BLOCK, LANES), bf16),
            pltpu.SemaphoreType.DMA((sp_count,)),
            pltpu.SemaphoreType.DMA((sp_count,)),
        ],
        compiler_params=pltpu.CompilerParams(collective_id=number, has_side_effects=True),
    )(read, keys, values, erase, decay, spike)


class Ring:
    def __init__(self, axis, chips):
        self.axis, self.chips = axis, chips
        self.me = lax.axis_index(axis)
        self.chip, self.core = self.me // 2, lax.rem(self.me, 2)
        self.steps = chips - 1
        self.far = chips // 2
        self.next = (self.slot(1, self.core), self.slot(-1, self.core))
        self.twin = self.chip * 2 + 1 - self.core
        self.sent = []

    def chip_at(self, distance):
        return lax.rem(self.chip + distance + self.chips, self.chips)

    def slot(self, distance, which):
        return self.chip_at(distance) * 2 + which

    def copy(self, source, target, send, recv, peer):
        return pltpu.make_async_remote_copy(
            src_ref=source, dst_ref=target, send_sem=send, recv_sem=recv, device_id={self.axis: peer}
        )

    def start(self, copy):
        copy.start()
        self.sent.append(copy)

    def half_of(self, way, step):
        return step % 2 if way == 0 else 1 - step % 2


class Gather:
    def __init__(self, ring, own, blocks, sems):
        self.ring, self.own, self.blocks = ring, own, blocks
        self.send, self.recv, self.pass_send, self.pass_recv = sems
        self.half = own.shape[0] // 2

    def piece(self, way, step):
        return pl.ds(self.ring.half_of(way, step) * self.half, self.half)

    def hop(self, way, step):
        ring, piece = self.ring, self.piece(way, step)
        at = ring.slot((step // 2) * (-1 if way == 0 else 1), ring.core)
        source = self.own.at[piece] if step < 2 else self.blocks.at[at, piece]
        return ring.copy(
            source,
            self.blocks.at[at, piece],
            self.send.at[way, step],
            self.recv.at[way, step],
            ring.next[way],
        )

    def hand(self, way, step):
        ring, piece = self.ring, self.piece(way, step)
        at = ring.slot((step // 2 + 1) * (-1 if way == 0 else 1), ring.core)
        return ring.copy(
            self.blocks.at[at, piece],
            self.blocks.at[at, piece],
            self.pass_send.at[way, step],
            self.pass_recv.at[way, step],
            ring.twin,
        )

    def hand_own(self):
        ring = self.ring
        return ring.copy(
            self.own,
            self.blocks.at[ring.me],
            self.pass_send.at[0, ring.steps],
            self.pass_recv.at[0, ring.steps],
            ring.twin,
        )

    def begin(self):
        for step in (0, 1):
            for way in (0, 1):
                self.ring.start(self.hop(way, step))
        self.ring.start(self.hand_own())
        self.blocks[self.ring.me] = self.own[...]

    def advance(self, step):
        for way in (0, 1):
            self.hop(way, step).wait_recv()
            if step + 2 < self.ring.steps:
                self.ring.start(self.hop(way, step + 2))
            self.ring.start(self.hand(way, step))

    def handed(self, *steps):
        for step in steps:
            for way in (0, 1):
                self.hand(way, step).wait_recv()


class Sum:
    def __init__(self, ring, partial, other, inbox, sems):
        self.ring, self.partial, self.other, self.inbox = ring, partial, other, inbox
        self.pair_send, self.pair_recv, self.send_sem, self.recv_sem = sems
        self.half = partial.shape[1] // 2
        self.met = set()

    def pair(self, distance):
        ring = self.ring
        index = ring.chip_at(distance)
        return ring.copy(
            self.partial.at[ring.slot(distance, 1 - ring.core)],
            self.other.at[index],
            self.pair_send.at[index],
            self.pair_recv.at[index],
            ring.twin,
        )

    def give(self, *distances):
        for distance in distances:
            self.ring.start(self.pair(distance))

    def meet(self, distance):
        key = distance % self.ring.chips
        if key not in self.met:
            self.met.add(key)
            self.pair(distance).wait_recv()

    def place(self, way, step):
        ring = self.ring
        distance = (ring.far - (step + 1) // 2) * (1 if way == 0 else -1)
        return distance, pl.ds(ring.half_of(way, step) * self.half, self.half)

    def hop(self, way, step):
        ring = self.ring
        distance, piece = self.place(way, step)
        return ring.copy(
            self.partial.at[ring.slot(distance, ring.core), piece],
            self.inbox.at[way, step],
            self.send_sem.at[way, step],
            self.recv_sem.at[way, step],
            ring.next[way],
        )

    def both_cores(self, distance, piece):
        ring = self.ring
        return self.partial[ring.slot(distance, ring.core), piece, :].astype(f32) + self.other[
            ring.chip_at(distance), piece, :
        ].astype(f32)

    def advance(self, step):
        ring = self.ring
        for way in (0, 1):
            distance, piece = self.place(way, step)
            self.meet(distance)
            total = self.both_cores(distance, piece)
            if step >= 2:
                self.hop(way, step - 2).wait_recv()
                total = total + self.inbox[way, step - 2].astype(f32)
            self.partial[ring.slot(distance, ring.core), piece, :] = total.astype(bf16)
        for way in (0, 1):
            ring.start(self.hop(way, step))

    def own_half(self, which):
        ring = self.ring
        self.meet(0)
        total = self.both_cores(0, pl.ds(which * self.half, self.half))
        for way in (0, 1):
            step = ring.steps - 2 if ring.half_of(way, ring.steps - 2) == which else ring.steps - 1
            self.hop(way, step).wait_recv()
            total = total + self.inbox[way, step].astype(f32)
        return total


class Push:
    def __init__(self, axis, source, target, sems):
        self.axis, self.source, self.target = axis, source, target
        self.send, self.recv = sems
        self.count = target.shape[0]
        self.me = lax.axis_index(axis)
        self.copies = []

    def begin(self):
        for k in range(1, self.count):
            peer = lax.rem(self.me + k, self.count)
            copy = pltpu.make_async_remote_copy(
                src_ref=self.source(peer),
                dst_ref=self.target.at[self.me],
                send_sem=self.send.at[k],
                recv_sem=self.recv.at[k],
                device_id={self.axis: peer},
            )
            copy.start()
            self.copies.append(copy)
        self.target[self.me] = self.source(self.me)[...]

    def arrive(self):
        for copy in self.copies:
            copy.wait_recv()

    def leave(self):
        for copy in self.copies:
            copy.wait_send()


def meet_peers(axis, count, others):
    me = lax.axis_index(axis)
    barrier = pltpu.get_barrier_semaphore()
    for k in range(1, count):
        pl.semaphore_signal(barrier, inc=1, device_id={axis: lax.rem(me + k, count)})
    for name, peer in others:
        pl.semaphore_signal(barrier, inc=1, device_id={name: peer})
    return barrier, count - 1 + len(others)


def finish_blocks(place, got_ref, local_ref, readout_ref, prefix_ref, start_ref, gain_ref, mixed_ref):
    count = got_ref.shape[0]
    blocks = range(prefix_ref.shape[1])
    entry = [jnp.zeros((BLOCK, LANES), f32)] * 2
    for k in range(count - 1):
        for way in range(2):
            j = k if way == 0 else count - 1 - k
            passed = j < place if way == 0 else j > place
            moved = exact_right_dot(entry[way], both_heads(got_ref[j, :BLOCK, :]), NN)
            entry[way] = jnp.where(passed, moved + got_ref[j, BLOCK:, :].astype(f32), entry[way])
    gain = gain_ref[...].astype(f32)
    states = []
    for way in range(2):
        high, low = halves(entry[way])
        stacked = jnp.concatenate([high, low], axis=0)
        prefixes = [[both_heads(p) for p in halves(prefix_ref[way, b])] for b in blocks]
        boths = [raw_dot(stacked, p[0], NN) for p in prefixes]
        rests = [raw_dot(high, p[1], NN) for p in prefixes]
        states.append(
            [
                [both_heads(p) for p in halves(x[:BLOCK] + x[BLOCK:] + y + start_ref[way, b])]
                for x, y, b in zip(boths, rests, blocks)
            ]
        )
    places = [slice(b * BLOCK, (b + 1) * BLOCK) for b in blocks]
    mixes = []
    for b in blocks:
        state_high, state_low = [
            jnp.concatenate([states[0][b][k], states[1][b][k]], axis=1) for k in (0, 1)
        ]
        read_high, read_low = halves(readout_ref[places[b], :])
        both = raw_dot(jnp.concatenate([read_high, read_low], axis=0), state_high, NT)
        mixes.append(
            local_ref[places[b], :] + both[:BLOCK] + both[BLOCK:] + raw_dot(read_high, state_low, NT)
        )
    centers = [mix - head_sum(mix) * (1.0 / BLOCK) for mix in mixes]
    spreads = [head_sum(center * center) * (1.0 / BLOCK) for center in centers]
    for b in blocks:
        mixed_ref[places[b], :] = (centers[b] * lax.rsqrt(spreads[b] + GN_EPS) * gain).astype(bf16)


def layer_kernel(
    got_ref,
    local_ref,
    readout_ref,
    prefix_ref,
    start_ref,
    gain_ref,
    mix_weight_ref,
    input_ref,
    norm_gain_ref,
    placing_ref,
    weighting_ref,
    packing_ref,
    expert_gate,
    expert_up,
    expert_down,
    shared_gate,
    shared_up,
    shared_down,
    o_ref,
    mixed,
    residual,
    normed,
    outgoing,
    arrived,
    packed,
    unpacked,
    returned,
    shared_blocks,
    routed_blocks,
    mix_partial,
    shared_partial,
    routed_partial,
    mix_other,
    shared_other,
    routed_other,
    mix_inbox,
    shared_inbox,
    routed_inbox,
    gate,
    up,
    down,
    weight_sem,
    *sems,
    devices,
    sp_count,
):
    ring = Ring(TP, devices // 2)
    local_experts = expert_gate.shape[0]
    width = input_ref.shape[1]
    used = packing_ref.shape[0] // local_experts
    weight_copies = []
    for k, (pair, single, into) in enumerate(
        ((expert_gate, shared_gate, gate), (expert_up, shared_up, up), (expert_down, shared_down, down))
    ):
        weight_copies.append(
            pltpu.make_async_copy(pair, into.at[pl.ds(0, local_experts)], weight_sem.at[2 * k])
        )
        weight_copies.append(
            pltpu.make_async_copy(single, into.at[local_experts], weight_sem.at[2 * k + 1])
        )
    for copy in weight_copies:
        copy.start()
    barrier, expected = meet_peers(
        SP, sp_count, [(TP, ring.next[0]), (TP, ring.next[1]), (TP, ring.twin)]
    )

    finish_blocks(
        lax.axis_index(SP), got_ref, local_ref, readout_ref, prefix_ref, start_ref, gain_ref, mixed
    )
    columns = 512

    def project(k, _):
        at = pl.ds(pl.multiple_of(k * columns, columns), columns)
        product = raw_dot(mixed[...], mix_weight_ref[:, at], NN).astype(bf16)
        mix_partial[:, :, at] = product.reshape(mix_partial.shape[0], mix_partial.shape[1], columns)
        return 0

    lax.fori_loop(0, width // columns, project, 0)
    pl.semaphore_wait(barrier, expected)
    mix_sum = Sum(ring, mix_partial, mix_other, mix_inbox, sems[0:4])
    mix_sum.give(ring.far, ring.far - 1, 1 - ring.far, *range(ring.far - 2, 1 - ring.far, -1))
    for step in range(ring.steps):
        mix_sum.advance(step)
    half = residual.shape[0] // 2
    for which in (0, 1):
        piece = slice(which * half, (which + 1) * half)
        rows = input_ref[piece, :].astype(f32) + mix_sum.own_half(which)
        residual[piece, :] = rows
        scale = lax.rsqrt(jnp.mean(rows * rows, axis=-1, keepdims=True) + RMS_EPS)
        normed[piece, :] = (rows * scale * norm_gain_ref[...].astype(f32)).astype(bf16)

    shared_in = Gather(ring, normed, shared_blocks, sems[4:8])
    outgoing[...] = (
        raw_dot(placing_ref[...], normed[...], TN).astype(bf16).reshape(outgoing.shape)
    )
    shared_in.begin()
    dispatch = Push(SP, lambda peer: outgoing.at[peer], arrived, sems[8:10])
    dispatch.begin()
    for step in range(ring.steps - 1):
        shared_in.advance(step)
    dispatch.arrive()
    packed[...] = raw_dot(
        packing_ref[...], arrived[...].reshape(packing_ref.shape[1], width), NN
    ).astype(bf16)
    routed_in = Gather(ring, packed, routed_blocks, sems[10:14])
    routed_in.begin()
    shared_in.advance(ring.steps - 1)

    def expert_on(blocks, partial, first, count, at, which):
        rows = at.size
        x = blocks[pl.ds(first, count), at, :].reshape(count * rows, width)
        gated = raw_dot(x, gate[which], NN)
        lifted = raw_dot(x, up[which], NN)
        inner = (gated / (1.0 + jnp.exp(-gated)) * lifted).astype(bf16)
        partial[pl.ds(first, count), at, :] = (
            raw_dot(inner, down[which], NN).astype(bf16).reshape(count, rows, width)
        )

    def routed_on(distance):
        first = ring.chip_at(distance) * 2

        def one(k, _):
            at = pl.ds(pl.multiple_of(k * used, 16), used)
            expert_on(routed_blocks, routed_partial, first, 2, at, k)
            return 0

        lax.fori_loop(0, local_experts, one, 0)

    def shared_on(quarter):
        count = devices // 4
        at = pl.ds(0, normed.shape[0])
        expert_on(shared_blocks, shared_partial, quarter * count, count, at, local_experts)

    routed_sum = Sum(ring, routed_partial, routed_other, routed_inbox, sems[14:18])
    shared_sum = Sum(ring, shared_partial, shared_other, shared_inbox, sems[18:22])
    for copy in weight_copies:
        copy.wait()
    shared_in.hand_own().wait_recv()
    shared_in.handed(*range(ring.steps))

    def quarters(first):
        def one(k, _):
            shared_on(first + k)
            return 0

        lax.fori_loop(0, 2, one, 0)

    quarters(0)
    for step in range(ring.steps):
        routed_in.advance(step)
        if step == 0:
            quarters(2)
        elif step % 2 == 1:
            distance = (step + 1) // 2
            routed_in.handed(step - 1, step)

            def both(k, _):
                routed_on(distance * (2 * k - 1))
                return 0

            lax.fori_loop(0, 2, both, 0)
        elif step == 2:
            routed_in.hand_own().wait_recv()
            routed_on(0)
            routed_sum.give(-1, 1)
        elif step == 4:
            routed_sum.give(0, -2, 2)
        elif step == 6:
            routed_sum.give(-3, 3)
    routed_in.handed(ring.steps - 1)
    routed_on(ring.far)
    routed_sum.give(ring.far)
    shared_sum.give(ring.far, ring.far - 1, 1 - ring.far, *range(ring.far - 2, 1 - ring.far, -1))
    for step in range(ring.steps):
        routed_sum.advance(step)
    shared_sum.advance(0)
    shared_sum.advance(1)
    summed = jnp.concatenate([routed_sum.own_half(which).astype(bf16) for which in (0, 1)], axis=0)
    unpacked[...] = raw_dot(packing_ref[...], summed, TN).astype(bf16).reshape(unpacked.shape)
    back = Push(SP, lambda peer: unpacked.at[peer], returned, sems[22:24])
    back.begin()
    for step in range(2, ring.steps):
        shared_sum.advance(step)
    half = residual.shape[0] // 2
    for which in (0, 1):
        piece = slice(which * half, (which + 1) * half)
        residual[piece, :] = residual[piece, :] + shared_sum.own_half(which)
    back.arrive()
    rows = returned[...].reshape(weighting_ref.shape[1], width)
    routed = exact_right_dot(weighting_ref[...], rows, NN)
    o_ref[...] = (residual[...] + routed).astype(bf16)
    for copy in ring.sent:
        copy.wait_send()
    dispatch.leave()
    back.leave()


def layer(arrays, weights, devices, sp_count, room, number, name):
    got, local, readout, prefix, start, gain, mix_weight, layer_input, norm_gain = arrays[:9]
    placing, weighting, packing = arrays[9:]
    rows, width = layer_input.shape
    hidden = weights[3].shape[1]
    local_experts = weights[0].shape[0]
    packed_rows = packing.shape[0]
    chips = devices // 2
    steps = chips - 1
    dma = pltpu.SemaphoreType.DMA
    anywhere = pl.BlockSpec(memory_space=pl.ANY)
    buffer = lambda *shape: pltpu.VMEM(shape, bf16)
    gather_sems = [dma((2, steps)), dma((2, steps)), dma((2, steps + 1)), dma((2, steps + 1))]
    sum_sems = [dma((chips,)), dma((chips,)), dma((2, steps)), dma((2, steps))]
    push_sems = [dma((sp_count,)), dma((sp_count,))]
    return pl.pallas_call(
        functools.partial(layer_kernel, devices=devices, sp_count=sp_count),
        name=name,
        out_shape=jax.ShapeDtypeStruct((rows, width), bf16),
        in_specs=[VMEM] * 12 + [anywhere] * 6,
        out_specs=VMEM,
        scratch_shapes=[
            buffer(*local.shape),
            pltpu.VMEM((rows, width), f32),
            buffer(rows, width),
            buffer(sp_count, room, width),
            buffer(sp_count, room, width),
            buffer(packed_rows, width),
            buffer(sp_count, room, width),
            buffer(sp_count, room, width),
            buffer(devices, rows, width),
            buffer(devices, packed_rows, width),
            buffer(devices, rows, width),
            buffer(devices, rows, width),
            buffer(devices, packed_rows, width),
            buffer(chips, rows, width),
            buffer(chips, rows, width),
            buffer(chips, packed_rows, width),
            buffer(2, steps, rows // 2, width),
            buffer(2, steps, rows // 2, width),
            buffer(2, steps, packed_rows // 2, width),
            buffer(local_experts + 1, width, hidden),
            buffer(local_experts + 1, width, hidden),
            buffer(local_experts + 1, hidden, width),
            dma((6,)),
        ]
        + sum_sems
        + gather_sems
        + push_sems
        + gather_sems
        + sum_sems
        + sum_sems
        + push_sems,
        compiler_params=pltpu.CompilerParams(
            collective_id=number, has_side_effects=True, vmem_limit_bytes=62 * 1024 * 1024
        ),
    )(*arrays, *weights)


def body(
    layer_input,
    receptance,
    keys,
    values,
    erase_preact,
    decay_preact,
    decay_spike,
    head_norm_gain,
    output_weight,
    expert_norm_gain,
    routes,
    routing_weight,
    expert_gate_weight,
    expert_up_weight,
    expert_down_weight,
    shared_gate_weight,
    shared_up_weight,
    shared_down_weight,
):
    sp_count, tp_count = lax.axis_size(SP), lax.axis_size(TP)
    local, readout, prefix, start, got = mixer_terms(
        receptance, keys, values, erase_preact, decay_preact, decay_spike, sp_count, 0
    )
    row_count = layer_input.shape[0]
    top_count = routes.shape[1]
    expert_local = expert_gate_weight.shape[0]
    capacity = 3
    room = 8
    slot_total = sp_count * room
    entries = routes.reshape(-1)
    entry_count = entries.shape[0]
    expert_hot = (entries[:, None] == jnp.arange(expert_local * sp_count)[None, :]).astype(jnp.int32)
    rank_in = jnp.sum((jnp.cumsum(expert_hot, axis=0) - 1) * expert_hot, axis=1)
    slot_of = entries // expert_local * room + entries % expert_local * capacity + rank_in
    slot_hot = slot_of[:, None] == jnp.arange(slot_total)[None, :]
    placing = jnp.sum(
        slot_hot.reshape(row_count, top_count, slot_total).astype(f32), axis=1
    ).astype(bf16)
    weighting = jnp.sum(
        jnp.where(slot_hot, routing_weight.reshape(-1, 1), 0.0).reshape(
            row_count, top_count, slot_total
        ),
        axis=1,
    )
    used = sp_count * capacity
    packed_row = jnp.arange(expert_local * used)
    from_slot = (
        packed_row % used // capacity * room
        + packed_row // used * capacity
        + packed_row % capacity
    )
    packing = (from_slot[:, None] == jnp.arange(slot_total)[None, :]).astype(bf16)
    return layer(
        (
            got,
            local,
            readout,
            prefix,
            start,
            head_norm_gain.reshape(1, -1),
            output_weight,
            layer_input,
            expert_norm_gain.reshape(1, -1),
            placing,
            weighting,
            packing,
        ),
        (
            expert_gate_weight,
            expert_up_weight,
            expert_down_weight,
            shared_gate_weight,
            shared_up_weight,
            shared_down_weight,
        ),
        tp_count,
        sp_count,
        room,
        1,
        "layer",
    )


def solution(mesh):
    both = (SP, TP)
    in_specs = (
        P(both, None),
        P(SP, TP),
        P(SP, TP),
        P(SP, TP),
        P(SP, TP),
        P(SP, TP),
        P(SP, TP),
        P(TP),
        P(TP, None),
        P(),
        P(both, None),
        P(both, None),
        P(SP, None, TP),
        P(SP, None, TP),
        P(SP, TP, None),
        P(None, TP),
        P(None, TP),
        P(TP, None),
    )
    return jax.shard_map(
        body, mesh=mesh, in_specs=in_specs, out_specs=P(both, None), check_vma=False
    )
```

```python
import functools

import jax
import jax.numpy as jnp
from jax import lax
from jax.experimental import pallas as pl
from jax.experimental.pallas import tpu as pltpu
from jax.sharding import PartitionSpec as P

SP = "sp"
TP = "tp"
BLOCK = 64
LANES = 128
GN_EPS = 0.00064
RMS_EPS = 1e-06
f32 = jnp.float32
bf16 = jnp.bfloat16
VMEM = pl.BlockSpec(memory_space=pltpu.VMEM)
NN = (((1,), (0,)), ((), ()))
NT = (((1,), (1,)), ((), ()))
TN = (((0,), (0,)), ((), ()))


def iota(shape, dim):
    return lax.broadcasted_iota(jnp.int32, shape, dim)


def halves(array):
    high = array.astype(bf16)
    return high, (array - high.astype(f32)).astype(bf16)


def raw_dot(left, right, dims):
    return lax.dot_general(left, right, dims, preferred_element_type=f32)


def head_mask(count, dtype):
    first = (iota((count, LANES), 1) < BLOCK).astype(f32)
    return first.astype(dtype), (1.0 - first).astype(dtype)


def both_heads(rows):
    first, second = head_mask(rows.shape[0], rows.dtype)
    return jnp.concatenate([rows * first, rows * second], axis=0)


def fine_dot(left, right, dims, spread=False):
    left_high, left_low = halves(left)
    right_high, right_low = halves(right)
    if spread:
        right_high, right_low = both_heads(right_high), both_heads(right_low)
    if dims == TN:
        return raw_dot(
            jnp.concatenate([left_high, left_high, left_low], axis=0),
            jnp.concatenate([right_high, right_low, right_high], axis=0),
            TN,
        )
    count = left.shape[0]
    both = raw_dot(jnp.concatenate([left_high, left_low], axis=0), right_high, dims)
    return both[:count] + both[count:] + raw_dot(left_high, right_low, dims)


def exact_right_dot(left, right, dims):
    left_high, left_low = halves(left)
    count = left.shape[0]
    both = raw_dot(jnp.concatenate([left_high, left_low], axis=0), right, dims)
    return both[:count] + both[count:]


def head_sum(rows):
    ones = (iota((LANES, LANES), 0) // BLOCK == iota((LANES, LANES), 1) // BLOCK).astype(bf16)
    return exact_right_dot(rows, ones, NN)


def block_sums(log_decay):
    high, middle, low = three_parts(log_decay)
    count = log_decay.shape[0]
    ones = (iota((count, count), 0) >= iota((count, count), 1)).astype(bf16)
    width = log_decay.shape[1]
    sums = raw_dot(ones, jnp.concatenate([high, middle, low], axis=1), NN)
    return sums[:, :width] + sums[:, width : 2 * width] + sums[:, 2 * width :]


def inverses(stricts):
    row, lane = iota((BLOCK, LANES), 0), iota((BLOCK, LANES), 1) % BLOCK

    def within(size):
        return row // size == lane // size

    def products(lefts, rights):
        return [fine_dot(left, right, NN, spread=True) for left, right in zip(lefts, rights)]

    smalls = [jnp.where(within(8), strict, 0.0) for strict in stricts]
    starts = [jnp.where(row == lane, 1.0, 0.0) - small for small in smalls]
    squares = products(smalls, smalls)
    boths = products([jnp.concatenate(p, axis=0) for p in zip(starts, squares)], squares)
    results = [start + both[:BLOCK] for start, both in zip(starts, boths)]
    more = products(results, [both[BLOCK:] for both in boths])
    results = [r + m for r, m in zip(results, more)]
    for size in (8, 16, 32):
        keep = within(2 * size) & ~within(size)
        edges = products(results, [jnp.where(keep, strict, 0.0) for strict in stricts])
        more = products(edges, results)
        results = [r - m for r, m in zip(results, more)]
    return results


def block_terms(chains):
    row, lane = iota((BLOCK, LANES), 0), iota((BLOCK, LANES), 1) % BLOCK
    scaled, pairs = [], []
    for unit, beta, key_rows, _, read, left_unit, left_read, right, _, _ in chains:
        scaled.append((unit * left_unit, read * left_read, beta * right, key_rows * right))
    for unit_mid, read_mid, beta_mid, key_mid in scaled:
        left_high, left_low = halves(jnp.concatenate([unit_mid, read_mid], axis=0))
        right_high, right_low = [
            jnp.concatenate([both_heads(b), both_heads(k)], axis=0)
            for b, k in zip(halves(beta_mid), halves(key_mid))
        ]
        both = raw_dot(jnp.concatenate([left_high, left_low], axis=0), right_high, NT)
        pairs.append(both[: 2 * BLOCK] + both[2 * BLOCK :] + raw_dot(left_high, right_low, NT))
    erase_betas, keyeds, read_betas = [], [], []
    for pair, chain in zip(pairs, chains):
        strict = row > lane if chain[-1] else row < lane
        upto = row >= lane if chain[-1] else row <= lane
        erase_betas.append(jnp.where(strict, pair[:BLOCK, :LANES], 0.0))
        erase_key = jnp.where(strict, pair[:BLOCK, LANES:], 0.0)
        read_betas.append(jnp.where(upto, pair[BLOCK:, :LANES], 0.0))
        read_key = jnp.where(upto, pair[BLOCK:, LANES:], 0.0)
        keyeds.append(
            exact_right_dot(jnp.concatenate([erase_key, read_key], axis=0), chain[3], NN)
        )
    solvers = inverses(erase_betas)
    solved = []
    for solver, (unit_mid, _, _, _), keyed, chain in zip(solvers, scaled, keyeds, chains):
        solver_high, solver_low = halves(solver)
        right_high, right_low = [
            jnp.concatenate([both_heads(u), both_heads(k)], axis=1)
            for u, k in zip(halves(unit_mid * chain[8]), halves(-keyed[:BLOCK]))
        ]
        both = raw_dot(jnp.concatenate([solver_high, solver_low], axis=0), right_high, NN)
        solved.append(both[:BLOCK] + both[BLOCK:] + raw_dot(solver_high, right_low, NN))
    terms = []
    for found, read_beta, keyed, scale, chain in zip(solved, read_betas, keyeds, scaled, chains):
        spread_parts = [
            jnp.concatenate([both_heads(p[:, :LANES]), both_heads(p[:, LANES:])], axis=1)
            for p in halves(found)
        ]
        read_high, read_low = halves(read_beta)
        both = raw_dot(jnp.concatenate([read_high, read_low], axis=0), spread_parts[0], NN)
        applied = both[:BLOCK] + both[BLOCK:] + raw_dot(read_high, spread_parts[1], NN)
        readout = scale[1] * chain[8] - applied[:, :LANES]
        local = applied[:, LANES:] + keyed[BLOCK:]
        terms.append((found, scale[2] * chain[8], scale[3] * chain[8], readout, local))
    return terms


def three_parts(array):
    high = array.astype(bf16)
    rest = array - high.astype(f32)
    middle = rest.astype(bf16)
    return high, middle, (rest - middle.astype(f32)).astype(bf16)


def to_columns(rows, pick):
    chosen = [(pick == k).astype(bf16) for k in range(2)]
    parts = three_parts(rows)
    return raw_dot(
        jnp.concatenate(parts, axis=0), jnp.concatenate([jnp.concatenate(chosen, axis=0)] * 3, axis=0), TN
    )


def mixer_stage(
    read_ref,
    key_ref,
    value_ref,
    erase_ref,
    decay_ref,
    spike_ref,
    local_ref,
    readout_ref,
    prefix_ref,
    start_ref,
    move_ref,
    carry_ref,
    whole_ref,
    together,
):
    tokens = key_ref.shape[0]
    block_count = tokens // BLOCK
    same_head = iota((LANES, LANES), 0) // BLOCK == iota((LANES, LANES), 1) // BLOCK
    diagonal = iota((LANES, LANES), 0) == iota((LANES, LANES), 1)

    def some_blocks(index):
        blocks = [index * together + k for k in range(together)]
        span = together * BLOCK
        spikes = to_columns(
            spike_ref[:, pl.ds(pl.multiple_of(index * span, span), span)],
            iota((1, LANES), 1) // BLOCK,
        )
        chains, totals, values = [], [], []
        places = [pl.ds(pl.multiple_of(block * BLOCK, BLOCK), BLOCK) for block in blocks]
        for k, at in enumerate(places):
            key_rows = key_ref[at, :].astype(f32)
            read = read_ref[at, :].astype(f32)
            value = value_ref[at, :]
            unit = key_rows * lax.rsqrt(head_sum(key_rows * key_rows) + 1e-06)
            beta = unit * jax.nn.sigmoid(erase_ref[at, :].astype(f32))
            decay_in = decay_ref[at, :].astype(f32)
            spike = spikes[k * BLOCK : (k + 1) * BLOCK]
            log_decay = -jnp.exp(-jax.nn.softplus(-decay_in) - 0.5) + spike
            upto = block_sums(log_decay)
            total = upto[BLOCK - 1 :, :]
            middle = 0.5 * total
            ahead = upto - log_decay
            before, after = jnp.exp(ahead - middle), jnp.exp(upto - middle)
            until, since = jnp.exp(middle - upto), jnp.exp(middle - ahead)
            edge = jnp.exp(middle)
            shared = (unit, beta, key_rows, both_heads(value), read)
            chains.append(shared + (before, after, until, edge, True))
            chains.append(shared + (until, since, before, edge, False))
            totals.append(total)
            values.append(value)
        terms = block_terms(chains)
        for k, at in enumerate(places):
            local_ref[at, :] = terms[2 * k][4] + terms[2 * k + 1][4]
        for k, (solved, beta_end, key_end, readout, _) in enumerate(terms):
            way, at, value = k % 2, places[k // 2], values[k // 2]
            readout_ref[at, way * LANES : (way + 1) * LANES] = readout
            moved = fine_dot(solved, beta_end, TN)
            key_high, key_low = halves(key_end)
            keyed = raw_dot(
                jnp.concatenate([value, value], axis=0),
                jnp.concatenate([key_high, key_low], axis=0),
                TN,
            )
            move_ref[way, blocks[k // 2]] = jnp.where(
                same_head, jnp.where(diagonal, jnp.exp(totals[k // 2]), 0.0) - moved[:LANES], 0.0
            )
            carry = jnp.where(same_head, moved[LANES:] + keyed, 0.0)
            carry_ref[way, blocks[k // 2]] = carry[:BLOCK] + carry[BLOCK:]

    def step(index, _):
        some_blocks(index)
        return 0

    lax.fori_loop(0, block_count // together, step, 0)
    identity = jnp.where(iota((BLOCK, LANES), 0) == iota((BLOCK, LANES), 1) % BLOCK, 1.0, 0.0)
    running = [jnp.concatenate([identity, jnp.zeros_like(identity)], axis=0)] * 2
    for k in range(block_count):
        for way in range(2):
            block = k if way == 0 else block_count - 1 - k
            now = running[way]
            prefix_ref[way, block] = now[:BLOCK]
            start_ref[way, block] = now[BLOCK:]
            after = fine_dot(now, move_ref[way, block], NN)
            running[way] = jnp.concatenate(
                [after[:BLOCK], after[BLOCK:] + carry_ref[way, block]], axis=0
            )
    for way in range(2):
        whole_ref[way] = running[way].astype(bf16)


class Ring:
    def __init__(self, axis, chips):
        self.axis, self.chips = axis, chips
        self.me = lax.axis_index(axis)
        self.chip, self.core = self.me // 2, lax.rem(self.me, 2)
        self.steps = chips - 1
        self.far = chips // 2
        self.next = (self.slot(1, self.core), self.slot(-1, self.core))
        self.twin = self.chip * 2 + 1 - self.core
        self.sent = []

    def chip_at(self, distance):
        return lax.rem(self.chip + distance + self.chips, self.chips)

    def slot(self, distance, which):
        return self.chip_at(distance) * 2 + which

    def copy(self, source, target, send, recv, peer):
        return pltpu.make_async_remote_copy(
            src_ref=source, dst_ref=target, send_sem=send, recv_sem=recv, device_id={self.axis: peer}
        )

    def start(self, copy):
        copy.start()
        self.sent.append(copy)

    def half_of(self, way, step):
        return step % 2 if way == 0 else 1 - step % 2


class Gather:
    def __init__(self, ring, own, blocks, sems):
        self.ring, self.own, self.blocks = ring, own, blocks
        self.send, self.recv, self.pass_send, self.pass_recv = sems
        self.half = own.shape[0] // 2

    def piece(self, way, step):
        return pl.ds(self.ring.half_of(way, step) * self.half, self.half)

    def hop(self, way, step):
        ring, piece = self.ring, self.piece(way, step)
        at = ring.slot((step // 2) * (-1 if way == 0 else 1), ring.core)
        source = self.own.at[piece] if step < 2 else self.blocks.at[at, piece]
        return ring.copy(
            source,
            self.blocks.at[at, piece],
            self.send.at[way, step],
            self.recv.at[way, step],
            ring.next[way],
        )

    def hand(self, way, step):
        ring, piece = self.ring, self.piece(way, step)
        at = ring.slot((step // 2 + 1) * (-1 if way == 0 else 1), ring.core)
        return ring.copy(
            self.blocks.at[at, piece],
            self.blocks.at[at, piece],
            self.pass_send.at[way, step],
            self.pass_recv.at[way, step],
            ring.twin,
        )

    def hand_own(self):
        ring = self.ring
        return ring.copy(
            self.own,
            self.blocks.at[ring.me],
            self.pass_send.at[0, ring.steps],
            self.pass_recv.at[0, ring.steps],
            ring.twin,
        )

    def begin(self):
        for step in (0, 1):
            for way in (0, 1):
                self.ring.start(self.hop(way, step))
        self.ring.start(self.hand_own())
        self.blocks[self.ring.me] = self.own[...]

    def advance(self, step):
        for way in (0, 1):
            self.hop(way, step).wait_recv()
            if step + 2 < self.ring.steps:
                self.ring.start(self.hop(way, step + 2))
            self.ring.start(self.hand(way, step))

    def handed(self, *steps):
        for step in steps:
            for way in (0, 1):
                self.hand(way, step).wait_recv()


class Sum:
    def __init__(self, ring, partial, other, inbox, sems):
        self.ring, self.partial, self.other, self.inbox = ring, partial, other, inbox
        self.pair_send, self.pair_recv, self.send_sem, self.recv_sem = sems
        self.half = partial.shape[1] // 2
        self.met = set()

    def pair(self, distance):
        ring = self.ring
        index = ring.chip_at(distance)
        return ring.copy(
            self.partial.at[ring.slot(distance, 1 - ring.core)],
            self.other.at[index],
            self.pair_send.at[index],
            self.pair_recv.at[index],
            ring.twin,
        )

    def give(self, *distances):
        for distance in distances:
            self.ring.start(self.pair(distance))

    def meet(self, distance):
        key = distance % self.ring.chips
        if key not in self.met:
            self.met.add(key)
            self.pair(distance).wait_recv()

    def place(self, way, step):
        ring = self.ring
        distance = (ring.far - (step + 1) // 2) * (1 if way == 0 else -1)
        return distance, pl.ds(ring.half_of(way, step) * self.half, self.half)

    def hop(self, way, step):
        ring = self.ring
        distance, piece = self.place(way, step)
        return ring.copy(
            self.partial.at[ring.slot(distance, ring.core), piece],
            self.inbox.at[way, step],
            self.send_sem.at[way, step],
            self.recv_sem.at[way, step],
            ring.next[way],
        )

    def both_cores(self, distance, piece):
        ring = self.ring
        return self.partial[ring.slot(distance, ring.core), piece, :].astype(f32) + self.other[
            ring.chip_at(distance), piece, :
        ].astype(f32)

    def advance(self, step):
        ring = self.ring
        for way in (0, 1):
            distance, piece = self.place(way, step)
            self.meet(distance)
            total = self.both_cores(distance, piece)
            if step >= 2:
                self.hop(way, step - 2).wait_recv()
                total = total + self.inbox[way, step - 2].astype(f32)
            self.partial[ring.slot(distance, ring.core), piece, :] = total.astype(bf16)
        for way in (0, 1):
            ring.start(self.hop(way, step))

    def own_half(self, which):
        ring = self.ring
        self.meet(0)
        total = self.both_cores(0, pl.ds(which * self.half, self.half))
        for way in (0, 1):
            step = ring.steps - 2 if ring.half_of(way, ring.steps - 2) == which else ring.steps - 1
            self.hop(way, step).wait_recv()
            total = total + self.inbox[way, step].astype(f32)
        return total


class Push:
    def __init__(self, axis, source, target, sems):
        self.axis, self.source, self.target = axis, source, target
        self.send, self.recv = sems
        self.count = target.shape[0]
        self.me = lax.axis_index(axis)
        self.copies = []

    def begin(self):
        for k in range(1, self.count):
            peer = lax.rem(self.me + k, self.count)
            copy = pltpu.make_async_remote_copy(
                src_ref=self.source(peer),
                dst_ref=self.target.at[self.me],
                send_sem=self.send.at[k],
                recv_sem=self.recv.at[k],
                device_id={self.axis: peer},
            )
            copy.start()
            self.copies.append(copy)
        self.target[self.me] = self.source(self.me)[...]

    def arrive(self):
        for copy in self.copies:
            copy.wait_recv()

    def leave(self):
        for copy in self.copies:
            copy.wait_send()


def meet_peers(axis, count, others):
    me = lax.axis_index(axis)
    barrier = pltpu.get_barrier_semaphore()
    for k in range(1, count):
        pl.semaphore_signal(barrier, inc=1, device_id={axis: lax.rem(me + k, count)})
    for name, peer in others:
        pl.semaphore_signal(barrier, inc=1, device_id={name: peer})
    return barrier, count - 1 + len(others)


def finish_blocks(place, got_ref, local_ref, readout_ref, prefix_ref, start_ref, gain_ref, mixed_ref):
    count = got_ref.shape[0]
    blocks = range(prefix_ref.shape[1])
    entry = [jnp.zeros((BLOCK, LANES), f32)] * 2
    for k in range(count - 1):
        for way in range(2):
            j = k if way == 0 else count - 1 - k
            passed = j < place if way == 0 else j > place
            moved = exact_right_dot(entry[way], both_heads(got_ref[j, :BLOCK, :]), NN)
            entry[way] = jnp.where(passed, moved + got_ref[j, BLOCK:, :].astype(f32), entry[way])
    gain = gain_ref[...].astype(f32)
    states = []
    for way in range(2):
        high, low = halves(entry[way])
        stacked = jnp.concatenate([high, low], axis=0)
        prefixes = [[both_heads(p) for p in halves(prefix_ref[way, b])] for b in blocks]
        boths = [raw_dot(stacked, p[0], NN) for p in prefixes]
        rests = [raw_dot(high, p[1], NN) for p in prefixes]
        states.append(
            [
                [both_heads(p) for p in halves(x[:BLOCK] + x[BLOCK:] + y + start_ref[way, b])]
                for x, y, b in zip(boths, rests, blocks)
            ]
        )
    places = [slice(b * BLOCK, (b + 1) * BLOCK) for b in blocks]
    mixes = []
    for b in blocks:
        state_high, state_low = [
            jnp.concatenate([states[0][b][k], states[1][b][k]], axis=1) for k in (0, 1)
        ]
        read_high, read_low = halves(readout_ref[places[b], :])
        both = raw_dot(jnp.concatenate([read_high, read_low], axis=0), state_high, NT)
        mixes.append(
            local_ref[places[b], :] + both[:BLOCK] + both[BLOCK:] + raw_dot(read_high, state_low, NT)
        )
    centers = [mix - head_sum(mix) * (1.0 / BLOCK) for mix in mixes]
    spreads = [head_sum(center * center) * (1.0 / BLOCK) for center in centers]
    for b in blocks:
        mixed_ref[places[b], :] = (centers[b] * lax.rsqrt(spreads[b] + GN_EPS) * gain).astype(bf16)


def routing(routes_ref, weights_ref, room, capacity):
    rows = routes_ref.shape[1]
    slot = iota((rows, LANES), 1)
    within = slot % room
    second = (within >= capacity).astype(jnp.int32)
    rank = within - second * capacity
    in_use = within < 2 * capacity
    expert = (slot // room * 2 + second).astype(f32)
    named = []
    for k in range(2):
        pick = jnp.full((1, LANES), k, jnp.int32)
        named.append(
            (
                jnp.where((to_columns(routes_ref[...].astype(f32), pick) == expert) & in_use, 1.0, 0.0),
                to_columns(weights_ref[...], pick),
            )
        )
    either = named[0][0] + named[1][0]
    before = (iota((rows, rows), 0) > iota((rows, rows), 1)).astype(bf16)
    taken = raw_dot(before, either.astype(bf16), NN)
    here = jnp.where(taken == rank.astype(f32), 1.0, 0.0)
    placing = (either * here).astype(bf16)
    weighting = (named[0][0] * named[0][1] + named[1][0] * named[1][1]) * here
    per_expert = LANES // room * capacity
    shape = (2 * per_expert, LANES)
    slot = iota(shape, 1)
    within = slot % room
    second = (within >= capacity).astype(jnp.int32)
    target = second * per_expert + slot // room * capacity + within - second * capacity
    packing = jnp.where((iota(shape, 0) == target) & (within < 2 * capacity), 1.0, 0.0).astype(bf16)
    return placing, weighting, packing


def layer_kernel(
    read_ref,
    key_ref,
    value_ref,
    erase_ref,
    decay_ref,
    spike_ref,
    gain_ref,
    mix_weight_ref,
    input_ref,
    norm_gain_ref,
    routes_ref,
    route_weights_ref,
    expert_gate,
    expert_up,
    expert_down,
    shared_gate,
    shared_up,
    shared_down,
    o_ref,
    local_ref,
    readout_ref,
    prefix_ref,
    start_ref,
    move_ref,
    carry_ref,
    whole_ref,
    got_ref,
    mixed,
    residual,
    normed,
    outgoing,
    arrived,
    packed,
    unpacked,
    returned,
    shared_blocks,
    routed_blocks,
    mix_partial,
    shared_partial,
    routed_partial,
    mix_other,
    shared_other,
    routed_other,
    mix_inbox,
    shared_inbox,
    routed_inbox,
    gate,
    up,
    down,
    weight_sem,
    *sems,
    devices,
    sp_count,
):
    ring = Ring(TP, devices // 2)
    local_experts = expert_gate.shape[0]
    width = input_ref.shape[1]
    capacity, room = 3, outgoing.shape[1]
    used = packed.shape[0] // local_experts
    weight_copies = []
    for k, (pair, single, into) in enumerate(
        ((expert_gate, shared_gate, gate), (expert_up, shared_up, up), (expert_down, shared_down, down))
    ):
        weight_copies.append(
            pltpu.make_async_copy(pair, into.at[pl.ds(0, local_experts)], weight_sem.at[2 * k])
        )
        weight_copies.append(
            pltpu.make_async_copy(single, into.at[local_experts], weight_sem.at[2 * k + 1])
        )
    for copy in weight_copies:
        copy.start()
    barrier, expected = meet_peers(
        SP, sp_count, [(TP, ring.next[0]), (TP, ring.next[1]), (TP, ring.twin)]
    )

    placing, weighting, packing = routing(routes_ref, route_weights_ref, room, capacity)
    mixer_stage(
        read_ref,
        key_ref,
        value_ref,
        erase_ref,
        decay_ref,
        spike_ref,
        local_ref,
        readout_ref,
        prefix_ref,
        start_ref,
        move_ref,
        carry_ref,
        whole_ref,
        4,
    )
    pl.semaphore_wait(barrier, expected)
    here = lax.axis_index(SP)
    states = Push(
        SP,
        lambda peer: whole_ref.at[(here + sp_count - peer) // (sp_count + 1)],
        got_ref,
        sems[24:26],
    )
    states.begin()
    states.arrive()

    finish_blocks(
        lax.axis_index(SP), got_ref, local_ref, readout_ref, prefix_ref, start_ref, gain_ref, mixed
    )
    columns = 512

    def project(k, _):
        at = pl.ds(pl.multiple_of(k * columns, columns), columns)
        product = raw_dot(mixed[...], mix_weight_ref[:, at], NN).astype(bf16)
        mix_partial[:, :, at] = product.reshape(mix_partial.shape[0], mix_partial.shape[1], columns)
        return 0

    lax.fori_loop(0, width // columns, project, 0)
    mix_sum = Sum(ring, mix_partial, mix_other, mix_inbox, sems[0:4])
    mix_sum.give(ring.far, ring.far - 1, 1 - ring.far, *range(ring.far - 2, 1 - ring.far, -1))
    for step in range(ring.steps):
        mix_sum.advance(step)
    gains = norm_gain_ref[...].astype(f32)
    norm_gain = jnp.concatenate([gains[k : k + 1] for k in range(gains.shape[0])], axis=1)
    half = residual.shape[0] // 2
    for which in (0, 1):
        piece = slice(which * half, (which + 1) * half)
        rows = input_ref[piece, :].astype(f32) + mix_sum.own_half(which)
        residual[piece, :] = rows
        scale = lax.rsqrt(jnp.mean(rows * rows, axis=-1, keepdims=True) + RMS_EPS)
        normed[piece, :] = (rows * scale * norm_gain).astype(bf16)

    shared_in = Gather(ring, normed, shared_blocks, sems[4:8])
    outgoing[...] = (
        raw_dot(placing, normed[...], TN).astype(bf16).reshape(outgoing.shape)
    )
    shared_in.begin()
    dispatch = Push(SP, lambda peer: outgoing.at[peer], arrived, sems[8:10])
    dispatch.begin()
    for step in range(ring.steps - 1):
        shared_in.advance(step)
    dispatch.arrive()
    packed[...] = raw_dot(
        packing, arrived[...].reshape(packing.shape[1], width), NN
    ).astype(bf16)
    routed_in = Gather(ring, packed, routed_blocks, sems[10:14])
    routed_in.begin()
    shared_in.advance(ring.steps - 1)

    def expert_on(blocks, partial, first, count, at, which):
        rows = at.size
        x = blocks[pl.ds(first, count), at, :].reshape(count * rows, width)
        gated = raw_dot(x, gate[which], NN)
        lifted = raw_dot(x, up[which], NN)
        inner = (gated / (1.0 + jnp.exp(-gated)) * lifted).astype(bf16)
        partial[pl.ds(first, count), at, :] = (
            raw_dot(inner, down[which], NN).astype(bf16).reshape(count, rows, width)
        )

    def routed_on(distance):
        first = ring.chip_at(distance) * 2

        def one(k, _):
            at = pl.ds(pl.multiple_of(k * used, 16), used)
            expert_on(routed_blocks, routed_partial, first, 2, at, k)
            return 0

        lax.fori_loop(0, local_experts, one, 0)

    def shared_on(quarter):
        count = devices // 4
        at = pl.ds(0, normed.shape[0])
        expert_on(shared_blocks, shared_partial, quarter * count, count, at, local_experts)

    routed_sum = Sum(ring, routed_partial, routed_other, routed_inbox, sems[14:18])
    shared_sum = Sum(ring, shared_partial, shared_other, shared_inbox, sems[18:22])
    for copy in weight_copies:
        copy.wait()
    shared_in.hand_own().wait_recv()
    shared_in.handed(*range(ring.steps))

    def quarters(first):
        def one(k, _):
            shared_on(first + k)
            return 0

        lax.fori_loop(0, 2, one, 0)

    quarters(0)
    for step in range(ring.steps):
        routed_in.advance(step)
        if step == 0:
            quarters(2)
        elif step % 2 == 1:
            distance = (step + 1) // 2
            routed_in.handed(step - 1, step)

            def both(k, _):
                routed_on(distance * (2 * k - 1))
                return 0

            lax.fori_loop(0, 2, both, 0)
        elif step == 2:
            routed_in.hand_own().wait_recv()
            routed_on(0)
            routed_sum.give(-1, 1)
        elif step == 4:
            routed_sum.give(0, -2, 2)
        elif step == 6:
            routed_sum.give(-3, 3)
    routed_in.handed(ring.steps - 1)
    routed_on(ring.far)
    routed_sum.give(ring.far)
    shared_sum.give(ring.far, ring.far - 1, 1 - ring.far, *range(ring.far - 2, 1 - ring.far, -1))
    for step in range(ring.steps):
        routed_sum.advance(step)
    shared_sum.advance(0)
    shared_sum.advance(1)
    summed = jnp.concatenate([routed_sum.own_half(which).astype(bf16) for which in (0, 1)], axis=0)
    unpacked[...] = raw_dot(packing, summed, TN).astype(bf16).reshape(unpacked.shape)
    back = Push(SP, lambda peer: unpacked.at[peer], returned, sems[22:24])
    back.begin()
    for step in range(2, ring.steps):
        shared_sum.advance(step)
    half = residual.shape[0] // 2
    for which in (0, 1):
        piece = slice(which * half, (which + 1) * half)
        residual[piece, :] = residual[piece, :] + shared_sum.own_half(which)
    back.arrive()
    rows = returned[...].reshape(weighting.shape[1], width)
    routed = exact_right_dot(weighting, rows, NN)
    o_ref[...] = (residual[...] + routed).astype(bf16)
    for copy in ring.sent:
        copy.wait_send()
    dispatch.leave()
    back.leave()
    states.leave()


def layer(arrays, weights, devices, sp_count, capacity, room, number, name):
    tokens = arrays[1].shape[0]
    rows, width = arrays[8].shape
    hidden = weights[3].shape[1]
    local_experts = weights[0].shape[0]
    packed_rows = sp_count * local_experts * capacity
    block_count = tokens // BLOCK
    chips = devices // 2
    steps = chips - 1
    dma = pltpu.SemaphoreType.DMA
    anywhere = pl.BlockSpec(memory_space=pl.ANY)
    buffer = lambda *shape: pltpu.VMEM(shape, bf16)
    gather_sems = [dma((2, steps)), dma((2, steps)), dma((2, steps + 1)), dma((2, steps + 1))]
    sum_sems = [dma((chips,)), dma((chips,)), dma((2, steps)), dma((2, steps))]
    push_sems = [dma((sp_count,)), dma((sp_count,))]
    return pl.pallas_call(
        functools.partial(layer_kernel, devices=devices, sp_count=sp_count),
        name=name,
        out_shape=jax.ShapeDtypeStruct((rows, width), bf16),
        in_specs=[VMEM] * 12 + [anywhere] * 6,
        out_specs=VMEM,
        scratch_shapes=[
            pltpu.VMEM((tokens, LANES), f32),
            pltpu.VMEM((tokens, 2 * LANES), f32),
            pltpu.VMEM((2, block_count, BLOCK, LANES), f32),
            pltpu.VMEM((2, block_count, BLOCK, LANES), f32),
            pltpu.VMEM((2, block_count, LANES, LANES), f32),
            pltpu.VMEM((2, block_count, BLOCK, LANES), f32),
            buffer(2, 2 * BLOCK, LANES),
            buffer(sp_count, 2 * BLOCK, LANES),
            buffer(tokens, LANES),
            pltpu.VMEM((rows, width), f32),
            buffer(rows, width),
            buffer(sp_count, room, width),
            buffer(sp_count, room, width),
            buffer(packed_rows, width),
            buffer(sp_count, room, width),
            buffer(sp_count, room, width),
            buffer(devices, rows, width),
            buffer(devices, packed_rows, width),
            buffer(devices, rows, width),
            buffer(devices, rows, width),
            buffer(devices, packed_rows, width),
            buffer(chips, rows, width),
            buffer(chips, rows, width),
            buffer(chips, packed_rows, width),
            buffer(2, steps, rows // 2, width),
            buffer(2, steps, rows // 2, width),
            buffer(2, steps, packed_rows // 2, width),
            buffer(local_experts + 1, width, hidden),
            buffer(local_experts + 1, width, hidden),
            buffer(local_experts + 1, hidden, width),
            dma((6,)),
        ]
        + sum_sems
        + gather_sems
        + push_sems
        + gather_sems
        + sum_sems
        + sum_sems
        + push_sems
        + push_sems,
        compiler_params=pltpu.CompilerParams(
            collective_id=number, has_side_effects=True, vmem_limit_bytes=62 * 1024 * 1024
        ),
    )(*arrays, *weights)


def body(
    layer_input,
    receptance,
    keys,
    values,
    erase_preact,
    decay_preact,
    decay_spike,
    head_norm_gain,
    output_weight,
    expert_norm_gain,
    routes,
    routing_weight,
    expert_gate_weight,
    expert_up_weight,
    expert_down_weight,
    shared_gate_weight,
    shared_up_weight,
    shared_down_weight,
):
    sp_count, tp_count = lax.axis_size(SP), lax.axis_size(TP)
    return layer(
        (
            receptance,
            keys,
            values,
            erase_preact,
            decay_preact,
            decay_spike.T,
            head_norm_gain.reshape(1, -1),
            output_weight,
            layer_input,
            expert_norm_gain.reshape(-1, LANES),
            routes.T,
            routing_weight.T,
        ),
        (
            expert_gate_weight,
            expert_up_weight,
            expert_down_weight,
            shared_gate_weight,
            shared_up_weight,
            shared_down_weight,
        ),
        tp_count,
        sp_count,
        3,
        8,
        0,
        "layer",
    )


def solution(mesh):
    both = (SP, TP)
    in_specs = (
        P(both, None),
        P(SP, TP),
        P(SP, TP),
        P(SP, TP),
        P(SP, TP),
        P(SP, TP),
        P(SP, TP),
        P(TP),
        P(TP, None),
        P(),
        P(both, None),
        P(both, None),
        P(SP, None, TP),
        P(SP, None, TP),
        P(SP, TP, None),
        P(None, TP),
        P(None, TP),
        P(TP, None),
    )
    return jax.shard_map(
        body, mesh=mesh, in_specs=in_specs, out_specs=P(both, None), check_vma=False
    )
```

```python
import functools

import jax
import jax.numpy as jnp
from jax import lax
from jax.experimental import pallas as pl
from jax.experimental.pallas import tpu as pltpu
from jax.sharding import PartitionSpec as P

SP = "sp"
TP = "tp"
BLOCK = 64
LANES = 128
GN_EPS = 0.00064
RMS_EPS = 1e-06
f32 = jnp.float32
bf16 = jnp.bfloat16
VMEM = pl.BlockSpec(memory_space=pltpu.VMEM)
NN = (((1,), (0,)), ((), ()))
NT = (((1,), (1,)), ((), ()))
TN = (((0,), (0,)), ((), ()))


def iota(shape, dim):
    return lax.broadcasted_iota(jnp.int32, shape, dim)


def halves(array):
    high = array.astype(bf16)
    return high, (array - high.astype(f32)).astype(bf16)


def raw_dot(left, right, dims):
    return lax.dot_general(left, right, dims, preferred_element_type=f32)


def head_mask(count, dtype):
    first = (iota((count, LANES), 1) < BLOCK).astype(f32)
    return first.astype(dtype), (1.0 - first).astype(dtype)


def both_heads(rows):
    first, second = head_mask(rows.shape[0], rows.dtype)
    return jnp.concatenate([rows * first, rows * second], axis=0)


def fine_dot(left, right, dims, spread=False):
    left_high, left_low = halves(left)
    right_high, right_low = halves(right)
    if spread:
        right_high, right_low = both_heads(right_high), both_heads(right_low)
    if dims == TN:
        return raw_dot(
            jnp.concatenate([left_high, left_high, left_low], axis=0),
            jnp.concatenate([right_high, right_low, right_high], axis=0),
            TN,
        )
    count = left.shape[0]
    both = raw_dot(jnp.concatenate([left_high, left_low], axis=0), right_high, dims)
    return both[:count] + both[count:] + raw_dot(left_high, right_low, dims)


def exact_right_dot(left, right, dims):
    left_high, left_low = halves(left)
    count = left.shape[0]
    both = raw_dot(jnp.concatenate([left_high, left_low], axis=0), right, dims)
    return both[:count] + both[count:]


def head_sum(rows):
    ones = (iota((LANES, LANES), 0) // BLOCK == iota((LANES, LANES), 1) // BLOCK).astype(bf16)
    return exact_right_dot(rows, ones, NN)


def block_sums(log_decay):
    high, middle, low = three_parts(log_decay)
    count = log_decay.shape[0]
    ones = (iota((count, count), 0) >= iota((count, count), 1)).astype(bf16)
    width = log_decay.shape[1]
    sums = raw_dot(ones, jnp.concatenate([high, middle, low], axis=1), NN)
    return sums[:, :width] + sums[:, width : 2 * width] + sums[:, 2 * width :]


def inverses(stricts):
    row, lane = iota((BLOCK, LANES), 0), iota((BLOCK, LANES), 1) % BLOCK

    def within(size):
        return row // size == lane // size

    def products(lefts, rights):
        return [fine_dot(left, right, NN, spread=True) for left, right in zip(lefts, rights)]

    smalls = [jnp.where(within(8), strict, 0.0) for strict in stricts]
    starts = [jnp.where(row == lane, 1.0, 0.0) - small for small in smalls]
    squares = products(smalls, smalls)
    boths = products([jnp.concatenate(p, axis=0) for p in zip(starts, squares)], squares)
    results = [start + both[:BLOCK] for start, both in zip(starts, boths)]
    more = products(results, [both[BLOCK:] for both in boths])
    results = [r + m for r, m in zip(results, more)]
    for size in (8, 16, 32):
        keep = within(2 * size) & ~within(size)
        edges = products(results, [jnp.where(keep, strict, 0.0) for strict in stricts])
        more = products(edges, results)
        results = [r - m for r, m in zip(results, more)]
    return results


def block_terms(chains):
    row, lane = iota((BLOCK, LANES), 0), iota((BLOCK, LANES), 1) % BLOCK
    scaled, pairs = [], []
    for unit, beta, key_rows, _, read, left_unit, left_read, right, _, _ in chains:
        scaled.append((unit * left_unit, read * left_read, beta * right, key_rows * right))
    for unit_mid, read_mid, beta_mid, key_mid in scaled:
        left_high, left_low = halves(jnp.concatenate([unit_mid, read_mid], axis=0))
        right_high, right_low = [
            jnp.concatenate([both_heads(b), both_heads(k)], axis=0)
            for b, k in zip(halves(beta_mid), halves(key_mid))
        ]
        both = raw_dot(jnp.concatenate([left_high, left_low], axis=0), right_high, NT)
        pairs.append(both[: 2 * BLOCK] + both[2 * BLOCK :] + raw_dot(left_high, right_low, NT))
    erase_betas, keyeds, read_betas = [], [], []
    for pair, chain in zip(pairs, chains):
        strict = row > lane if chain[-1] else row < lane
        upto = row >= lane if chain[-1] else row <= lane
        erase_betas.append(jnp.where(strict, pair[:BLOCK, :LANES], 0.0))
        erase_key = jnp.where(strict, pair[:BLOCK, LANES:], 0.0)
        read_betas.append(jnp.where(upto, pair[BLOCK:, :LANES], 0.0))
        read_key = jnp.where(upto, pair[BLOCK:, LANES:], 0.0)
        keyeds.append(
            exact_right_dot(jnp.concatenate([erase_key, read_key], axis=0), chain[3], NN)
        )
    solvers = inverses(erase_betas)
    solved = []
    for solver, (unit_mid, _, _, _), keyed, chain in zip(solvers, scaled, keyeds, chains):
        solver_high, solver_low = halves(solver)
        right_high, right_low = [
            jnp.concatenate([both_heads(u), both_heads(k)], axis=1)
            for u, k in zip(halves(unit_mid * chain[8]), halves(-keyed[:BLOCK]))
        ]
        both = raw_dot(jnp.concatenate([solver_high, solver_low], axis=0), right_high, NN)
        solved.append(both[:BLOCK] + both[BLOCK:] + raw_dot(solver_high, right_low, NN))
    terms = []
    for found, read_beta, keyed, scale, chain in zip(solved, read_betas, keyeds, scaled, chains):
        spread_parts = [
            jnp.concatenate([both_heads(p[:, :LANES]), both_heads(p[:, LANES:])], axis=1)
            for p in halves(found)
        ]
        read_high, read_low = halves(read_beta)
        both = raw_dot(jnp.concatenate([read_high, read_low], axis=0), spread_parts[0], NN)
        applied = both[:BLOCK] + both[BLOCK:] + raw_dot(read_high, spread_parts[1], NN)
        readout = scale[1] * chain[8] - applied[:, :LANES]
        local = applied[:, LANES:] + keyed[BLOCK:]
        terms.append((found, scale[2] * chain[8], scale[3] * chain[8], readout, local))
    return terms


def three_parts(array):
    high = array.astype(bf16)
    rest = array - high.astype(f32)
    middle = rest.astype(bf16)
    return high, middle, (rest - middle.astype(f32)).astype(bf16)


def to_columns(rows, pick):
    chosen = [(pick == k).astype(bf16) for k in range(2)]
    parts = three_parts(rows)
    return raw_dot(
        jnp.concatenate(parts, axis=0), jnp.concatenate([jnp.concatenate(chosen, axis=0)] * 3, axis=0), TN
    )


def mixer_stage(
    read_ref,
    key_ref,
    value_ref,
    erase_ref,
    decay_ref,
    spike_ref,
    local_ref,
    readout_ref,
    prefix_ref,
    start_ref,
    move_ref,
    carry_ref,
    whole_ref,
    together,
):
    tokens = key_ref.shape[0]
    block_count = tokens // BLOCK
    same_head = iota((LANES, LANES), 0) // BLOCK == iota((LANES, LANES), 1) // BLOCK
    diagonal = iota((LANES, LANES), 0) == iota((LANES, LANES), 1)

    def some_blocks(index):
        blocks = [index * together + k for k in range(together)]
        span = together * BLOCK
        spikes = to_columns(
            spike_ref[:, pl.ds(pl.multiple_of(index * span, span), span)],
            iota((1, LANES), 1) // BLOCK,
        )
        chains, totals, values = [], [], []
        places = [pl.ds(pl.multiple_of(block * BLOCK, BLOCK), BLOCK) for block in blocks]
        for k, at in enumerate(places):
            key_rows = key_ref[at, :].astype(f32)
            read = read_ref[at, :].astype(f32)
            value = value_ref[at, :]
            unit = key_rows * lax.rsqrt(head_sum(key_rows * key_rows) + 1e-06)
            beta = unit * jax.nn.sigmoid(erase_ref[at, :].astype(f32))
            decay_in = decay_ref[at, :].astype(f32)
            spike = spikes[k * BLOCK : (k + 1) * BLOCK]
            log_decay = -jnp.exp(-jax.nn.softplus(-decay_in) - 0.5) + spike
            upto = block_sums(log_decay)
            total = upto[BLOCK - 1 :, :]
            middle = 0.5 * total
            ahead = upto - log_decay
            before, after = jnp.exp(ahead - middle), jnp.exp(upto - middle)
            until, since = jnp.exp(middle - upto), jnp.exp(middle - ahead)
            edge = jnp.exp(middle)
            shared = (unit, beta, key_rows, both_heads(value), read)
            chains.append(shared + (before, after, until, edge, True))
            chains.append(shared + (until, since, before, edge, False))
            totals.append(total)
            values.append(value)
        terms = block_terms(chains)
        for k, at in enumerate(places):
            local_ref[at, :] = terms[2 * k][4] + terms[2 * k + 1][4]
        for k, (solved, beta_end, key_end, readout, _) in enumerate(terms):
            way, at, value = k % 2, places[k // 2], values[k // 2]
            readout_ref[at, way * LANES : (way + 1) * LANES] = readout
            moved = fine_dot(solved, beta_end, TN)
            key_high, key_low = halves(key_end)
            keyed = raw_dot(
                jnp.concatenate([value, value], axis=0),
                jnp.concatenate([key_high, key_low], axis=0),
                TN,
            )
            move_ref[way, blocks[k // 2]] = jnp.where(
                same_head, jnp.where(diagonal, jnp.exp(totals[k // 2]), 0.0) - moved[:LANES], 0.0
            )
            carry = jnp.where(same_head, moved[LANES:] + keyed, 0.0)
            carry_ref[way, blocks[k // 2]] = carry[:BLOCK] + carry[BLOCK:]

    def step(index, _):
        some_blocks(index)
        return 0

    lax.fori_loop(0, block_count // together, step, 0)
    identity = jnp.where(iota((BLOCK, LANES), 0) == iota((BLOCK, LANES), 1) % BLOCK, 1.0, 0.0)
    running = [jnp.concatenate([identity, jnp.zeros_like(identity)], axis=0)] * 2
    for k in range(block_count):
        for way in range(2):
            block = k if way == 0 else block_count - 1 - k
            now = running[way]
            prefix_ref[way, block] = now[:BLOCK]
            start_ref[way, block] = now[BLOCK:]
            after = fine_dot(now, move_ref[way, block], NN)
            running[way] = jnp.concatenate(
                [after[:BLOCK], after[BLOCK:] + carry_ref[way, block]], axis=0
            )
    for way in range(2):
        whole_ref[way] = running[way].astype(bf16)


class Ring:
    def __init__(self, axis, chips):
        self.axis, self.chips = axis, chips
        self.me = lax.axis_index(axis)
        self.chip, self.core = self.me // 2, lax.rem(self.me, 2)
        self.steps = chips - 1
        self.far = chips // 2
        self.next = (self.slot(1, self.core), self.slot(-1, self.core))
        self.twin = self.chip * 2 + 1 - self.core
        self.sent = []

    def chip_at(self, distance):
        return lax.rem(self.chip + distance + self.chips, self.chips)

    def slot(self, distance, which):
        return self.chip_at(distance) * 2 + which

    def copy(self, source, target, send, recv, peer):
        return pltpu.make_async_remote_copy(
            src_ref=source, dst_ref=target, send_sem=send, recv_sem=recv, device_id={self.axis: peer}
        )

    def start(self, copy):
        copy.start()
        self.sent.append(copy)

    def half_of(self, way, step):
        return step % 2 if way == 0 else 1 - step % 2


class Gather:
    def __init__(self, ring, own, blocks, sems):
        self.ring, self.own, self.blocks = ring, own, blocks
        self.send, self.recv, self.pass_send, self.pass_recv = sems
        self.half = own.shape[0] // 2

    def piece(self, way, step):
        return pl.ds(self.ring.half_of(way, step) * self.half, self.half)

    def hop(self, way, step):
        ring, piece = self.ring, self.piece(way, step)
        at = ring.slot((step // 2) * (-1 if way == 0 else 1), ring.core)
        source = self.own.at[piece] if step < 2 else self.blocks.at[at, piece]
        return ring.copy(
            source,
            self.blocks.at[at, piece],
            self.send.at[way, step],
            self.recv.at[way, step],
            ring.next[way],
        )

    def hand(self, way, step):
        ring, piece = self.ring, self.piece(way, step)
        at = ring.slot((step // 2 + 1) * (-1 if way == 0 else 1), ring.core)
        return ring.copy(
            self.blocks.at[at, piece],
            self.blocks.at[at, piece],
            self.pass_send.at[way, step],
            self.pass_recv.at[way, step],
            ring.twin,
        )

    def hand_own(self):
        ring = self.ring
        return ring.copy(
            self.own,
            self.blocks.at[ring.me],
            self.pass_send.at[0, ring.steps],
            self.pass_recv.at[0, ring.steps],
            ring.twin,
        )

    def begin(self):
        for step in (0, 1):
            for way in (0, 1):
                self.ring.start(self.hop(way, step))
        self.ring.start(self.hand_own())
        self.blocks[self.ring.me] = self.own[...]

    def advance(self, step):
        for way in (0, 1):
            self.hop(way, step).wait_recv()
            if step + 2 < self.ring.steps:
                self.ring.start(self.hop(way, step + 2))
            self.ring.start(self.hand(way, step))

    def handed(self, *steps):
        for step in steps:
            for way in (0, 1):
                self.hand(way, step).wait_recv()


class Sum:
    def __init__(self, ring, partial, other, inbox, sems):
        self.ring, self.partial, self.other, self.inbox = ring, partial, other, inbox
        self.pair_send, self.pair_recv, self.send_sem, self.recv_sem = sems
        self.half = partial.shape[1] // 2
        self.met = set()

    def pair(self, distance):
        ring = self.ring
        index = ring.chip_at(distance)
        return ring.copy(
            self.partial.at[ring.slot(distance, 1 - ring.core)],
            self.other.at[index],
            self.pair_send.at[index],
            self.pair_recv.at[index],
            ring.twin,
        )

    def give(self, *distances):
        for distance in distances:
            self.ring.start(self.pair(distance))

    def meet(self, distance):
        key = distance % self.ring.chips
        if key not in self.met:
            self.met.add(key)
            self.pair(distance).wait_recv()

    def place(self, way, step):
        ring = self.ring
        distance = (ring.far - (step + 1) // 2) * (1 if way == 0 else -1)
        return distance, pl.ds(ring.half_of(way, step) * self.half, self.half)

    def hop(self, way, step):
        ring = self.ring
        distance, piece = self.place(way, step)
        return ring.copy(
            self.partial.at[ring.slot(distance, ring.core), piece],
            self.inbox.at[way, step],
            self.send_sem.at[way, step],
            self.recv_sem.at[way, step],
            ring.next[way],
        )

    def both_cores(self, distance, piece):
        ring = self.ring
        return self.partial[ring.slot(distance, ring.core), piece, :].astype(f32) + self.other[
            ring.chip_at(distance), piece, :
        ].astype(f32)

    def advance(self, step):
        ring = self.ring
        for way in (0, 1):
            distance, piece = self.place(way, step)
            self.meet(distance)
            total = self.both_cores(distance, piece)
            if step >= 2:
                self.hop(way, step - 2).wait_recv()
                total = total + self.inbox[way, step - 2].astype(f32)
            self.partial[ring.slot(distance, ring.core), piece, :] = total.astype(bf16)
        for way in (0, 1):
            ring.start(self.hop(way, step))

    def own_half(self, which):
        ring = self.ring
        self.meet(0)
        total = self.both_cores(0, pl.ds(which * self.half, self.half))
        for way in (0, 1):
            step = ring.steps - 2 if ring.half_of(way, ring.steps - 2) == which else ring.steps - 1
            self.hop(way, step).wait_recv()
            total = total + self.inbox[way, step].astype(f32)
        return total


class Push:
    def __init__(self, axis, count, source, target, sems, base=0):
        self.axis, self.source, self.target = axis, source, target
        self.send, self.recv = sems
        self.count, self.base = count, base
        self.me = lax.axis_index(axis)
        self.copies = []

    def begin(self):
        for k in range(1, self.count):
            peer = lax.rem(self.me + k, self.count)
            copy = pltpu.make_async_remote_copy(
                src_ref=self.source(peer),
                dst_ref=self.target.at[self.base + self.me],
                send_sem=self.send.at[k],
                recv_sem=self.recv.at[k],
                device_id={self.axis: peer},
            )
            copy.start()
            self.copies.append(copy)
        self.target[self.base + self.me] = self.source(self.me)[...]

    def arrive(self):
        for copy in self.copies:
            copy.wait_recv()

    def leave(self):
        for copy in self.copies:
            copy.wait_send()


def meet_peers(axis, count, others):
    me = lax.axis_index(axis)
    barrier = pltpu.get_barrier_semaphore()
    for k in range(1, count):
        pl.semaphore_signal(barrier, inc=1, device_id={axis: lax.rem(me + k, count)})
    for name, peer in others:
        pl.semaphore_signal(barrier, inc=1, device_id={name: peer})
    return barrier, count - 1 + len(others)


def finish_blocks(place, got_ref, local_ref, readout_ref, prefix_ref, start_ref, gain_ref, mixed_ref):
    count = got_ref.shape[0]
    blocks = range(prefix_ref.shape[1])
    entry = [jnp.zeros((BLOCK, LANES), f32)] * 2
    for k in range(count - 1):
        for way in range(2):
            j = k if way == 0 else count - 1 - k
            passed = j < place if way == 0 else j > place
            moved = exact_right_dot(entry[way], both_heads(got_ref[j, :BLOCK, :]), NN)
            entry[way] = jnp.where(passed, moved + got_ref[j, BLOCK:, :].astype(f32), entry[way])
    gain = gain_ref[...].astype(f32)
    states = []
    for way in range(2):
        high, low = halves(entry[way])
        stacked = jnp.concatenate([high, low], axis=0)
        prefixes = [[both_heads(p) for p in halves(prefix_ref[way, b])] for b in blocks]
        boths = [raw_dot(stacked, p[0], NN) for p in prefixes]
        rests = [raw_dot(high, p[1], NN) for p in prefixes]
        states.append(
            [
                [both_heads(p) for p in halves(x[:BLOCK] + x[BLOCK:] + y + start_ref[way, b])]
                for x, y, b in zip(boths, rests, blocks)
            ]
        )
    places = [slice(b * BLOCK, (b + 1) * BLOCK) for b in blocks]
    mixes = []
    for b in blocks:
        state_high, state_low = [
            jnp.concatenate([states[0][b][k], states[1][b][k]], axis=1) for k in (0, 1)
        ]
        read_high, read_low = halves(readout_ref[places[b], :])
        both = raw_dot(jnp.concatenate([read_high, read_low], axis=0), state_high, NT)
        mixes.append(
            local_ref[places[b], :] + both[:BLOCK] + both[BLOCK:] + raw_dot(read_high, state_low, NT)
        )
    centers = [mix - head_sum(mix) * (1.0 / BLOCK) for mix in mixes]
    spreads = [head_sum(center * center) * (1.0 / BLOCK) for center in centers]
    for b in blocks:
        mixed_ref[places[b], :] = (centers[b] * lax.rsqrt(spreads[b] + GN_EPS) * gain).astype(bf16)


def routing(routes_ref, weights_ref):
    rows = routes_ref.shape[1]
    slot = iota((rows, LANES), 1)
    names, values = [], []
    for k in range(2):
        pick = jnp.full((1, LANES), k, jnp.int32)
        names.append(to_columns(routes_ref[...].astype(f32), pick))
        values.append(to_columns(weights_ref[...], pick))
    before = (iota((rows, rows), 0) > iota((rows, rows), 1)).astype(bf16)

    def filled(expert, rank):
        named = [jnp.where(name == expert.astype(f32), 1.0, 0.0) for name in names]
        either = named[0] + named[1]
        taken = raw_dot(before, either.astype(bf16), NN)
        here = jnp.where(taken == rank.astype(f32), 1.0, 0.0)
        return either * here, (named[0] * values[0] + named[1] * values[1]) * here

    placing, weighting = filled(slot // 8 * 2 + slot % 4 // 2, slot % 2)
    late, late_weight = filled(slot % 32, jnp.full_like(slot, 2))
    high, low = halves(late_weight)
    kind = slot // 32
    info = jnp.where(
        kind == 0,
        late,
        jnp.where(kind == 1, high.astype(f32), jnp.where(kind == 2, low.astype(f32), 0.0)),
    )
    per_expert = LANES // 8 * 2
    shape = (2 * per_expert, LANES)
    at = iota(shape, 1)
    target = at % 4 // 2 * per_expert + at // 8 * 2 + at % 2
    column = at % 8 // 4
    packing = [
        jnp.where((iota(shape, 0) == target) & (column == k), 1.0, 0.0).astype(bf16) for k in range(2)
    ]
    return placing, weighting, info, packing


def late_pick(lanes_per_part, part, core, peers, blocks):
    row, lane = iota((peers * blocks, LANES), 0), iota((peers * blocks, LANES), 1)
    return jnp.where(lane == part * lanes_per_part + row // blocks * 2 + core, 1.0, 0.0).astype(bf16)


def layer_kernel(
    read_ref,
    key_ref,
    value_ref,
    erase_ref,
    decay_ref,
    spike_ref,
    gain_ref,
    mix_weight_ref,
    input_ref,
    norm_gain_ref,
    routes_ref,
    route_weights_ref,
    expert_gate,
    expert_up,
    expert_down,
    shared_gate,
    shared_up,
    shared_down,
    o_ref,
    local_ref,
    readout_ref,
    prefix_ref,
    start_ref,
    move_ref,
    carry_ref,
    whole_ref,
    got_ref,
    mixed,
    residual,
    normed,
    outgoing,
    arrived,
    packed,
    unpacked,
    returned,
    shared_blocks,
    routed_blocks,
    late_out,
    late_blocks,
    late_partial,
    late_other,
    late_back,
    late_returned,
    mix_partial,
    shared_partial,
    routed_partial,
    mix_other,
    shared_other,
    routed_other,
    mix_inbox,
    shared_inbox,
    routed_inbox,
    gate,
    up,
    down,
    weight_sem,
    *sems,
    devices,
    sp_count,
):
    ring = Ring(TP, devices // 2)
    local_experts = expert_gate.shape[0]
    width = input_ref.shape[1]
    used = packed.shape[0] // local_experts
    weight_copies = []
    for k, (pair, single, into) in enumerate(
        ((expert_gate, shared_gate, gate), (expert_up, shared_up, up), (expert_down, shared_down, down))
    ):
        weight_copies.append(
            pltpu.make_async_copy(pair, into.at[pl.ds(0, local_experts)], weight_sem.at[2 * k])
        )
        weight_copies.append(
            pltpu.make_async_copy(single, into.at[local_experts], weight_sem.at[2 * k + 1])
        )
    for copy in weight_copies:
        copy.start()
    barrier, expected = meet_peers(
        SP, sp_count, [(TP, ring.next[0]), (TP, ring.next[1]), (TP, ring.twin)]
    )

    placing, weighting, info, packing = routing(routes_ref, route_weights_ref)
    slot = iota(placing.shape, 1)
    columns_of = [(slot % 8 // 4 == k).astype(f32) for k in range(2)]
    side = width // 2
    mixer_stage(
        read_ref,
        key_ref,
        value_ref,
        erase_ref,
        decay_ref,
        spike_ref,
        local_ref,
        readout_ref,
        prefix_ref,
        start_ref,
        move_ref,
        carry_ref,
        whole_ref,
        4,
    )
    pl.semaphore_wait(barrier, expected)
    here = lax.axis_index(SP)
    states = Push(
        SP,
        sp_count,
        lambda peer: whole_ref.at[(here + sp_count - peer) // (sp_count + 1)],
        got_ref,
        sems[24:26],
    )
    states.begin()
    states.arrive()

    finish_blocks(
        lax.axis_index(SP), got_ref, local_ref, readout_ref, prefix_ref, start_ref, gain_ref, mixed
    )
    columns = 512

    def project(k, _):
        at = pl.ds(pl.multiple_of(k * columns, columns), columns)
        product = raw_dot(mixed[...], mix_weight_ref[:, at], NN).astype(bf16)
        mix_partial[:, :, at] = product.reshape(mix_partial.shape[0], mix_partial.shape[1], columns)
        return 0

    lax.fori_loop(0, width // columns, project, 0)
    mix_sum = Sum(ring, mix_partial, mix_other, mix_inbox, sems[0:4])
    mix_sum.give(ring.far, ring.far - 1, 1 - ring.far, *range(ring.far - 2, 1 - ring.far, -1))
    for step in range(ring.steps):
        mix_sum.advance(step)
    gains = norm_gain_ref[...].astype(f32)
    norm_gain = jnp.concatenate([gains[k : k + 1] for k in range(gains.shape[0])], axis=1)
    half = residual.shape[0] // 2
    for which in (0, 1):
        piece = slice(which * half, (which + 1) * half)
        rows = input_ref[piece, :].astype(f32) + mix_sum.own_half(which)
        residual[piece, :] = rows
        scale = lax.rsqrt(jnp.mean(rows * rows, axis=-1, keepdims=True) + RMS_EPS)
        normed[piece, :width] = (rows * scale * norm_gain).astype(bf16)
        normed[piece, width:] = info[piece, :].astype(bf16)

    shared_in = Gather(ring, normed, shared_blocks, sems[4:8])
    outgoing[...] = (
        raw_dot(
            jnp.concatenate([(placing * c).astype(bf16) for c in columns_of], axis=0),
            jnp.concatenate([normed[:, :side], normed[:, side:width]], axis=0),
            TN,
        )
        .astype(bf16)
        .reshape(outgoing.shape)
    )
    shared_in.begin()
    dispatch = Push(SP, sp_count, lambda peer: outgoing.at[peer], arrived, sems[8:10])
    dispatch.begin()
    for step in range(ring.steps - 1):
        shared_in.advance(step)
    dispatch.arrive()
    arrivals = arrived[...].reshape(LANES, side)
    packed[...] = jnp.concatenate([raw_dot(p, arrivals, NN) for p in packing], axis=1).astype(bf16)
    routed_in = Gather(ring, packed, routed_blocks, sems[10:14])
    routed_in.begin()
    shared_in.advance(ring.steps - 1)

    def expert_on(blocks, partial, first, count, at, which):
        rows = at.size
        x = blocks[pl.ds(first, count), at, pl.ds(0, width)].reshape(count * rows, width)
        gated = raw_dot(x, gate[which], NN)
        lifted = raw_dot(x, up[which], NN)
        inner = (gated / (1.0 + jnp.exp(-gated)) * lifted).astype(bf16)
        partial[pl.ds(first, count), at, :] = (
            raw_dot(inner, down[which], NN).astype(bf16).reshape(count, rows, width)
        )

    def routed_on(distance):
        first = ring.chip_at(distance) * 2

        def one(k, _):
            at = pl.ds(pl.multiple_of(k * used, 16), used)
            expert_on(routed_blocks, routed_partial, first, 2, at, k)
            return 0

        lax.fori_loop(0, local_experts, one, 0)

    def shared_on(quarter):
        count = devices // 4
        at = pl.ds(0, normed.shape[0])
        expert_on(shared_blocks, shared_partial, quarter * count, count, at, local_experts)

    routed_sum = Sum(ring, routed_partial, routed_other, routed_inbox, sems[14:18])
    shared_sum = Sum(ring, shared_partial, shared_other, shared_inbox, sems[18:22])
    shared_in.hand_own().wait_recv()
    shared_in.handed(*range(ring.steps))

    block_rows = normed.shape[0]
    group_rows, late_rows = devices * block_rows, sp_count * devices
    infos = shared_blocks[:, :, pl.ds(width, LANES)].reshape(group_rows, LANES)
    of_block = (
        iota((late_rows, group_rows), 0) % devices == iota((late_rows, group_rows), 1) // block_rows
    )
    chosen = jnp.where(
        of_block, raw_dot(late_pick(32, 0, ring.core, sp_count, devices), infos, NT), 0.0
    ).astype(bf16)

    def choose(k, _):
        at = pl.ds(pl.multiple_of(k * columns, columns), columns)
        rows = raw_dot(chosen, shared_blocks[:, :, at].reshape(group_rows, columns), NN)
        late_out[:, :, at] = rows.astype(bf16).reshape(sp_count, devices, columns)
        return 0

    lax.fori_loop(0, width // columns, choose, 0)
    late_in = Push(
        SP, sp_count, lambda peer: late_out.at[peer], late_blocks, sems[26:28], ring.core * sp_count
    )
    late_in.begin()

    def late_hand(which):
        return ring.copy(
            late_blocks.at[which],
            late_blocks.at[which],
            sems[28].at[lax.rem(which, sp_count)],
            sems[29].at[lax.rem(which, sp_count)],
            ring.twin,
        )

    def late_handed(k):
        return late_hand((1 - ring.core) * sp_count + k)

    late_pair = ring.copy(
        late_partial.at[pl.ds((1 - ring.core) * sp_count, sp_count)],
        late_other,
        sems[30].at[0],
        sems[30].at[1],
        ring.twin,
    )
    for copy in weight_copies:
        copy.wait()

    def quarters(first):
        def one(k, _):
            shared_on(first + k)
            return 0

        lax.fori_loop(0, 2, one, 0)

    quarters(0)
    for step in range(ring.steps):
        routed_in.advance(step)
        if step == 0:
            quarters(2)
        elif step % 2 == 1:
            distance = (step + 1) // 2
            routed_in.handed(step - 1, step)

            def both(k, _):
                routed_on(distance * (2 * k - 1))
                return 0

            lax.fori_loop(0, 2, both, 0)
        elif step == 2:
            routed_in.hand_own().wait_recv()
            routed_on(0)
            routed_sum.give(-1, 1)
        elif step == 4:
            routed_sum.give(0, -2, 2)
        elif step == 6:
            routed_sum.give(-3, 3)
    ring.start(late_hand(ring.core * sp_count + here))
    for k in range(1, sp_count):
        late_in.copies[k - 1].wait_recv()
        ring.start(late_hand(ring.core * sp_count + lax.rem(here + sp_count - k, sp_count)))
    routed_in.handed(ring.steps - 1)
    routed_on(ring.far)
    routed_sum.give(ring.far)
    routed_sum.advance(0)
    routed_sum.advance(1)
    for k in range(sp_count):
        late_handed(k).wait_recv()

    def late_on(k, _):
        expert_on(late_blocks, late_partial, k * sp_count, sp_count, pl.ds(0, devices), k)
        return 0

    lax.fori_loop(0, local_experts, late_on, 0)
    routed_sum.advance(2)
    ring.start(late_pair)
    routed_sum.advance(3)
    late_pair.wait_recv()
    late_back[...] = (
        late_partial[pl.ds(ring.core * sp_count, sp_count)].astype(f32) + late_other[...].astype(f32)
    ).astype(bf16)
    late_home = Push(SP, sp_count, lambda peer: late_back.at[peer], late_returned, sems[31:33])
    late_home.begin()
    for step in range(4, ring.steps):
        routed_sum.advance(step)
    summed = jnp.concatenate([routed_sum.own_half(which).astype(bf16) for which in (0, 1)], axis=0)
    unpacked[...] = (
        (
            raw_dot(packing[0], summed[:, :side], TN) + raw_dot(packing[1], summed[:, side:], TN)
        )
        .astype(bf16)
        .reshape(unpacked.shape)
    )
    back = Push(SP, sp_count, lambda peer: unpacked.at[peer], returned, sems[22:24])
    back.begin()
    late_home.arrive()
    by_row = iota((group_rows, late_rows), 0) // block_rows == iota((group_rows, late_rows), 1) % devices
    late_weights = [
        jnp.where(by_row, raw_dot(infos, late_pick(32, k, ring.core, sp_count, devices), NT), 0.0).astype(bf16)
        for k in (1, 2)
    ]

    def add_late(k, _):
        at = pl.ds(pl.multiple_of(k * columns, columns), columns)
        rows = late_returned[:, :, at].reshape(late_rows, columns)
        added = raw_dot(late_weights[0], rows, NN) + raw_dot(late_weights[1], rows, NN)
        shared_partial[:, :, at] = (
            shared_partial[:, :, at].astype(f32) + added.reshape(devices, block_rows, columns)
        ).astype(bf16)
        return 0

    lax.fori_loop(0, width // columns, add_late, 0)
    shared_sum.give(ring.far, ring.far - 1, 1 - ring.far, *range(ring.far - 2, 1 - ring.far, -1))
    for step in range(ring.steps):
        shared_sum.advance(step)
    half = residual.shape[0] // 2
    for which in (0, 1):
        piece = slice(which * half, (which + 1) * half)
        residual[piece, :] = residual[piece, :] + shared_sum.own_half(which)
    back.arrive()
    rows = returned[...].reshape(LANES, side)
    routed = jnp.concatenate([exact_right_dot(weighting * c, rows, NN) for c in columns_of], axis=1)
    o_ref[...] = (residual[...] + routed).astype(bf16)
    for copy in ring.sent:
        copy.wait_send()
    dispatch.leave()
    back.leave()
    states.leave()
    late_in.leave()
    late_home.leave()


def layer(arrays, weights, devices, sp_count, capacity, room, number, name):
    tokens = arrays[1].shape[0]
    rows, width = arrays[8].shape
    hidden = weights[3].shape[1]
    local_experts = weights[0].shape[0]
    packed_rows = sp_count * local_experts * capacity
    block_count = tokens // BLOCK
    chips = devices // 2
    steps = chips - 1
    dma = pltpu.SemaphoreType.DMA
    anywhere = pl.BlockSpec(memory_space=pl.ANY)
    buffer = lambda *shape: pltpu.VMEM(shape, bf16)
    gather_sems = [dma((2, steps)), dma((2, steps)), dma((2, steps + 1)), dma((2, steps + 1))]
    sum_sems = [dma((chips,)), dma((chips,)), dma((2, steps)), dma((2, steps))]
    push_sems = [dma((sp_count,)), dma((sp_count,))]
    return pl.pallas_call(
        functools.partial(layer_kernel, devices=devices, sp_count=sp_count),
        name=name,
        out_shape=jax.ShapeDtypeStruct((rows, width), bf16),
        in_specs=[VMEM] * 12 + [anywhere] * 6,
        out_specs=VMEM,
        scratch_shapes=[
            pltpu.VMEM((tokens, LANES), f32),
            pltpu.VMEM((tokens, 2 * LANES), f32),
            pltpu.VMEM((2, block_count, BLOCK, LANES), f32),
            pltpu.VMEM((2, block_count, BLOCK, LANES), f32),
            pltpu.VMEM((2, block_count, LANES, LANES), f32),
            pltpu.VMEM((2, block_count, BLOCK, LANES), f32),
            buffer(2, 2 * BLOCK, LANES),
            buffer(sp_count, 2 * BLOCK, LANES),
            buffer(tokens, LANES),
            pltpu.VMEM((rows, width), f32),
            buffer(rows, width + LANES),
            buffer(sp_count, room, width // 2),
            buffer(sp_count, room, width // 2),
            buffer(packed_rows, width),
            buffer(sp_count, room, width // 2),
            buffer(sp_count, room, width // 2),
            buffer(devices, rows, width + LANES),
            buffer(devices, packed_rows, width),
            buffer(sp_count, devices, width),
            buffer(local_experts * sp_count, devices, width),
            buffer(local_experts * sp_count, devices, width),
            buffer(sp_count, devices, width),
            buffer(sp_count, devices, width),
            buffer(sp_count, devices, width),
            buffer(devices, rows, width),
            buffer(devices, rows, width),
            buffer(devices, packed_rows, width),
            buffer(chips, rows, width),
            buffer(chips, rows, width),
            buffer(chips, packed_rows, width),
            buffer(2, steps, rows // 2, width),
            buffer(2, steps, rows // 2, width),
            buffer(2, steps, packed_rows // 2, width),
            buffer(local_experts + 1, width, hidden),
            buffer(local_experts + 1, width, hidden),
            buffer(local_experts + 1, hidden, width),
            dma((6,)),
        ]
        + sum_sems
        + gather_sems
        + push_sems
        + gather_sems
        + sum_sems
        + sum_sems
        + push_sems
        + push_sems
        + push_sems
        + push_sems
        + [dma((2,))]
        + push_sems,
        compiler_params=pltpu.CompilerParams(
            collective_id=number, has_side_effects=True, vmem_limit_bytes=62 * 1024 * 1024
        ),
    )(*arrays, *weights)


def body(
    layer_input,
    receptance,
    keys,
    values,
    erase_preact,
    decay_preact,
    decay_spike,
    head_norm_gain,
    output_weight,
    expert_norm_gain,
    routes,
    routing_weight,
    expert_gate_weight,
    expert_up_weight,
    expert_down_weight,
    shared_gate_weight,
    shared_up_weight,
    shared_down_weight,
):
    sp_count, tp_count = lax.axis_size(SP), lax.axis_size(TP)
    return layer(
        (
            receptance,
            keys,
            values,
            erase_preact,
            decay_preact,
            decay_spike.T,
            head_norm_gain.reshape(1, -1),
            output_weight,
            layer_input,
            expert_norm_gain.reshape(-1, LANES),
            routes.T,
            routing_weight.T,
        ),
        (
            expert_gate_weight,
            expert_up_weight,
            expert_down_weight,
            shared_gate_weight,
            shared_up_weight,
            shared_down_weight,
        ),
        tp_count,
        sp_count,
        2,
        8,
        0,
        "layer",
    )


def solution(mesh):
    both = (SP, TP)
    in_specs = (
        P(both, None),
        P(SP, TP),
        P(SP, TP),
        P(SP, TP),
        P(SP, TP),
        P(SP, TP),
        P(SP, TP),
        P(TP),
        P(TP, None),
        P(),
        P(both, None),
        P(both, None),
        P(SP, None, TP),
        P(SP, None, TP),
        P(SP, TP, None),
        P(None, TP),
        P(None, TP),
        P(TP, None),
    )
    return jax.shard_map(
        body, mesh=mesh, in_specs=in_specs, out_specs=P(both, None), check_vma=False
    )
```

```python
import functools

import jax
import jax.numpy as jnp
from jax import lax
from jax.experimental import pallas as pl
from jax.experimental.pallas import tpu as pltpu
from jax.sharding import PartitionSpec as P

SP = "sp"
TP = "tp"
BLOCK = 64
LANES = 128
GN_EPS = 0.00064
RMS_EPS = 1e-06
f32 = jnp.float32
bf16 = jnp.bfloat16
VMEM = pl.BlockSpec(memory_space=pltpu.VMEM)
NN = (((1,), (0,)), ((), ()))
NT = (((1,), (1,)), ((), ()))
TN = (((0,), (0,)), ((), ()))


def iota(shape, dim):
    return lax.broadcasted_iota(jnp.int32, shape, dim)


def halves(array):
    high = array.astype(bf16)
    return high, (array - high.astype(f32)).astype(bf16)


def raw_dot(left, right, dims):
    return lax.dot_general(left, right, dims, preferred_element_type=f32)


def head_mask(count, dtype):
    first = (iota((count, LANES), 1) < BLOCK).astype(f32)
    return first.astype(dtype), (1.0 - first).astype(dtype)


def both_heads(rows):
    first, second = head_mask(rows.shape[0], rows.dtype)
    return jnp.concatenate([rows * first, rows * second], axis=0)


def fine_dot(left, right, dims, spread=False):
    left_high, left_low = halves(left)
    right_high, right_low = halves(right)
    if spread:
        right_high, right_low = both_heads(right_high), both_heads(right_low)
    if dims == TN:
        return raw_dot(
            jnp.concatenate([left_high, left_high, left_low], axis=0),
            jnp.concatenate([right_high, right_low, right_high], axis=0),
            TN,
        )
    count = left.shape[0]
    both = raw_dot(jnp.concatenate([left_high, left_low], axis=0), right_high, dims)
    return both[:count] + both[count:] + raw_dot(left_high, right_low, dims)


def exact_right_dot(left, right, dims):
    left_high, left_low = halves(left)
    count = left.shape[0]
    both = raw_dot(jnp.concatenate([left_high, left_low], axis=0), right, dims)
    return both[:count] + both[count:]


def head_sum(rows):
    ones = (iota((LANES, LANES), 0) // BLOCK == iota((LANES, LANES), 1) // BLOCK).astype(bf16)
    return exact_right_dot(rows, ones, NN)


def block_sums(log_decay):
    high, middle, low = three_parts(log_decay)
    count = log_decay.shape[0]
    ones = (iota((count, count), 0) >= iota((count, count), 1)).astype(bf16)
    width = log_decay.shape[1]
    sums = raw_dot(ones, jnp.concatenate([high, middle, low], axis=1), NN)
    return sums[:, :width] + sums[:, width : 2 * width] + sums[:, 2 * width :]


def inverses(stricts):
    row, lane = iota((BLOCK, LANES), 0), iota((BLOCK, LANES), 1) % BLOCK

    def within(size):
        return row // size == lane // size

    def products(lefts, rights):
        return [fine_dot(left, right, NN, spread=True) for left, right in zip(lefts, rights)]

    smalls = [jnp.where(within(8), strict, 0.0) for strict in stricts]
    starts = [jnp.where(row == lane, 1.0, 0.0) - small for small in smalls]
    squares = products(smalls, smalls)
    boths = products([jnp.concatenate(p, axis=0) for p in zip(starts, squares)], squares)
    results = [start + both[:BLOCK] for start, both in zip(starts, boths)]
    more = products(results, [both[BLOCK:] for both in boths])
    results = [r + m for r, m in zip(results, more)]
    for size in (8, 16, 32):
        keep = within(2 * size) & ~within(size)
        edges = products(results, [jnp.where(keep, strict, 0.0) for strict in stricts])
        more = products(edges, results)
        results = [r - m for r, m in zip(results, more)]
    return results


def block_terms(chains):
    row, lane = iota((BLOCK, LANES), 0), iota((BLOCK, LANES), 1) % BLOCK
    scaled, pairs = [], []
    for unit, beta, key_rows, _, read, left_unit, left_read, right, _, _ in chains:
        scaled.append((unit * left_unit, read * left_read, beta * right, key_rows * right))
    for unit_mid, read_mid, beta_mid, key_mid in scaled:
        left_high, left_low = halves(jnp.concatenate([unit_mid, read_mid], axis=0))
        right_high, right_low = [
            jnp.concatenate([both_heads(b), both_heads(k)], axis=0)
            for b, k in zip(halves(beta_mid), halves(key_mid))
        ]
        both = raw_dot(jnp.concatenate([left_high, left_low], axis=0), right_high, NT)
        pairs.append(both[: 2 * BLOCK] + both[2 * BLOCK :] + raw_dot(left_high, right_low, NT))
    erase_betas, keyeds, read_betas = [], [], []
    for pair, chain in zip(pairs, chains):
        strict = row > lane if chain[-1] else row < lane
        upto = row >= lane if chain[-1] else row <= lane
        erase_betas.append(jnp.where(strict, pair[:BLOCK, :LANES], 0.0))
        erase_key = jnp.where(strict, pair[:BLOCK, LANES:], 0.0)
        read_betas.append(jnp.where(upto, pair[BLOCK:, :LANES], 0.0))
        read_key = jnp.where(upto, pair[BLOCK:, LANES:], 0.0)
        keyeds.append(
            exact_right_dot(jnp.concatenate([erase_key, read_key], axis=0), chain[3], NN)
        )
    solvers = inverses(erase_betas)
    solved = []
    for solver, (unit_mid, _, _, _), keyed, chain in zip(solvers, scaled, keyeds, chains):
        solver_high, solver_low = halves(solver)
        right_high, right_low = [
            jnp.concatenate([both_heads(u), both_heads(k)], axis=1)
            for u, k in zip(halves(unit_mid * chain[8]), halves(-keyed[:BLOCK]))
        ]
        both = raw_dot(jnp.concatenate([solver_high, solver_low], axis=0), right_high, NN)
        solved.append(both[:BLOCK] + both[BLOCK:] + raw_dot(solver_high, right_low, NN))
    terms = []
    for found, read_beta, keyed, scale, chain in zip(solved, read_betas, keyeds, scaled, chains):
        spread_parts = [
            jnp.concatenate([both_heads(p[:, :LANES]), both_heads(p[:, LANES:])], axis=1)
            for p in halves(found)
        ]
        read_high, read_low = halves(read_beta)
        both = raw_dot(jnp.concatenate([read_high, read_low], axis=0), spread_parts[0], NN)
        applied = both[:BLOCK] + both[BLOCK:] + raw_dot(read_high, spread_parts[1], NN)
        readout = scale[1] * chain[8] - applied[:, :LANES]
        local = applied[:, LANES:] + keyed[BLOCK:]
        terms.append((found, scale[2] * chain[8], scale[3] * chain[8], readout, local))
    return terms


def three_parts(array):
    high = array.astype(bf16)
    rest = array - high.astype(f32)
    middle = rest.astype(bf16)
    return high, middle, (rest - middle.astype(f32)).astype(bf16)


def to_columns(rows, pick):
    chosen = [(pick == k).astype(bf16) for k in range(2)]
    parts = three_parts(rows)
    return raw_dot(
        jnp.concatenate(parts, axis=0), jnp.concatenate([jnp.concatenate(chosen, axis=0)] * 3, axis=0), TN
    )


def mixer_stage(
    read_ref,
    key_ref,
    value_ref,
    erase_ref,
    decay_ref,
    spike_ref,
    local_ref,
    readout_ref,
    prefix_ref,
    start_ref,
    move_ref,
    carry_ref,
    whole_ref,
    together,
):
    tokens = key_ref.shape[0]
    block_count = tokens // BLOCK
    same_head = iota((LANES, LANES), 0) // BLOCK == iota((LANES, LANES), 1) // BLOCK
    diagonal = iota((LANES, LANES), 0) == iota((LANES, LANES), 1)

    def some_blocks(index):
        blocks = [index * together + k for k in range(together)]
        span = together * BLOCK
        spikes = to_columns(
            spike_ref[:, pl.ds(pl.multiple_of(index * span, span), span)],
            iota((1, LANES), 1) // BLOCK,
        )
        chains, totals, values = [], [], []
        places = [pl.ds(pl.multiple_of(block * BLOCK, BLOCK), BLOCK) for block in blocks]
        for k, at in enumerate(places):
            key_rows = key_ref[at, :].astype(f32)
            read = read_ref[at, :].astype(f32)
            value = value_ref[at, :]
            unit = key_rows * lax.rsqrt(head_sum(key_rows * key_rows) + 1e-06)
            beta = unit * jax.nn.sigmoid(erase_ref[at, :].astype(f32))
            decay_in = decay_ref[at, :].astype(f32)
            spike = spikes[k * BLOCK : (k + 1) * BLOCK]
            log_decay = -jnp.exp(-jax.nn.softplus(-decay_in) - 0.5) + spike
            upto = block_sums(log_decay)
            total = upto[BLOCK - 1 :, :]
            middle = 0.5 * total
            ahead = upto - log_decay
            before, after = jnp.exp(ahead - middle), jnp.exp(upto - middle)
            until, since = jnp.exp(middle - upto), jnp.exp(middle - ahead)
            edge = jnp.exp(middle)
            shared = (unit, beta, key_rows, both_heads(value), read)
            chains.append(shared + (before, after, until, edge, True))
            chains.append(shared + (until, since, before, edge, False))
            totals.append(total)
            values.append(value)
        terms = block_terms(chains)
        for k, at in enumerate(places):
            local_ref[at, :] = terms[2 * k][4] + terms[2 * k + 1][4]
        for k, (solved, beta_end, key_end, readout, _) in enumerate(terms):
            way, at, value = k % 2, places[k // 2], values[k // 2]
            readout_ref[at, way * LANES : (way + 1) * LANES] = readout
            moved = fine_dot(solved, beta_end, TN)
            key_high, key_low = halves(key_end)
            keyed = raw_dot(
                jnp.concatenate([value, value], axis=0),
                jnp.concatenate([key_high, key_low], axis=0),
                TN,
            )
            move_ref[way, blocks[k // 2]] = jnp.where(
                same_head, jnp.where(diagonal, jnp.exp(totals[k // 2]), 0.0) - moved[:LANES], 0.0
            )
            carry = jnp.where(same_head, moved[LANES:] + keyed, 0.0)
            carry_ref[way, blocks[k // 2]] = carry[:BLOCK] + carry[BLOCK:]

    def step(index, _):
        some_blocks(index)
        return 0

    lax.fori_loop(0, block_count // together, step, 0)
    identity = jnp.where(iota((BLOCK, LANES), 0) == iota((BLOCK, LANES), 1) % BLOCK, 1.0, 0.0)
    running = [jnp.concatenate([identity, jnp.zeros_like(identity)], axis=0)] * 2
    for k in range(block_count):
        for way in range(2):
            block = k if way == 0 else block_count - 1 - k
            now = running[way]
            prefix_ref[way, block] = now[:BLOCK]
            start_ref[way, block] = now[BLOCK:]
            after = fine_dot(now, move_ref[way, block], NN)
            running[way] = jnp.concatenate(
                [after[:BLOCK], after[BLOCK:] + carry_ref[way, block]], axis=0
            )
    for way in range(2):
        whole_ref[way] = running[way].astype(bf16)


class Ring:
    def __init__(self, axis, chips):
        self.axis, self.chips = axis, chips
        self.me = lax.axis_index(axis)
        self.chip, self.core = self.me // 2, lax.rem(self.me, 2)
        self.steps = chips - 1
        self.far = chips // 2
        self.next = (self.slot(1, self.core), self.slot(-1, self.core))
        self.twin = self.chip * 2 + 1 - self.core
        self.sent = []

    def chip_at(self, distance):
        return lax.rem(self.chip + distance + self.chips, self.chips)

    def slot(self, distance, which):
        return self.chip_at(distance) * 2 + which

    def copy(self, source, target, send, recv, peer):
        return pltpu.make_async_remote_copy(
            src_ref=source, dst_ref=target, send_sem=send, recv_sem=recv, device_id={self.axis: peer}
        )

    def start(self, copy):
        copy.start()
        self.sent.append(copy)

    def half_of(self, way, step):
        return step % 2 if way == 0 else 1 - step % 2


class Gather:
    def __init__(self, ring, own, blocks, sems):
        self.ring, self.own, self.blocks = ring, own, blocks
        self.send, self.recv, self.pass_send, self.pass_recv = sems
        self.half = own.shape[0] // 2

    def piece(self, way, step):
        return pl.ds(self.ring.half_of(way, step) * self.half, self.half)

    def hop(self, way, step):
        ring, piece = self.ring, self.piece(way, step)
        at = ring.slot((step // 2) * (-1 if way == 0 else 1), ring.core)
        source = self.own.at[piece] if step < 2 else self.blocks.at[at, piece]
        return ring.copy(
            source,
            self.blocks.at[at, piece],
            self.send.at[way, step],
            self.recv.at[way, step],
            ring.next[way],
        )

    def hand(self, way, step):
        ring, piece = self.ring, self.piece(way, step)
        at = ring.slot((step // 2 + 1) * (-1 if way == 0 else 1), ring.core)
        return ring.copy(
            self.blocks.at[at, piece],
            self.blocks.at[at, piece],
            self.pass_send.at[way, step],
            self.pass_recv.at[way, step],
            ring.twin,
        )

    def hand_own(self):
        ring = self.ring
        return ring.copy(
            self.own,
            self.blocks.at[ring.me],
            self.pass_send.at[0, ring.steps],
            self.pass_recv.at[0, ring.steps],
            ring.twin,
        )

    def begin(self):
        for step in (0, 1):
            for way in (0, 1):
                self.ring.start(self.hop(way, step))
        self.ring.start(self.hand_own())
        self.blocks[self.ring.me] = self.own[...]

    def advance(self, step):
        for way in (0, 1):
            self.hop(way, step).wait_recv()
            if step + 2 < self.ring.steps:
                self.ring.start(self.hop(way, step + 2))
            self.ring.start(self.hand(way, step))

    def handed(self, *steps):
        for step in steps:
            for way in (0, 1):
                self.hand(way, step).wait_recv()


class Sum:
    def __init__(self, ring, partial, other, inbox, sems):
        self.ring, self.partial, self.other, self.inbox = ring, partial, other, inbox
        self.pair_send, self.pair_recv, self.send_sem, self.recv_sem = sems
        self.half = partial.shape[1] // 2
        self.met = set()

    def pair(self, distance):
        ring = self.ring
        index = ring.chip_at(distance)
        return ring.copy(
            self.partial.at[ring.slot(distance, 1 - ring.core)],
            self.other.at[index],
            self.pair_send.at[index],
            self.pair_recv.at[index],
            ring.twin,
        )

    def give(self, *distances):
        for distance in distances:
            self.ring.start(self.pair(distance))

    def block(self, distance):
        ring = self.ring
        return ring.chip_at(distance) if self.other is None else ring.slot(distance, ring.core)

    def meet(self, distance):
        key = distance % self.ring.chips
        if self.other is not None and key not in self.met:
            self.met.add(key)
            self.pair(distance).wait_recv()

    def place(self, way, step):
        ring = self.ring
        distance = (ring.far - (step + 1) // 2) * (1 if way == 0 else -1)
        return distance, pl.ds(ring.half_of(way, step) * self.half, self.half)

    def hop(self, way, step):
        ring = self.ring
        distance, piece = self.place(way, step)
        return ring.copy(
            self.partial.at[self.block(distance), piece],
            self.inbox.at[way, step],
            self.send_sem.at[way, step],
            self.recv_sem.at[way, step],
            ring.next[way],
        )

    def both_cores(self, distance, piece):
        rows = self.partial[self.block(distance), piece, :].astype(f32)
        if self.other is None:
            return rows
        return rows + self.other[self.ring.chip_at(distance), piece, :].astype(f32)

    def advance(self, step):
        ring = self.ring
        for way in (0, 1):
            distance, piece = self.place(way, step)
            self.meet(distance)
            total = self.both_cores(distance, piece)
            if step >= 2:
                self.hop(way, step - 2).wait_recv()
                total = total + self.inbox[way, step - 2].astype(f32)
            self.partial[self.block(distance), piece, :] = total.astype(bf16)
        for way in (0, 1):
            ring.start(self.hop(way, step))

    def own_half(self, which):
        ring = self.ring
        self.meet(0)
        total = self.both_cores(0, pl.ds(which * self.half, self.half))
        for way in (0, 1):
            step = ring.steps - 2 if ring.half_of(way, ring.steps - 2) == which else ring.steps - 1
            self.hop(way, step).wait_recv()
            total = total + self.inbox[way, step].astype(f32)
        return total


class Push:
    def __init__(self, axis, count, source, target, sems, base=0):
        self.axis, self.source, self.target = axis, source, target
        self.send, self.recv = sems
        self.count, self.base = count, base
        self.me = lax.axis_index(axis)
        self.copies = []

    def begin(self):
        for k in range(1, self.count):
            peer = lax.rem(self.me + k, self.count)
            copy = pltpu.make_async_remote_copy(
                src_ref=self.source(peer),
                dst_ref=self.target.at[self.base + self.me],
                send_sem=self.send.at[k],
                recv_sem=self.recv.at[k],
                device_id={self.axis: peer},
            )
            copy.start()
            self.copies.append(copy)
        self.target[self.base + self.me] = self.source(self.me)[...]

    def arrive(self):
        for copy in self.copies:
            copy.wait_recv()

    def leave(self):
        for copy in self.copies:
            copy.wait_send()


def meet_peers(axis, count, others):
    me = lax.axis_index(axis)
    barrier = pltpu.get_barrier_semaphore()
    for k in range(1, count):
        pl.semaphore_signal(barrier, inc=1, device_id={axis: lax.rem(me + k, count)})
    for peer in others:
        pl.semaphore_signal(barrier, inc=1, device_id=peer)
    return barrier, count - 1 + len(others)


def finish_blocks(
    place, await_state, got_ref, local_ref, readout_ref, prefix_ref, start_ref, gain_ref, mixed_ref
):
    last = got_ref.shape[0] - 1
    blocks = range(prefix_ref.shape[1])

    def after(j, entry):
        await_state(j)
        moved = exact_right_dot(entry, both_heads(got_ref[j, :BLOCK, :]), NN)
        return moved + got_ref[j, BLOCK:, :].astype(f32)

    blank = jnp.zeros((BLOCK, LANES), f32)
    entry = [
        lax.fori_loop(0, place, after, blank),
        lax.fori_loop(0, last - place, lambda k, e: after(last - k, e), blank),
    ]
    gain = gain_ref[...].astype(f32)
    states = []
    for way in range(2):
        high, low = halves(entry[way])
        stacked = jnp.concatenate([high, low], axis=0)
        prefixes = [[both_heads(p) for p in halves(prefix_ref[way, b])] for b in blocks]
        boths = [raw_dot(stacked, p[0], NN) for p in prefixes]
        rests = [raw_dot(high, p[1], NN) for p in prefixes]
        states.append(
            [
                [both_heads(p) for p in halves(x[:BLOCK] + x[BLOCK:] + y + start_ref[way, b])]
                for x, y, b in zip(boths, rests, blocks)
            ]
        )
    places = [slice(b * BLOCK, (b + 1) * BLOCK) for b in blocks]
    mixes = []
    for b in blocks:
        state_high, state_low = [
            jnp.concatenate([states[0][b][k], states[1][b][k]], axis=1) for k in (0, 1)
        ]
        read_high, read_low = halves(readout_ref[places[b], :])
        both = raw_dot(jnp.concatenate([read_high, read_low], axis=0), state_high, NT)
        mixes.append(
            local_ref[places[b], :] + both[:BLOCK] + both[BLOCK:] + raw_dot(read_high, state_low, NT)
        )
    centers = [mix - head_sum(mix) * (1.0 / BLOCK) for mix in mixes]
    spreads = [head_sum(center * center) * (1.0 / BLOCK) for center in centers]
    for b in blocks:
        rows = (centers[b] * lax.rsqrt(spreads[b] + GN_EPS) * gain).astype(bf16)
        mixed_ref[b] = rows.reshape(mixed_ref.shape[1:])


def routing(routes_ref, weights_ref):
    rows = routes_ref.shape[1]
    slot = iota((rows, LANES), 1)
    names, values = [], []
    for k in range(2):
        pick = jnp.full((1, LANES), k, jnp.int32)
        names.append(to_columns(routes_ref[...].astype(f32), pick))
        values.append(to_columns(weights_ref[...], pick))
    before = (iota((rows, rows), 0) > iota((rows, rows), 1)).astype(bf16)

    def filled(expert, rank):
        named = [jnp.where(name == expert.astype(f32), 1.0, 0.0) for name in names]
        either = named[0] + named[1]
        taken = raw_dot(before, either.astype(bf16), NN)
        here = jnp.where(taken == rank.astype(f32), 1.0, 0.0)
        return either * here, (named[0] * values[0] + named[1] * values[1]) * here

    placing, weighting = filled(slot // 8 * 2 + slot % 4 // 2, slot % 2)
    late, late_weight = filled(slot % 32, jnp.full_like(slot, 2))
    high, low = halves(late_weight)
    kind = slot // 32
    info = jnp.where(
        kind == 0,
        late,
        jnp.where(kind == 1, high.astype(f32), jnp.where(kind == 2, low.astype(f32), 0.0)),
    )
    per_expert = LANES // 8 * 2
    shape = (2 * per_expert, LANES)
    at = iota(shape, 1)
    target = at % 4 // 2 * per_expert + at // 8 * 2 + at % 2
    column = at % 8 // 4
    packing = [
        jnp.where((iota(shape, 0) == target) & (column == k), 1.0, 0.0).astype(bf16) for k in range(2)
    ]
    return placing, weighting, info, packing


def late_pick(core, peers, blocks):
    row, lane = iota((peers * blocks, LANES), 0), iota((peers * blocks, LANES), 1)
    return jnp.where(lane == row // blocks * 2 + core, 1.0, 0.0).astype(bf16)


def layer_kernel(
    read_ref,
    key_ref,
    value_ref,
    erase_ref,
    decay_ref,
    spike_ref,
    gain_ref,
    mix_weight_ref,
    input_ref,
    norm_gain_ref,
    routes_ref,
    route_weights_ref,
    expert_gate,
    expert_up,
    expert_down,
    shared_gate,
    shared_up,
    shared_down,
    o_ref,
    local_ref,
    readout_ref,
    prefix_ref,
    start_ref,
    move_ref,
    carry_ref,
    whole_ref,
    got_ref,
    mixed,
    residual,
    normed,
    outgoing,
    arrived,
    packed,
    unpacked,
    returned,
    shared_blocks,
    routed_blocks,
    late_out,
    late_blocks,
    late_partial,
    late_other,
    late_back,
    late_returned,
    mix_weight_other,
    mixed_other,
    shared_chip,
    mix_partial,
    shared_partial,
    routed_partial,
    shared_other,
    routed_other,
    mix_inbox,
    shared_inbox,
    routed_inbox,
    gate,
    up,
    down,
    weight_sem,
    *sems,
    devices,
    sp_count,
):
    ring = Ring(TP, devices // 2)
    local_experts = expert_gate.shape[0]
    width = input_ref.shape[1]
    used = packed.shape[0] // local_experts
    weight_copies = []
    for k, (pair, single, into) in enumerate(
        ((expert_gate, shared_gate, gate), (expert_up, shared_up, up), (expert_down, shared_down, down))
    ):
        weight_copies.append(
            pltpu.make_async_copy(pair, into.at[pl.ds(0, local_experts)], weight_sem.at[2 * k])
        )
        weight_copies.append(
            pltpu.make_async_copy(single, into.at[local_experts], weight_sem.at[2 * k + 1])
        )
    for copy in weight_copies:
        copy.start()
    barrier, expected = meet_peers(
        SP,
        sp_count,
        [{TP: ring.next[0]}, {TP: ring.next[1]}, {TP: ring.twin}]
        + [
            {SP: lax.rem(lax.axis_index(SP) + k, sp_count), TP: ring.twin} for k in range(1, sp_count)
        ],
    )

    placing, weighting, info, packing = routing(routes_ref, route_weights_ref)
    slot = iota(placing.shape, 1)
    columns_of = [(slot % 8 // 4 == k).astype(f32) for k in range(2)]
    side = width // 2
    mixer_stage(
        read_ref,
        key_ref,
        value_ref,
        erase_ref,
        decay_ref,
        spike_ref,
        local_ref,
        readout_ref,
        prefix_ref,
        start_ref,
        move_ref,
        carry_ref,
        whole_ref,
        4,
    )
    pl.semaphore_wait(barrier, expected)
    here = lax.axis_index(SP)
    states = Push(
        SP,
        sp_count,
        lambda peer: whole_ref.at[(here + sp_count - peer) // (sp_count + 1)],
        got_ref,
        sems[24:26],
    )
    states.begin()
    twin_weight = ring.copy(
        mix_weight_ref, mix_weight_other, sems[33].at[0], sems[33].at[1], ring.twin
    )
    ring.start(twin_weight)

    def await_state(j):
        k = lax.rem(here + sp_count - j, sp_count)
        pltpu.make_async_remote_copy(
            src_ref=whole_ref.at[0],
            dst_ref=got_ref.at[j],
            send_sem=sems[24].at[k],
            recv_sem=sems[25].at[k],
            device_id={SP: j},
        ).wait_recv()

    finish_blocks(
        here, await_state, got_ref, local_ref, readout_ref, prefix_ref, start_ref, gain_ref, mixed
    )
    twin_mixed = ring.copy(
        mixed.at[:, 1 - ring.core], mixed_other, sems[33].at[2], sems[33].at[3], ring.twin
    )
    ring.start(twin_mixed)
    columns = 512
    own_rows = mix_partial.shape[0] * mix_partial.shape[1]
    twin_weight.wait_recv()
    own_mixed = mixed[:, ring.core].reshape(own_rows, LANES)
    twin_mixed.wait_recv()
    heads = jnp.concatenate([own_mixed, mixed_other[...].reshape(own_rows, LANES)], axis=1)

    def project(k, _):
        at = pl.ds(pl.multiple_of(k * columns, columns), columns)
        weight = jnp.concatenate([mix_weight_ref[:, at], mix_weight_other[:, at]], axis=0)
        product = raw_dot(heads, weight, NN).astype(bf16)
        mix_partial[:, :, at] = product.reshape(mix_partial.shape[0], mix_partial.shape[1], columns)
        return 0

    lax.fori_loop(0, width // columns, project, 0)
    mix_sum = Sum(ring, mix_partial, None, mix_inbox, sems[0:4])
    for step in range(ring.steps):
        mix_sum.advance(step)
    gains = norm_gain_ref[...].astype(f32)
    norm_gain = jnp.concatenate([gains[k : k + 1] for k in range(gains.shape[0])], axis=1)
    half = residual.shape[0] // 2
    for which in (0, 1):
        piece = slice(which * half, (which + 1) * half)
        rows = input_ref[piece, :].astype(f32) + mix_sum.own_half(which)
        residual[piece, :] = rows
        scale = lax.rsqrt(jnp.mean(rows * rows, axis=-1, keepdims=True) + RMS_EPS)
        normed[piece, :width] = (rows * scale * norm_gain).astype(bf16)
        normed[piece, width:] = info[piece, :].astype(bf16)

    shared_in = Gather(ring, normed, shared_blocks, sems[4:8])
    outgoing[...] = (
        raw_dot(
            jnp.concatenate([(placing * c).astype(bf16) for c in columns_of], axis=0),
            jnp.concatenate([normed[:, :side], normed[:, side:width]], axis=0),
            TN,
        )
        .astype(bf16)
        .reshape(outgoing.shape)
    )
    shared_in.begin()
    dispatch = Push(SP, sp_count, lambda peer: outgoing.at[peer], arrived, sems[8:10])
    dispatch.begin()
    for step in range(ring.steps - 2):
        shared_in.advance(step)
    dispatch.arrive()
    arrivals = arrived[...].reshape(LANES, side)
    packed[...] = jnp.concatenate([raw_dot(p, arrivals, NN) for p in packing], axis=1).astype(bf16)
    routed_in = Gather(ring, packed, routed_blocks, sems[10:14])
    routed_in.begin()
    shared_in.advance(ring.steps - 2)
    shared_in.advance(ring.steps - 1)

    def expert_on(blocks, partial, firsts, count, at, which):
        rows = at.size
        x = jnp.concatenate(
            [
                blocks[pl.ds(first, count), at, pl.ds(0, width)].reshape(count * rows, width)
                for first in firsts
            ],
            axis=0,
        )
        gated = raw_dot(x, gate[which], NN)
        lifted = raw_dot(x, up[which], NN)
        inner = (gated / (1.0 + jnp.exp(-gated)) * lifted).astype(bf16)
        outer = raw_dot(inner, down[which], NN).astype(bf16)
        for k, first in enumerate(firsts):
            partial[pl.ds(first, count), at, :] = outer[
                k * count * rows : (k + 1) * count * rows
            ].reshape(count, rows, width)

    def routed_on(*distances):
        firsts = [ring.chip_at(distance) * 2 for distance in distances]

        def one(k, _):
            at = pl.ds(pl.multiple_of(k * used, 16), used)
            expert_on(routed_blocks, routed_partial, firsts, 2, at, k)
            return 0

        lax.fori_loop(0, local_experts, one, 0)

    def shared_half(which):
        count = devices // 2
        at = pl.ds(0, normed.shape[0])
        expert_on(shared_blocks, shared_partial, [which * count], count, at, local_experts)

    routed_sum = Sum(ring, routed_partial, routed_other, routed_inbox, sems[14:18])
    shared_pairs = Sum(ring, shared_partial, shared_other, None, sems[18:20] + (None, None))
    shared_sum = Sum(ring, shared_chip, None, shared_inbox, (None, None) + sems[20:22])
    shared_in.hand_own().wait_recv()
    shared_in.handed(*range(ring.steps))

    block_rows = normed.shape[0]
    group_rows, late_rows = devices * block_rows, sp_count * devices
    infos = shared_blocks[:, :, pl.ds(width, LANES)].reshape(group_rows, LANES)
    order = iota((late_rows, group_rows), 0) % devices
    of_block = (
        order % ring.chips * 2 + order // ring.chips == iota((late_rows, group_rows), 1) // block_rows
    )
    chosen = jnp.where(
        of_block, raw_dot(late_pick(ring.core, sp_count, devices), infos, NT), 0.0
    ).astype(bf16)

    def choose(k, _):
        at = pl.ds(pl.multiple_of(k * columns, columns), columns)
        rows = raw_dot(chosen, shared_blocks[:, :, at].reshape(group_rows, columns), NN)
        late_out[:, :, at] = rows.astype(bf16).reshape(sp_count, devices, columns)
        return 0

    lax.fori_loop(0, width // columns, choose, 0)
    late_in = Push(
        SP, sp_count, lambda peer: late_out.at[peer], late_blocks, sems[26:28], ring.core * sp_count
    )
    late_in.begin()

    def late_hand(which):
        return ring.copy(
            late_blocks.at[which],
            late_blocks.at[which],
            sems[28].at[lax.rem(which, sp_count)],
            sems[29].at[lax.rem(which, sp_count)],
            ring.twin,
        )

    def late_handed(k):
        return late_hand((1 - ring.core) * sp_count + k)

    late_pair = ring.copy(
        late_partial.at[pl.ds((1 - ring.core) * sp_count, sp_count)],
        late_other,
        sems[30].at[0],
        sems[30].at[1],
        ring.twin,
    )
    for copy in weight_copies:
        copy.wait()

    shared_half(0)
    for step in range(ring.steps):
        routed_in.advance(step)
        if step == 0:
            shared_half(1)
        elif step == 1:
            shared_pairs.give(*range(ring.chips))
            routed_in.hand_own().wait_recv()
            routed_in.handed(0, 1)
            routed_on(0, -1, 1)
        elif step == 2:
            routed_sum.give(0, -1, 1)
        elif step % 2 == 1:
            distance = (step + 1) // 2
            routed_in.handed(step - 1, step)
            routed_on(-distance, distance)
        else:
            routed_sum.give(-(step // 2), step // 2)
    ring.start(late_hand(ring.core * sp_count + here))
    for k in range(1, sp_count):
        late_in.copies[k - 1].wait_recv()
        ring.start(late_hand(ring.core * sp_count + lax.rem(here + sp_count - k, sp_count)))
    routed_in.handed(ring.steps - 1)
    routed_on(ring.far)
    routed_sum.give(ring.far)
    routed_sum.advance(0)
    routed_sum.advance(1)
    for k in range(sp_count):
        late_handed(k).wait_recv()

    def late_on(k, _):
        expert_on(late_blocks, late_partial, [k * sp_count], sp_count, pl.ds(0, devices), k)
        return 0

    lax.fori_loop(0, local_experts, late_on, 0)
    routed_sum.advance(2)
    ring.start(late_pair)
    routed_sum.advance(3)
    late_pair.wait_recv()
    late_back[...] = (
        (
            late_partial[pl.ds(ring.core * sp_count, sp_count)].astype(f32)
            + late_other[...].astype(f32)
        )
        .reshape(late_back.shape)
        .astype(bf16)
    )
    at_home = ring.core * sp_count + here
    late_home = []
    for k in range(sp_count):
        for same in (0, 1):
            core = ring.core if same == 0 else 1 - ring.core
            peer = lax.rem(here + k, sp_count)
            if k == 0 and same == 0:
                late_returned[at_home] = late_back[here, core]
                continue
            copy = pltpu.make_async_remote_copy(
                src_ref=late_back.at[peer, core],
                dst_ref=late_returned.at[at_home],
                send_sem=sems[31].at[same, k],
                recv_sem=sems[32].at[same, k],
                device_id={SP: peer, TP: ring.chip * 2 + core},
            )
            ring.start(copy)
            late_home.append(copy)
    for step in range(4, ring.steps):
        routed_sum.advance(step)
    summed = jnp.concatenate([routed_sum.own_half(which).astype(bf16) for which in (0, 1)], axis=0)
    unpacked[...] = (
        (
            raw_dot(packing[0], summed[:, :side], TN) + raw_dot(packing[1], summed[:, side:], TN)
        )
        .astype(bf16)
        .reshape(unpacked.shape)
    )
    back = Push(SP, sp_count, lambda peer: unpacked.at[peer], returned, sems[22:24])
    back.begin()
    own_slots = [2 * k + ring.core for k in range(ring.chips)]
    own_infos = jnp.concatenate([shared_blocks[k, :, pl.ds(width, LANES)] for k in own_slots], axis=0)
    column, lane = iota((late_rows, LANES), 0), iota((late_rows, LANES), 1)
    wanted = column % LANES // ring.chips * 2 + column // LANES
    shape = (own_rows, late_rows)
    by_row = iota(shape, 0) // block_rows == iota(shape, 1) % ring.chips
    late_weights = [
        jnp.where(
            by_row,
            raw_dot(own_infos, jnp.where(lane == 32 * k + wanted, 1.0, 0.0).astype(bf16), NT),
            0.0,
        ).astype(bf16)
        for k in (1, 2)
    ]
    for k in range(ring.chips):
        shared_pairs.meet(k)
    for copy in late_home:
        copy.wait_recv()

    def add_late(k, _):
        at = pl.ds(pl.multiple_of(k * columns, columns), columns)
        rows = late_returned[:, :, at].reshape(late_rows, columns)
        own = jnp.concatenate([shared_partial[slot, :, at] for slot in own_slots], axis=0).astype(f32)
        total = (
            own
            + shared_other[:, :, at].reshape(own_rows, columns).astype(f32)
            + raw_dot(late_weights[0], rows, NN)
            + raw_dot(late_weights[1], rows, NN)
        )
        shared_chip[:, :, at] = total.astype(bf16).reshape(ring.chips, block_rows, columns)
        return 0

    lax.fori_loop(0, width // columns, add_late, 0)
    for step in range(ring.steps):
        shared_sum.advance(step)
    half = residual.shape[0] // 2
    for which in (0, 1):
        piece = slice(which * half, (which + 1) * half)
        residual[piece, :] = residual[piece, :] + shared_sum.own_half(which)
    back.arrive()
    rows = returned[...].reshape(LANES, side)
    routed = jnp.concatenate([exact_right_dot(weighting * c, rows, NN) for c in columns_of], axis=1)
    o_ref[...] = (residual[...] + routed).astype(bf16)
    for copy in ring.sent:
        copy.wait_send()
    dispatch.leave()
    back.leave()
    states.leave()
    late_in.leave()


def layer(arrays, weights, devices, sp_count, capacity, room, number, name):
    tokens = arrays[1].shape[0]
    rows, width = arrays[8].shape
    hidden = weights[3].shape[1]
    local_experts = weights[0].shape[0]
    packed_rows = sp_count * local_experts * capacity
    block_count = tokens // BLOCK
    chips = devices // 2
    steps = chips - 1
    dma = pltpu.SemaphoreType.DMA
    anywhere = pl.BlockSpec(memory_space=pl.ANY)
    buffer = lambda *shape: pltpu.VMEM(shape, bf16)
    gather_sems = [dma((2, steps)), dma((2, steps)), dma((2, steps + 1)), dma((2, steps + 1))]
    sum_sems = [dma((chips,)), dma((chips,)), dma((2, steps)), dma((2, steps))]
    push_sems = [dma((sp_count,)), dma((sp_count,))]
    return pl.pallas_call(
        functools.partial(layer_kernel, devices=devices, sp_count=sp_count),
        name=name,
        out_shape=jax.ShapeDtypeStruct((rows, width), bf16),
        in_specs=[VMEM] * 12 + [anywhere] * 6,
        out_specs=VMEM,
        scratch_shapes=[
            pltpu.VMEM((tokens, LANES), f32),
            pltpu.VMEM((tokens, 2 * LANES), f32),
            pltpu.VMEM((2, block_count, BLOCK, LANES), f32),
            pltpu.VMEM((2, block_count, BLOCK, LANES), f32),
            pltpu.VMEM((2, block_count, LANES, LANES), f32),
            pltpu.VMEM((2, block_count, BLOCK, LANES), f32),
            buffer(2, 2 * BLOCK, LANES),
            buffer(sp_count, 2 * BLOCK, LANES),
            buffer(chips, 2, rows, LANES),
            pltpu.VMEM((rows, width), f32),
            buffer(rows, width + LANES),
            buffer(sp_count, room, width // 2),
            buffer(sp_count, room, width // 2),
            buffer(packed_rows, width),
            buffer(sp_count, room, width // 2),
            buffer(sp_count, room, width // 2),
            buffer(devices, rows, width + LANES),
            buffer(devices, packed_rows, width),
            buffer(sp_count, devices, width),
            buffer(local_experts * sp_count, devices, width),
            buffer(local_experts * sp_count, devices, width),
            buffer(sp_count, devices, width),
            buffer(sp_count, 2, chips, width),
            buffer(2 * sp_count, chips, width),
            buffer(LANES, width),
            buffer(chips, rows, LANES),
            buffer(chips, rows, width),
            buffer(chips, rows, width),
            buffer(devices, rows, width),
            buffer(devices, packed_rows, width),
            buffer(chips, rows, width),
            buffer(chips, packed_rows, width),
            buffer(2, steps, rows // 2, width),
            buffer(2, steps, rows // 2, width),
            buffer(2, steps, packed_rows // 2, width),
            buffer(local_experts + 1, width, hidden),
            buffer(local_experts + 1, width, hidden),
            buffer(local_experts + 1, hidden, width),
            dma((6,)),
        ]
        + sum_sems
        + gather_sems
        + push_sems
        + gather_sems
        + sum_sems
        + sum_sems
        + push_sems
        + push_sems
        + push_sems
        + push_sems
        + [dma((2,)), dma((2, sp_count)), dma((2, sp_count)), dma((4,))],
        compiler_params=pltpu.CompilerParams(
            collective_id=number, has_side_effects=True, vmem_limit_bytes=62 * 1024 * 1024
        ),
    )(*arrays, *weights)


def body(
    layer_input,
    receptance,
    keys,
    values,
    erase_preact,
    decay_preact,
    decay_spike,
    head_norm_gain,
    output_weight,
    expert_norm_gain,
    routes,
    routing_weight,
    expert_gate_weight,
    expert_up_weight,
    expert_down_weight,
    shared_gate_weight,
    shared_up_weight,
    shared_down_weight,
):
    sp_count, tp_count = lax.axis_size(SP), lax.axis_size(TP)
    return layer(
        (
            receptance,
            keys,
            values,
            erase_preact,
            decay_preact,
            decay_spike.T,
            head_norm_gain.reshape(1, -1),
            output_weight,
            layer_input,
            expert_norm_gain.reshape(-1, LANES),
            routes.T,
            routing_weight.T,
        ),
        (
            expert_gate_weight,
            expert_up_weight,
            expert_down_weight,
            shared_gate_weight,
            shared_up_weight,
            shared_down_weight,
        ),
        tp_count,
        sp_count,
        2,
        8,
        0,
        "layer",
    )


def solution(mesh):
    both = (SP, TP)
    in_specs = (
        P(both, None),
        P(SP, TP),
        P(SP, TP),
        P(SP, TP),
        P(SP, TP),
        P(SP, TP),
        P(SP, TP),
        P(TP),
        P(TP, None),
        P(),
        P(both, None),
        P(both, None),
        P(SP, None, TP),
        P(SP, None, TP),
        P(SP, TP, None),
        P(None, TP),
        P(None, TP),
        P(TP, None),
    )
    return jax.shard_map(
        body, mesh=mesh, in_specs=in_specs, out_specs=P(both, None), check_vma=False
    )
```

```python
import functools

import jax
import jax.numpy as jnp
from jax import lax
from jax.experimental import pallas as pl
from jax.experimental.pallas import tpu as pltpu
from jax.sharding import PartitionSpec as P

SP = "sp"
TP = "tp"
BLOCK = 64
LANES = 128
GN_EPS = 0.00064
RMS_EPS = 1e-06
f32 = jnp.float32
bf16 = jnp.bfloat16
VMEM = pl.BlockSpec(memory_space=pltpu.VMEM)
NN = (((1,), (0,)), ((), ()))
NT = (((1,), (1,)), ((), ()))
TN = (((0,), (0,)), ((), ()))


def iota(shape, dim):
    return lax.broadcasted_iota(jnp.int32, shape, dim)


def halves(array):
    high = array.astype(bf16)
    return high, (array - high.astype(f32)).astype(bf16)


def raw_dot(left, right, dims):
    return lax.dot_general(left, right, dims, preferred_element_type=f32)


def head_mask(count, dtype):
    first = (iota((count, LANES), 1) < BLOCK).astype(f32)
    return first.astype(dtype), (1.0 - first).astype(dtype)


def both_heads(rows):
    first, second = head_mask(rows.shape[0], rows.dtype)
    return jnp.concatenate([rows * first, rows * second], axis=0)


def fine_dot(left, right, dims, spread=False):
    left_high, left_low = halves(left)
    right_high, right_low = halves(right)
    if spread:
        right_high, right_low = both_heads(right_high), both_heads(right_low)
    if dims == TN:
        return raw_dot(
            jnp.concatenate([left_high, left_high, left_low], axis=0),
            jnp.concatenate([right_high, right_low, right_high], axis=0),
            TN,
        )
    count = left.shape[0]
    both = raw_dot(jnp.concatenate([left_high, left_low], axis=0), right_high, dims)
    return both[:count] + both[count:] + raw_dot(left_high, right_low, dims)


def exact_right_dot(left, right, dims):
    left_high, left_low = halves(left)
    count = left.shape[0]
    both = raw_dot(jnp.concatenate([left_high, left_low], axis=0), right, dims)
    return both[:count] + both[count:]


def head_sum(rows):
    ones = (iota((LANES, LANES), 0) // BLOCK == iota((LANES, LANES), 1) // BLOCK).astype(bf16)
    return exact_right_dot(rows, ones, NN)


def block_sums(log_decay):
    high, middle, low = three_parts(log_decay)
    count = log_decay.shape[0]
    ones = (iota((count, count), 0) >= iota((count, count), 1)).astype(bf16)
    width = log_decay.shape[1]
    sums = raw_dot(ones, jnp.concatenate([high, middle, low], axis=1), NN)
    return sums[:, :width] + sums[:, width : 2 * width] + sums[:, 2 * width :]


def inverses(stricts):
    row, lane = iota((BLOCK, LANES), 0), iota((BLOCK, LANES), 1) % BLOCK

    def within(size):
        return row // size == lane // size

    def products(lefts, rights):
        return [fine_dot(left, right, NN, spread=True) for left, right in zip(lefts, rights)]

    smalls = [jnp.where(within(8), strict, 0.0) for strict in stricts]
    starts = [jnp.where(row == lane, 1.0, 0.0) - small for small in smalls]
    squares = products(smalls, smalls)
    boths = products([jnp.concatenate(p, axis=0) for p in zip(starts, squares)], squares)
    results = [start + both[:BLOCK] for start, both in zip(starts, boths)]
    more = products(results, [both[BLOCK:] for both in boths])
    results = [r + m for r, m in zip(results, more)]
    for size in (8, 16, 32):
        keep = within(2 * size) & ~within(size)
        edges = products(results, [jnp.where(keep, strict, 0.0) for strict in stricts])
        more = products(edges, results)
        results = [r - m for r, m in zip(results, more)]
    return results


def block_terms(chains):
    row, lane = iota((BLOCK, LANES), 0), iota((BLOCK, LANES), 1) % BLOCK
    scaled, pairs = [], []
    for unit, beta, key_rows, _, read, left_unit, left_read, right, _, _ in chains:
        scaled.append((unit * left_unit, read * left_read, beta * right, key_rows * right))
    for unit_mid, read_mid, beta_mid, key_mid in scaled:
        left_high, left_low = halves(jnp.concatenate([unit_mid, read_mid], axis=0))
        right_high, right_low = [
            jnp.concatenate([both_heads(b), both_heads(k)], axis=0)
            for b, k in zip(halves(beta_mid), halves(key_mid))
        ]
        both = raw_dot(jnp.concatenate([left_high, left_low], axis=0), right_high, NT)
        pairs.append(both[: 2 * BLOCK] + both[2 * BLOCK :] + raw_dot(left_high, right_low, NT))
    erase_betas, keyeds, read_betas = [], [], []
    for pair, chain in zip(pairs, chains):
        strict = row > lane if chain[-1] else row < lane
        upto = row >= lane if chain[-1] else row <= lane
        erase_betas.append(jnp.where(strict, pair[:BLOCK, :LANES], 0.0))
        erase_key = jnp.where(strict, pair[:BLOCK, LANES:], 0.0)
        read_betas.append(jnp.where(upto, pair[BLOCK:, :LANES], 0.0))
        read_key = jnp.where(upto, pair[BLOCK:, LANES:], 0.0)
        keyeds.append(
            exact_right_dot(jnp.concatenate([erase_key, read_key], axis=0), chain[3], NN)
        )
    solvers = inverses(erase_betas)
    solved = []
    for solver, (unit_mid, _, _, _), keyed, chain in zip(solvers, scaled, keyeds, chains):
        solver_high, solver_low = halves(solver)
        right_high, right_low = [
            jnp.concatenate([both_heads(u), both_heads(k)], axis=1)
            for u, k in zip(halves(unit_mid * chain[8]), halves(-keyed[:BLOCK]))
        ]
        both = raw_dot(jnp.concatenate([solver_high, solver_low], axis=0), right_high, NN)
        solved.append(both[:BLOCK] + both[BLOCK:] + raw_dot(solver_high, right_low, NN))
    terms = []
    for found, read_beta, keyed, scale, chain in zip(solved, read_betas, keyeds, scaled, chains):
        spread_parts = [
            jnp.concatenate([both_heads(p[:, :LANES]), both_heads(p[:, LANES:])], axis=1)
            for p in halves(found)
        ]
        read_high, read_low = halves(read_beta)
        both = raw_dot(jnp.concatenate([read_high, read_low], axis=0), spread_parts[0], NN)
        applied = both[:BLOCK] + both[BLOCK:] + raw_dot(read_high, spread_parts[1], NN)
        readout = scale[1] * chain[8] - applied[:, :LANES]
        local = applied[:, LANES:] + keyed[BLOCK:]
        terms.append((found, scale[2] * chain[8], scale[3] * chain[8], readout, local))
    return terms


def three_parts(array):
    high = array.astype(bf16)
    rest = array - high.astype(f32)
    middle = rest.astype(bf16)
    return high, middle, (rest - middle.astype(f32)).astype(bf16)


def to_columns(rows, pick):
    chosen = [(pick == k).astype(bf16) for k in range(2)]
    parts = three_parts(rows)
    return raw_dot(
        jnp.concatenate(parts, axis=0), jnp.concatenate([jnp.concatenate(chosen, axis=0)] * 3, axis=0), TN
    )


def mixer_stage(
    read_ref,
    key_ref,
    value_ref,
    erase_ref,
    decay_ref,
    spike_ref,
    local_ref,
    readout_ref,
    prefix_ref,
    start_ref,
    move_ref,
    carry_ref,
    whole_ref,
    together,
):
    tokens = key_ref.shape[0]
    block_count = tokens // BLOCK
    same_head = iota((LANES, LANES), 0) // BLOCK == iota((LANES, LANES), 1) // BLOCK
    diagonal = iota((LANES, LANES), 0) == iota((LANES, LANES), 1)

    def some_blocks(index):
        blocks = [index * together + k for k in range(together)]
        span = together * BLOCK
        spikes = to_columns(
            spike_ref[:, pl.ds(pl.multiple_of(index * span, span), span)],
            iota((1, LANES), 1) // BLOCK,
        )
        chains, totals, values = [], [], []
        places = [pl.ds(pl.multiple_of(block * BLOCK, BLOCK), BLOCK) for block in blocks]
        for k, at in enumerate(places):
            key_rows = key_ref[at, :].astype(f32)
            read = read_ref[at, :].astype(f32)
            value = value_ref[at, :]
            unit = key_rows * lax.rsqrt(head_sum(key_rows * key_rows) + 1e-06)
            beta = unit * jax.nn.sigmoid(erase_ref[at, :].astype(f32))
            decay_in = decay_ref[at, :].astype(f32)
            spike = spikes[k * BLOCK : (k + 1) * BLOCK]
            log_decay = -jnp.exp(-jax.nn.softplus(-decay_in) - 0.5) + spike
            upto = block_sums(log_decay)
            total = upto[BLOCK - 1 :, :]
            middle = 0.5 * total
            ahead = upto - log_decay
            before, after = jnp.exp(ahead - middle), jnp.exp(upto - middle)
            until, since = jnp.exp(middle - upto), jnp.exp(middle - ahead)
            edge = jnp.exp(middle)
            shared = (unit, beta, key_rows, both_heads(value), read)
            chains.append(shared + (before, after, until, edge, True))
            chains.append(shared + (until, since, before, edge, False))
            totals.append(total)
            values.append(value)
        terms = block_terms(chains)
        for k, at in enumerate(places):
            local_ref[at, :] = terms[2 * k][4] + terms[2 * k + 1][4]
        for k, (solved, beta_end, key_end, readout, _) in enumerate(terms):
            way, at, value = k % 2, places[k // 2], values[k // 2]
            readout_ref[at, way * LANES : (way + 1) * LANES] = readout
            moved = fine_dot(solved, beta_end, TN)
            key_high, key_low = halves(key_end)
            keyed = raw_dot(
                jnp.concatenate([value, value], axis=0),
                jnp.concatenate([key_high, key_low], axis=0),
                TN,
            )
            move_ref[way, blocks[k // 2]] = jnp.where(
                same_head, jnp.where(diagonal, jnp.exp(totals[k // 2]), 0.0) - moved[:LANES], 0.0
            )
            carry = jnp.where(same_head, moved[LANES:] + keyed, 0.0)
            carry_ref[way, blocks[k // 2]] = carry[:BLOCK] + carry[BLOCK:]

    def step(index, _):
        some_blocks(index)
        return 0

    lax.fori_loop(0, block_count // together, step, 0)
    identity = jnp.where(iota((BLOCK, LANES), 0) == iota((BLOCK, LANES), 1) % BLOCK, 1.0, 0.0)
    running = [jnp.concatenate([identity, jnp.zeros_like(identity)], axis=0)] * 2
    for k in range(block_count):
        for way in range(2):
            block = k if way == 0 else block_count - 1 - k
            now = running[way]
            prefix_ref[way, block] = now[:BLOCK]
            start_ref[way, block] = now[BLOCK:]
            after = fine_dot(now, move_ref[way, block], NN)
            running[way] = jnp.concatenate(
                [after[:BLOCK], after[BLOCK:] + carry_ref[way, block]], axis=0
            )
    for way in range(2):
        whole_ref[way] = running[way].astype(bf16)


class Ring:
    def __init__(self, axis, chips):
        self.axis, self.chips = axis, chips
        self.me = lax.axis_index(axis)
        self.chip, self.core = self.me // 2, lax.rem(self.me, 2)
        self.steps = chips - 1
        self.far = chips // 2
        self.next = (self.slot(1, self.core), self.slot(-1, self.core))
        self.twin = self.chip * 2 + 1 - self.core
        self.sent = []

    def chip_at(self, distance):
        return lax.rem(self.chip + distance + self.chips, self.chips)

    def slot(self, distance, which):
        return self.chip_at(distance) * 2 + which

    def copy(self, source, target, send, recv, peer):
        return pltpu.make_async_remote_copy(
            src_ref=source, dst_ref=target, send_sem=send, recv_sem=recv, device_id={self.axis: peer}
        )

    def start(self, copy):
        copy.start()
        self.sent.append(copy)

    def half_of(self, way, step):
        return step % 2 if way == 0 else 1 - step % 2


PARTS = 2


def column_parts(width):
    side = width // LANES // PARTS * LANES
    return [pl.ds(0, side), pl.ds(side, width - side)]


class Gather:
    def __init__(self, ring, own, blocks, sems):
        self.ring, self.own, self.blocks = ring, own, blocks
        self.send, self.recv, self.pass_send, self.pass_recv = sems
        self.half = own.shape[0] // 2
        self.columns = column_parts(own.shape[1])

    def piece(self, way, step):
        return pl.ds(self.ring.half_of(way, step) * self.half, self.half)

    def hop(self, way, step, part):
        ring, piece, columns = self.ring, self.piece(way, step), self.columns[part]
        at = ring.slot((step // 2) * (-1 if way == 0 else 1), ring.core)
        source = self.own.at[piece, columns] if step < 2 else self.blocks.at[at, piece, columns]
        return ring.copy(
            source,
            self.blocks.at[at, piece, columns],
            self.send.at[way, step * PARTS + part],
            self.recv.at[way, step * PARTS + part],
            ring.next[way],
        )

    def hand(self, way, step, part):
        ring, piece, columns = self.ring, self.piece(way, step), self.columns[part]
        at = ring.slot((step // 2 + 1) * (-1 if way == 0 else 1), ring.core)
        return ring.copy(
            self.blocks.at[at, piece, columns],
            self.blocks.at[at, piece, columns],
            self.pass_send.at[way, step * PARTS + part],
            self.pass_recv.at[way, step * PARTS + part],
            ring.twin,
        )

    def hand_own(self):
        ring = self.ring
        return ring.copy(
            self.own,
            self.blocks.at[ring.me],
            self.pass_send.at[0, ring.steps * PARTS],
            self.pass_recv.at[0, ring.steps * PARTS],
            ring.twin,
        )

    def begin(self):
        for step in (0, 1):
            for part in range(PARTS):
                for way in (0, 1):
                    self.ring.start(self.hop(way, step, part))
        self.ring.start(self.hand_own())
        self.blocks[self.ring.me] = self.own[...]

    def advance(self, step):
        for part in range(PARTS):
            for way in (0, 1):
                self.hop(way, step, part).wait_recv()
                if step + 2 < self.ring.steps:
                    self.ring.start(self.hop(way, step + 2, part))
                self.ring.start(self.hand(way, step, part))

    def handed(self, *steps):
        for step in steps:
            for part in range(PARTS):
                for way in (0, 1):
                    self.hand(way, step, part).wait_recv()


class Sum:
    def __init__(self, ring, partial, other, inbox, sems):
        self.ring, self.partial, self.other, self.inbox = ring, partial, other, inbox
        self.pair_send, self.pair_recv, self.send_sem, self.recv_sem = sems
        self.half = partial.shape[1] // 2
        self.columns = column_parts(partial.shape[2])
        self.met = set()

    def pair(self, distance):
        ring = self.ring
        index = ring.chip_at(distance)
        return ring.copy(
            self.partial.at[ring.slot(distance, 1 - ring.core)],
            self.other.at[index],
            self.pair_send.at[index],
            self.pair_recv.at[index],
            ring.twin,
        )

    def give(self, *distances):
        for distance in distances:
            self.ring.start(self.pair(distance))

    def block(self, distance):
        ring = self.ring
        return ring.chip_at(distance) if self.other is None else ring.slot(distance, ring.core)

    def meet(self, distance):
        key = distance % self.ring.chips
        if self.other is not None and key not in self.met:
            self.met.add(key)
            self.pair(distance).wait_recv()

    def place(self, way, step):
        ring = self.ring
        distance = (ring.far - (step + 1) // 2) * (1 if way == 0 else -1)
        return distance, pl.ds(ring.half_of(way, step) * self.half, self.half)

    def hop(self, way, step, part):
        ring = self.ring
        distance, piece = self.place(way, step)
        columns = self.columns[part]
        return ring.copy(
            self.partial.at[self.block(distance), piece, columns],
            self.inbox.at[way, step, :, columns],
            self.send_sem.at[way, step * PARTS + part],
            self.recv_sem.at[way, step * PARTS + part],
            ring.next[way],
        )

    def both_cores(self, distance, piece, columns):
        rows = self.partial[self.block(distance), piece, columns].astype(f32)
        if self.other is None:
            return rows
        return rows + self.other[self.ring.chip_at(distance), piece, columns].astype(f32)

    def advance(self, step):
        ring = self.ring
        for part, columns in enumerate(self.columns):
            for way in (0, 1):
                distance, piece = self.place(way, step)
                self.meet(distance)
                if step >= 2 or self.other is not None:
                    total = self.both_cores(distance, piece, columns)
                    if step >= 2:
                        self.hop(way, step - 2, part).wait_recv()
                        total = total + self.inbox[way, step - 2, :, columns].astype(f32)
                    self.partial[self.block(distance), piece, columns] = total.astype(bf16)
            for way in (0, 1):
                ring.start(self.hop(way, step, part))

    def own_half(self, which):
        ring = self.ring
        self.meet(0)
        totals = []
        for part, columns in enumerate(self.columns):
            total = self.both_cores(0, pl.ds(which * self.half, self.half), columns)
            for way in (0, 1):
                even = ring.half_of(way, ring.steps - 2) == which
                step = ring.steps - 2 if even else ring.steps - 1
                self.hop(way, step, part).wait_recv()
                total = total + self.inbox[way, step, :, columns].astype(f32)
            totals.append(total)
        return jnp.concatenate(totals, axis=1)


class Push:
    def __init__(self, axis, count, source, target, sems, base=0):
        self.axis, self.source, self.target = axis, source, target
        self.send, self.recv = sems
        self.count, self.base = count, base
        self.me = lax.axis_index(axis)
        self.copies = []

    def begin(self):
        for k in range(1, self.count):
            peer = lax.rem(self.me + k, self.count)
            copy = pltpu.make_async_remote_copy(
                src_ref=self.source(peer),
                dst_ref=self.target.at[self.base + self.me],
                send_sem=self.send.at[k],
                recv_sem=self.recv.at[k],
                device_id={self.axis: peer},
            )
            copy.start()
            self.copies.append(copy)
        self.target[self.base + self.me] = self.source(self.me)[...]

    def arrive(self):
        for copy in self.copies:
            copy.wait_recv()

    def leave(self):
        for copy in self.copies:
            copy.wait_send()


def meet_peers(axis, count, others):
    me = lax.axis_index(axis)
    barrier = pltpu.get_barrier_semaphore()
    for k in range(1, count):
        pl.semaphore_signal(barrier, inc=1, device_id={axis: lax.rem(me + k, count)})
    for peer in others:
        pl.semaphore_signal(barrier, inc=1, device_id=peer)
    return barrier, count - 1 + len(others)


def finish_blocks(
    place, await_state, got_ref, local_ref, readout_ref, prefix_ref, start_ref, gain_ref, mixed_ref
):
    last = got_ref.shape[0] - 1
    blocks = range(prefix_ref.shape[1])

    def after(j, entry):
        await_state(j)
        moved = exact_right_dot(entry, both_heads(got_ref[j, :BLOCK, :]), NN)
        return moved + got_ref[j, BLOCK:, :].astype(f32)

    blank = jnp.zeros((BLOCK, LANES), f32)
    entry = [
        lax.fori_loop(0, place, after, blank),
        lax.fori_loop(0, last - place, lambda k, e: after(last - k, e), blank),
    ]
    gain = gain_ref[...].astype(f32)
    states = []
    for way in range(2):
        high, low = halves(entry[way])
        stacked = jnp.concatenate([high, low], axis=0)
        prefixes = [[both_heads(p) for p in halves(prefix_ref[way, b])] for b in blocks]
        boths = [raw_dot(stacked, p[0], NN) for p in prefixes]
        rests = [raw_dot(high, p[1], NN) for p in prefixes]
        states.append(
            [
                [both_heads(p) for p in halves(x[:BLOCK] + x[BLOCK:] + y + start_ref[way, b])]
                for x, y, b in zip(boths, rests, blocks)
            ]
        )
    places = [slice(b * BLOCK, (b + 1) * BLOCK) for b in blocks]
    mixes = []
    for b in blocks:
        state_high, state_low = [
            jnp.concatenate([states[0][b][k], states[1][b][k]], axis=1) for k in (0, 1)
        ]
        read_high, read_low = halves(readout_ref[places[b], :])
        both = raw_dot(jnp.concatenate([read_high, read_low], axis=0), state_high, NT)
        mixes.append(
            local_ref[places[b], :] + both[:BLOCK] + both[BLOCK:] + raw_dot(read_high, state_low, NT)
        )
    centers = [mix - head_sum(mix) * (1.0 / BLOCK) for mix in mixes]
    spreads = [head_sum(center * center) * (1.0 / BLOCK) for center in centers]
    for b in blocks:
        rows = (centers[b] * lax.rsqrt(spreads[b] + GN_EPS) * gain).astype(bf16)
        mixed_ref[b] = rows.reshape(mixed_ref.shape[1:])


def routing(routes_ref, weights_ref):
    rows = routes_ref.shape[1]
    slot = iota((rows, LANES), 1)
    names, values = [], []
    for k in range(2):
        pick = jnp.full((1, LANES), k, jnp.int32)
        names.append(to_columns(routes_ref[...].astype(f32), pick))
        values.append(to_columns(weights_ref[...], pick))
    before = (iota((rows, rows), 0) > iota((rows, rows), 1)).astype(bf16)

    def filled(expert, rank):
        named = [jnp.where(name == expert.astype(f32), 1.0, 0.0) for name in names]
        either = named[0] + named[1]
        taken = raw_dot(before, either.astype(bf16), NN)
        here = jnp.where(taken == rank.astype(f32), 1.0, 0.0)
        return either * here, (named[0] * values[0] + named[1] * values[1]) * here

    placing, weighting = filled(slot // 8 * 2 + slot % 4 // 2, slot % 2)
    late, late_weight = filled(slot % 32, jnp.full_like(slot, 2))
    high, low = halves(late_weight)
    kind = slot // 32
    info = jnp.where(
        kind == 0,
        late,
        jnp.where(kind == 1, high.astype(f32), jnp.where(kind == 2, low.astype(f32), 0.0)),
    )
    per_expert = LANES // 8 * 2
    shape = (2 * per_expert, LANES)
    at = iota(shape, 1)
    target = at % 4 // 2 * per_expert + at // 8 * 2 + at % 2
    column = at % 8 // 4
    packing = [
        jnp.where((iota(shape, 0) == target) & (column == k), 1.0, 0.0).astype(bf16) for k in range(2)
    ]
    return placing, weighting, info, packing


def late_pick(core, peers, blocks):
    row, lane = iota((peers * blocks, LANES), 0), iota((peers * blocks, LANES), 1)
    return jnp.where(lane == row // blocks * 2 + core, 1.0, 0.0).astype(bf16)


def layer_kernel(
    read_ref,
    key_ref,
    value_ref,
    erase_ref,
    decay_ref,
    spike_ref,
    gain_ref,
    mix_weight_ref,
    input_ref,
    norm_gain_ref,
    routes_ref,
    route_weights_ref,
    expert_gate,
    expert_up,
    expert_down,
    shared_gate,
    shared_up,
    shared_down,
    o_ref,
    local_ref,
    readout_ref,
    prefix_ref,
    start_ref,
    move_ref,
    carry_ref,
    whole_ref,
    got_ref,
    mixed,
    residual,
    normed,
    outgoing,
    arrived,
    packed,
    unpacked,
    returned,
    shared_blocks,
    routed_blocks,
    late_out,
    late_blocks,
    late_partial,
    late_other,
    late_back,
    late_returned,
    mix_weight_other,
    mixed_other,
    shared_chip,
    mix_partial,
    shared_partial,
    routed_partial,
    shared_other,
    routed_other,
    mix_inbox,
    shared_inbox,
    routed_inbox,
    gate,
    up,
    down,
    weight_sem,
    *sems,
    devices,
    sp_count,
):
    ring = Ring(TP, devices // 2)
    local_experts = expert_gate.shape[0]
    width = input_ref.shape[1]
    used = packed.shape[0] // local_experts
    weight_copies = []
    for k, (pair, single, into) in enumerate(
        ((expert_gate, shared_gate, gate), (expert_up, shared_up, up), (expert_down, shared_down, down))
    ):
        weight_copies.append(
            pltpu.make_async_copy(pair, into.at[pl.ds(0, local_experts)], weight_sem.at[2 * k])
        )
        weight_copies.append(
            pltpu.make_async_copy(single, into.at[local_experts], weight_sem.at[2 * k + 1])
        )
    for copy in weight_copies:
        copy.start()
    barrier, expected = meet_peers(
        SP,
        sp_count,
        [{TP: ring.next[0]}, {TP: ring.next[1]}, {TP: ring.twin}]
        + [
            {SP: lax.rem(lax.axis_index(SP) + k, sp_count), TP: ring.twin} for k in range(1, sp_count)
        ],
    )

    placing, weighting, info, packing = routing(routes_ref, route_weights_ref)
    slot = iota(placing.shape, 1)
    columns_of = [(slot % 8 // 4 == k).astype(f32) for k in range(2)]
    side = width // 2
    mixer_stage(
        read_ref,
        key_ref,
        value_ref,
        erase_ref,
        decay_ref,
        spike_ref,
        local_ref,
        readout_ref,
        prefix_ref,
        start_ref,
        move_ref,
        carry_ref,
        whole_ref,
        4,
    )
    pl.semaphore_wait(barrier, expected)
    here = lax.axis_index(SP)
    states = Push(
        SP,
        sp_count,
        lambda peer: whole_ref.at[(here + sp_count - peer) // (sp_count + 1)],
        got_ref,
        sems[24:26],
    )
    states.begin()
    twin_weight = ring.copy(
        mix_weight_ref, mix_weight_other, sems[33].at[0], sems[33].at[1], ring.twin
    )
    ring.start(twin_weight)

    def await_state(j):
        k = lax.rem(here + sp_count - j, sp_count)
        pltpu.make_async_remote_copy(
            src_ref=whole_ref.at[0],
            dst_ref=got_ref.at[j],
            send_sem=sems[24].at[k],
            recv_sem=sems[25].at[k],
            device_id={SP: j},
        ).wait_recv()

    finish_blocks(
        here, await_state, got_ref, local_ref, readout_ref, prefix_ref, start_ref, gain_ref, mixed
    )
    twin_mixed = ring.copy(
        mixed.at[:, 1 - ring.core], mixed_other, sems[33].at[2], sems[33].at[3], ring.twin
    )
    ring.start(twin_mixed)
    columns = 512
    own_rows = mix_partial.shape[0] * mix_partial.shape[1]
    twin_weight.wait_recv()
    own_mixed = mixed[:, ring.core].reshape(own_rows, LANES)
    twin_mixed.wait_recv()
    heads = jnp.concatenate([own_mixed, mixed_other[...].reshape(own_rows, LANES)], axis=1)

    def project(k, _):
        at = pl.ds(pl.multiple_of(k * columns, columns), columns)
        weight = jnp.concatenate([mix_weight_ref[:, at], mix_weight_other[:, at]], axis=0)
        product = raw_dot(heads, weight, NN).astype(bf16)
        mix_partial[:, :, at] = product.reshape(mix_partial.shape[0], mix_partial.shape[1], columns)
        return 0

    lax.fori_loop(0, width // columns, project, 0)
    mix_sum = Sum(ring, mix_partial, None, mix_inbox, sems[0:4])
    for step in range(ring.steps):
        mix_sum.advance(step)
    gains = norm_gain_ref[...].astype(f32)
    norm_gain = jnp.concatenate([gains[k : k + 1] for k in range(gains.shape[0])], axis=1)
    half = residual.shape[0] // 2
    for which in (0, 1):
        piece = slice(which * half, (which + 1) * half)
        rows = input_ref[piece, :].astype(f32) + mix_sum.own_half(which)
        residual[piece, :] = rows
        scale = lax.rsqrt(jnp.mean(rows * rows, axis=-1, keepdims=True) + RMS_EPS)
        normed[piece, :width] = (rows * scale * norm_gain).astype(bf16)
        normed[piece, width:] = info[piece, :].astype(bf16)

    shared_in = Gather(ring, normed, shared_blocks, sems[4:8])
    outgoing[...] = (
        raw_dot(
            jnp.concatenate([(placing * c).astype(bf16) for c in columns_of], axis=0),
            jnp.concatenate([normed[:, :side], normed[:, side:width]], axis=0),
            TN,
        )
        .astype(bf16)
        .reshape(outgoing.shape)
    )
    shared_in.begin()
    dispatch = Push(SP, sp_count, lambda peer: outgoing.at[peer], arrived, sems[8:10])
    dispatch.begin()
    for step in range(ring.steps - 2):
        shared_in.advance(step)
    dispatch.arrive()
    arrivals = arrived[...].reshape(LANES, side)
    packed[...] = jnp.concatenate([raw_dot(p, arrivals, NN) for p in packing], axis=1).astype(bf16)
    routed_in = Gather(ring, packed, routed_blocks, sems[10:14])
    routed_in.begin()
    shared_in.advance(ring.steps - 2)
    shared_in.advance(ring.steps - 1)

    def expert_on(blocks, partial, firsts, count, at, which):
        rows = at.size
        x = jnp.concatenate(
            [
                blocks[pl.ds(first, count), at, pl.ds(0, width)].reshape(count * rows, width)
                for first in firsts
            ],
            axis=0,
        )
        gated = raw_dot(x, gate[which], NN)
        lifted = raw_dot(x, up[which], NN)
        inner = (gated / (1.0 + jnp.exp(-gated)) * lifted).astype(bf16)
        outer = raw_dot(inner, down[which], NN).astype(bf16)
        for k, first in enumerate(firsts):
            partial[pl.ds(first, count), at, :] = outer[
                k * count * rows : (k + 1) * count * rows
            ].reshape(count, rows, width)

    def routed_on(*distances):
        firsts = [ring.chip_at(distance) * 2 for distance in distances]

        def one(k, _):
            at = pl.ds(pl.multiple_of(k * used, 16), used)
            expert_on(routed_blocks, routed_partial, firsts, 2, at, k)
            return 0

        lax.fori_loop(0, local_experts, one, 0)

    def shared_half(which):
        count = devices // 2
        at = pl.ds(0, normed.shape[0])
        expert_on(shared_blocks, shared_partial, [which * count], count, at, local_experts)

    routed_sum = Sum(ring, routed_partial, routed_other, routed_inbox, sems[14:18])
    shared_pairs = Sum(ring, shared_partial, shared_other, None, sems[18:20] + (None, None))
    shared_sum = Sum(ring, shared_chip, None, shared_inbox, (None, None) + sems[20:22])
    shared_in.hand_own().wait_recv()
    shared_in.handed(*range(ring.steps))

    block_rows = normed.shape[0]
    group_rows, late_rows = devices * block_rows, sp_count * devices
    infos = shared_blocks[:, :, pl.ds(width, LANES)].reshape(group_rows, LANES)
    order = iota((late_rows, group_rows), 0) % devices
    of_block = (
        order % ring.chips * 2 + order // ring.chips == iota((late_rows, group_rows), 1) // block_rows
    )
    chosen = jnp.where(
        of_block, raw_dot(late_pick(ring.core, sp_count, devices), infos, NT), 0.0
    ).astype(bf16)

    def choose(k, _):
        at = pl.ds(pl.multiple_of(k * columns, columns), columns)
        rows = raw_dot(chosen, shared_blocks[:, :, at].reshape(group_rows, columns), NN)
        late_out[:, :, at] = rows.astype(bf16).reshape(sp_count, devices, columns)
        return 0

    lax.fori_loop(0, width // columns, choose, 0)
    late_in = Push(
        SP, sp_count, lambda peer: late_out.at[peer], late_blocks, sems[26:28], ring.core * sp_count
    )
    late_in.begin()

    def late_hand(which):
        return ring.copy(
            late_blocks.at[which],
            late_blocks.at[which],
            sems[28].at[lax.rem(which, sp_count)],
            sems[29].at[lax.rem(which, sp_count)],
            ring.twin,
        )

    def late_handed(k):
        return late_hand((1 - ring.core) * sp_count + k)

    late_pair = ring.copy(
        late_partial.at[pl.ds((1 - ring.core) * sp_count, sp_count)],
        late_other,
        sems[30].at[0],
        sems[30].at[1],
        ring.twin,
    )
    for copy in weight_copies:
        copy.wait()

    shared_half(0)
    for step in range(ring.steps):
        routed_in.advance(step)
        if step == 0:
            shared_half(1)
        elif step == 1:
            shared_pairs.give(*range(ring.chips))
            routed_in.hand_own().wait_recv()
            routed_in.handed(0, 1)
            routed_on(0, -1, 1)
        elif step == 2:
            routed_sum.give(0, -1, 1)
        elif step % 2 == 1:
            distance = (step + 1) // 2
            routed_in.handed(step - 1, step)
            routed_on(-distance, distance)
        else:
            routed_sum.give(-(step // 2), step // 2)
    ring.start(late_hand(ring.core * sp_count + here))
    for k in range(1, sp_count):
        late_in.copies[k - 1].wait_recv()
        ring.start(late_hand(ring.core * sp_count + lax.rem(here + sp_count - k, sp_count)))
    routed_in.handed(ring.steps - 1)
    routed_on(ring.far)
    routed_sum.give(ring.far)
    routed_sum.advance(0)
    routed_sum.advance(1)
    for k in range(sp_count):
        late_handed(k).wait_recv()

    def late_on(k, _):
        expert_on(late_blocks, late_partial, [k * sp_count], sp_count, pl.ds(0, devices), k)
        return 0

    lax.fori_loop(0, local_experts, late_on, 0)
    routed_sum.advance(2)
    ring.start(late_pair)
    routed_sum.advance(3)
    late_pair.wait_recv()
    late_back[...] = (
        (
            late_partial[pl.ds(ring.core * sp_count, sp_count)].astype(f32)
            + late_other[...].astype(f32)
        )
        .reshape(late_back.shape)
        .astype(bf16)
    )
    at_home = ring.core * sp_count + here
    late_home = []
    for k in range(sp_count):
        for same in (0, 1):
            core = ring.core if same == 0 else 1 - ring.core
            peer = lax.rem(here + k, sp_count)
            if k == 0 and same == 0:
                late_returned[at_home] = late_back[here, core]
                continue
            copy = pltpu.make_async_remote_copy(
                src_ref=late_back.at[peer, core],
                dst_ref=late_returned.at[at_home],
                send_sem=sems[31].at[same, k],
                recv_sem=sems[32].at[same, k],
                device_id={SP: peer, TP: ring.chip * 2 + core},
            )
            ring.start(copy)
            late_home.append(copy)
    for step in range(4, ring.steps):
        routed_sum.advance(step)
    summed = jnp.concatenate([routed_sum.own_half(which).astype(bf16) for which in (0, 1)], axis=0)
    unpacked[...] = (
        (
            raw_dot(packing[0], summed[:, :side], TN) + raw_dot(packing[1], summed[:, side:], TN)
        )
        .astype(bf16)
        .reshape(unpacked.shape)
    )
    back = Push(SP, sp_count, lambda peer: unpacked.at[peer], returned, sems[22:24])
    back.begin()
    own_slots = [2 * k + ring.core for k in range(ring.chips)]
    own_infos = jnp.concatenate([shared_blocks[k, :, pl.ds(width, LANES)] for k in own_slots], axis=0)
    column, lane = iota((late_rows, LANES), 0), iota((late_rows, LANES), 1)
    wanted = column % LANES // ring.chips * 2 + column // LANES
    shape = (own_rows, late_rows)
    by_row = iota(shape, 0) // block_rows == iota(shape, 1) % ring.chips
    late_weights = [
        jnp.where(
            by_row,
            raw_dot(own_infos, jnp.where(lane == 32 * k + wanted, 1.0, 0.0).astype(bf16), NT),
            0.0,
        ).astype(bf16)
        for k in (1, 2)
    ]
    for k in range(ring.chips):
        shared_pairs.meet(k)
    for copy in late_home:
        copy.wait_recv()

    def add_late(k, _):
        at = pl.ds(pl.multiple_of(k * columns, columns), columns)
        rows = late_returned[:, :, at].reshape(late_rows, columns)
        own = jnp.concatenate([shared_partial[slot, :, at] for slot in own_slots], axis=0).astype(f32)
        total = (
            own
            + shared_other[:, :, at].reshape(own_rows, columns).astype(f32)
            + raw_dot(late_weights[0], rows, NN)
            + raw_dot(late_weights[1], rows, NN)
        )
        shared_chip[:, :, at] = total.astype(bf16).reshape(ring.chips, block_rows, columns)
        return 0

    lax.fori_loop(0, width // columns, add_late, 0)
    for step in range(ring.steps):
        shared_sum.advance(step)
    half = residual.shape[0] // 2
    for which in (0, 1):
        piece = slice(which * half, (which + 1) * half)
        residual[piece, :] = residual[piece, :] + shared_sum.own_half(which)
    back.arrive()
    rows = returned[...].reshape(LANES, side)
    routed = jnp.concatenate([exact_right_dot(weighting * c, rows, NN) for c in columns_of], axis=1)
    o_ref[...] = (residual[...] + routed).astype(bf16)
    for copy in ring.sent:
        copy.wait_send()
    dispatch.leave()
    back.leave()
    states.leave()
    late_in.leave()


def layer(arrays, weights, devices, sp_count, capacity, room, number, name):
    tokens = arrays[1].shape[0]
    rows, width = arrays[8].shape
    hidden = weights[3].shape[1]
    local_experts = weights[0].shape[0]
    packed_rows = sp_count * local_experts * capacity
    block_count = tokens // BLOCK
    chips = devices // 2
    steps = chips - 1
    dma = pltpu.SemaphoreType.DMA
    anywhere = pl.BlockSpec(memory_space=pl.ANY)
    buffer = lambda *shape: pltpu.VMEM(shape, bf16)
    hops = steps * PARTS
    gather_sems = [dma((2, hops)), dma((2, hops)), dma((2, hops + 1)), dma((2, hops + 1))]
    sum_sems = [dma((chips,)), dma((chips,)), dma((2, hops)), dma((2, hops))]
    push_sems = [dma((sp_count,)), dma((sp_count,))]
    return pl.pallas_call(
        functools.partial(layer_kernel, devices=devices, sp_count=sp_count),
        name=name,
        out_shape=jax.ShapeDtypeStruct((rows, width), bf16),
        in_specs=[VMEM] * 12 + [anywhere] * 6,
        out_specs=VMEM,
        scratch_shapes=[
            pltpu.VMEM((tokens, LANES), f32),
            pltpu.VMEM((tokens, 2 * LANES), f32),
            pltpu.VMEM((2, block_count, BLOCK, LANES), f32),
            pltpu.VMEM((2, block_count, BLOCK, LANES), f32),
            pltpu.VMEM((2, block_count, LANES, LANES), f32),
            pltpu.VMEM((2, block_count, BLOCK, LANES), f32),
            buffer(2, 2 * BLOCK, LANES),
            buffer(sp_count, 2 * BLOCK, LANES),
            buffer(chips, 2, rows, LANES),
            pltpu.VMEM((rows, width), f32),
            buffer(rows, width + LANES),
            buffer(sp_count, room, width // 2),
            buffer(sp_count, room, width // 2),
            buffer(packed_rows, width),
            buffer(sp_count, room, width // 2),
            buffer(sp_count, room, width // 2),
            buffer(devices, rows, width + LANES),
            buffer(devices, packed_rows, width),
            buffer(sp_count, devices, width),
            buffer(local_experts * sp_count, devices, width),
            buffer(local_experts * sp_count, devices, width),
            buffer(sp_count, devices, width),
            buffer(sp_count, 2, chips, width),
            buffer(2 * sp_count, chips, width),
            buffer(LANES, width),
            buffer(chips, rows, LANES),
            buffer(chips, rows, width),
            buffer(chips, rows, width),
            buffer(devices, rows, width),
            buffer(devices, packed_rows, width),
            buffer(chips, rows, width),
            buffer(chips, packed_rows, width),
            buffer(2, steps, rows // 2, width),
            buffer(2, steps, rows // 2, width),
            buffer(2, steps, packed_rows // 2, width),
            buffer(local_experts + 1, width, hidden),
            buffer(local_experts + 1, width, hidden),
            buffer(local_experts + 1, hidden, width),
            dma((6,)),
        ]
        + sum_sems
        + gather_sems
        + push_sems
        + gather_sems
        + sum_sems
        + sum_sems
        + push_sems
        + push_sems
        + push_sems
        + push_sems
        + [dma((2,)), dma((2, sp_count)), dma((2, sp_count)), dma((4,))],
        compiler_params=pltpu.CompilerParams(
            collective_id=number, has_side_effects=True, vmem_limit_bytes=62 * 1024 * 1024
        ),
    )(*arrays, *weights)


def body(
    layer_input,
    receptance,
    keys,
    values,
    erase_preact,
    decay_preact,
    decay_spike,
    head_norm_gain,
    output_weight,
    expert_norm_gain,
    routes,
    routing_weight,
    expert_gate_weight,
    expert_up_weight,
    expert_down_weight,
    shared_gate_weight,
    shared_up_weight,
    shared_down_weight,
):
    sp_count, tp_count = lax.axis_size(SP), lax.axis_size(TP)
    return layer(
        (
            receptance,
            keys,
            values,
            erase_preact,
            decay_preact,
            decay_spike.T,
            head_norm_gain.reshape(1, -1),
            output_weight,
            layer_input,
            expert_norm_gain.reshape(-1, LANES),
            routes.T,
            routing_weight.T,
        ),
        (
            expert_gate_weight,
            expert_up_weight,
            expert_down_weight,
            shared_gate_weight,
            shared_up_weight,
            shared_down_weight,
        ),
        tp_count,
        sp_count,
        2,
        8,
        0,
        "layer",
    )


def solution(mesh):
    both = (SP, TP)
    in_specs = (
        P(both, None),
        P(SP, TP),
        P(SP, TP),
        P(SP, TP),
        P(SP, TP),
        P(SP, TP),
        P(SP, TP),
        P(TP),
        P(TP, None),
        P(),
        P(both, None),
        P(both, None),
        P(SP, None, TP),
        P(SP, None, TP),
        P(SP, TP, None),
        P(None, TP),
        P(None, TP),
        P(TP, None),
    )
    return jax.shard_map(
        body, mesh=mesh, in_specs=in_specs, out_specs=P(both, None), check_vma=False
    )
```

```python
import functools

import jax
import jax.numpy as jnp
from jax import lax
from jax.experimental import pallas as pl
from jax.experimental.pallas import tpu as pltpu
from jax.sharding import PartitionSpec as P

SP = "sp"
TP = "tp"
BLOCK = 64
LANES = 128
GN_EPS = 0.00064
RMS_EPS = 1e-06
f32 = jnp.float32
bf16 = jnp.bfloat16
VMEM = pl.BlockSpec(memory_space=pltpu.VMEM)
NN = (((1,), (0,)), ((), ()))
NT = (((1,), (1,)), ((), ()))
TN = (((0,), (0,)), ((), ()))


def iota(shape, dim):
    return lax.broadcasted_iota(jnp.int32, shape, dim)


def halves(array):
    high = array.astype(bf16)
    return high, (array - high.astype(f32)).astype(bf16)


def raw_dot(left, right, dims):
    return lax.dot_general(left, right, dims, preferred_element_type=f32)


def head_mask(count, dtype):
    first = (iota((count, LANES), 1) < BLOCK).astype(f32)
    return first.astype(dtype), (1.0 - first).astype(dtype)


def both_heads(rows):
    first, second = head_mask(rows.shape[0], rows.dtype)
    return jnp.concatenate([rows * first, rows * second], axis=0)


def fine_dot(left, right, dims, spread=False):
    left_high, left_low = halves(left)
    right_high, right_low = halves(right)
    if spread:
        right_high, right_low = both_heads(right_high), both_heads(right_low)
    if dims == TN:
        return raw_dot(
            jnp.concatenate([left_high, left_high, left_low], axis=0),
            jnp.concatenate([right_high, right_low, right_high], axis=0),
            TN,
        )
    count = left.shape[0]
    both = raw_dot(jnp.concatenate([left_high, left_low], axis=0), right_high, dims)
    return both[:count] + both[count:] + raw_dot(left_high, right_low, dims)


def exact_right_dot(left, right, dims):
    left_high, left_low = halves(left)
    count = left.shape[0]
    both = raw_dot(jnp.concatenate([left_high, left_low], axis=0), right, dims)
    return both[:count] + both[count:]


def head_sum(rows):
    ones = (iota((LANES, LANES), 0) // BLOCK == iota((LANES, LANES), 1) // BLOCK).astype(bf16)
    return exact_right_dot(rows, ones, NN)


def block_sums(log_decay):
    high, middle, low = three_parts(log_decay)
    count = log_decay.shape[0]
    ones = (iota((count, count), 0) >= iota((count, count), 1)).astype(bf16)
    width = log_decay.shape[1]
    sums = raw_dot(ones, jnp.concatenate([high, middle, low], axis=1), NN)
    return sums[:, :width] + sums[:, width : 2 * width] + sums[:, 2 * width :]


def inverses(stricts):
    row, lane = iota((BLOCK, LANES), 0), iota((BLOCK, LANES), 1) % BLOCK

    def within(size):
        return row // size == lane // size

    def products(lefts, rights):
        return [fine_dot(left, right, NN, spread=True) for left, right in zip(lefts, rights)]

    smalls = [jnp.where(within(8), strict, 0.0) for strict in stricts]
    starts = [jnp.where(row == lane, 1.0, 0.0) - small for small in smalls]
    squares = products(smalls, smalls)
    boths = products([jnp.concatenate(p, axis=0) for p in zip(starts, squares)], squares)
    results = [start + both[:BLOCK] for start, both in zip(starts, boths)]
    more = products(results, [both[BLOCK:] for both in boths])
    results = [r + m for r, m in zip(results, more)]
    for size in (8, 16, 32):
        keep = within(2 * size) & ~within(size)
        edges = products(results, [jnp.where(keep, strict, 0.0) for strict in stricts])
        more = products(edges, results)
        results = [r - m for r, m in zip(results, more)]
    return results


def block_terms(chains):
    row, lane = iota((BLOCK, LANES), 0), iota((BLOCK, LANES), 1) % BLOCK
    scaled, pairs = [], []
    for unit, beta, key_rows, _, read, left_unit, left_read, right, _, _ in chains:
        scaled.append((unit * left_unit, read * left_read, beta * right, key_rows * right))
    for unit_mid, read_mid, beta_mid, key_mid in scaled:
        left_high, left_low = halves(jnp.concatenate([unit_mid, read_mid], axis=0))
        right_high, right_low = [
            jnp.concatenate([both_heads(b), both_heads(k)], axis=0)
            for b, k in zip(halves(beta_mid), halves(key_mid))
        ]
        both = raw_dot(jnp.concatenate([left_high, left_low], axis=0), right_high, NT)
        pairs.append(both[: 2 * BLOCK] + both[2 * BLOCK :] + raw_dot(left_high, right_low, NT))
    erase_betas, keyeds, read_betas = [], [], []
    for pair, chain in zip(pairs, chains):
        strict = row > lane if chain[-1] else row < lane
        upto = row >= lane if chain[-1] else row <= lane
        erase_betas.append(jnp.where(strict, pair[:BLOCK, :LANES], 0.0))
        erase_key = jnp.where(strict, pair[:BLOCK, LANES:], 0.0)
        read_betas.append(jnp.where(upto, pair[BLOCK:, :LANES], 0.0))
        read_key = jnp.where(upto, pair[BLOCK:, LANES:], 0.0)
        keyeds.append(
            exact_right_dot(jnp.concatenate([erase_key, read_key], axis=0), chain[3], NN)
        )
    solvers = inverses(erase_betas)
    solved = []
    for solver, (unit_mid, _, _, _), keyed, chain in zip(solvers, scaled, keyeds, chains):
        solver_high, solver_low = halves(solver)
        right_high, right_low = [
            jnp.concatenate([both_heads(u), both_heads(k)], axis=1)
            for u, k in zip(halves(unit_mid * chain[8]), halves(-keyed[:BLOCK]))
        ]
        both = raw_dot(jnp.concatenate([solver_high, solver_low], axis=0), right_high, NN)
        solved.append(both[:BLOCK] + both[BLOCK:] + raw_dot(solver_high, right_low, NN))
    terms = []
    for found, read_beta, keyed, scale, chain in zip(solved, read_betas, keyeds, scaled, chains):
        spread_parts = [
            jnp.concatenate([both_heads(p[:, :LANES]), both_heads(p[:, LANES:])], axis=1)
            for p in halves(found)
        ]
        read_high, read_low = halves(read_beta)
        both = raw_dot(jnp.concatenate([read_high, read_low], axis=0), spread_parts[0], NN)
        applied = both[:BLOCK] + both[BLOCK:] + raw_dot(read_high, spread_parts[1], NN)
        readout = scale[1] * chain[8] - applied[:, :LANES]
        local = applied[:, LANES:] + keyed[BLOCK:]
        terms.append((found, scale[2] * chain[8], scale[3] * chain[8], readout, local))
    return terms


def three_parts(array):
    high = array.astype(bf16)
    rest = array - high.astype(f32)
    middle = rest.astype(bf16)
    return high, middle, (rest - middle.astype(f32)).astype(bf16)


def to_columns(rows, pick):
    chosen = [(pick == k).astype(bf16) for k in range(2)]
    parts = three_parts(rows)
    return raw_dot(
        jnp.concatenate(parts, axis=0), jnp.concatenate([jnp.concatenate(chosen, axis=0)] * 3, axis=0), TN
    )


def mixer_stage(
    read_ref,
    key_ref,
    value_ref,
    erase_ref,
    decay_ref,
    spike_ref,
    local_ref,
    readout_ref,
    prefix_ref,
    start_ref,
    move_ref,
    carry_ref,
    whole_ref,
    together,
):
    tokens = key_ref.shape[0]
    block_count = tokens // BLOCK
    same_head = iota((LANES, LANES), 0) // BLOCK == iota((LANES, LANES), 1) // BLOCK
    diagonal = iota((LANES, LANES), 0) == iota((LANES, LANES), 1)

    def some_blocks(index):
        blocks = [index * together + k for k in range(together)]
        span = together * BLOCK
        spikes = to_columns(
            spike_ref[:, pl.ds(pl.multiple_of(index * span, span), span)],
            iota((1, LANES), 1) // BLOCK,
        )
        chains, totals, values = [], [], []
        places = [pl.ds(pl.multiple_of(block * BLOCK, BLOCK), BLOCK) for block in blocks]
        for k, at in enumerate(places):
            key_rows = key_ref[at, :].astype(f32)
            read = read_ref[at, :].astype(f32)
            value = value_ref[at, :]
            unit = key_rows * lax.rsqrt(head_sum(key_rows * key_rows) + 1e-06)
            beta = unit * jax.nn.sigmoid(erase_ref[at, :].astype(f32))
            decay_in = decay_ref[at, :].astype(f32)
            spike = spikes[k * BLOCK : (k + 1) * BLOCK]
            log_decay = -jnp.exp(-jax.nn.softplus(-decay_in) - 0.5) + spike
            upto = block_sums(log_decay)
            total = upto[BLOCK - 1 :, :]
            middle = 0.5 * total
            ahead = upto - log_decay
            before, after = jnp.exp(ahead - middle), jnp.exp(upto - middle)
            until, since = jnp.exp(middle - upto), jnp.exp(middle - ahead)
            edge = jnp.exp(middle)
            shared = (unit, beta, key_rows, both_heads(value), read)
            chains.append(shared + (before, after, until, edge, True))
            chains.append(shared + (until, since, before, edge, False))
            totals.append(total)
            values.append(value)
        terms = block_terms(chains)
        for k, at in enumerate(places):
            local_ref[at, :] = terms[2 * k][4] + terms[2 * k + 1][4]
        for k, (solved, beta_end, key_end, readout, _) in enumerate(terms):
            way, at, value = k % 2, places[k // 2], values[k // 2]
            readout_ref[at, way * LANES : (way + 1) * LANES] = readout
            moved = fine_dot(solved, beta_end, TN)
            key_high, key_low = halves(key_end)
            keyed = raw_dot(
                jnp.concatenate([value, value], axis=0),
                jnp.concatenate([key_high, key_low], axis=0),
                TN,
            )
            move_ref[way, blocks[k // 2]] = jnp.where(
                same_head, jnp.where(diagonal, jnp.exp(totals[k // 2]), 0.0) - moved[:LANES], 0.0
            )
            carry = jnp.where(same_head, moved[LANES:] + keyed, 0.0)
            carry_ref[way, blocks[k // 2]] = carry[:BLOCK] + carry[BLOCK:]

    def step(index, _):
        some_blocks(index)
        return 0

    lax.fori_loop(0, block_count // together, step, 0)
    identity = jnp.where(iota((BLOCK, LANES), 0) == iota((BLOCK, LANES), 1) % BLOCK, 1.0, 0.0)
    running = [jnp.concatenate([identity, jnp.zeros_like(identity)], axis=0)] * 2
    for k in range(block_count):
        for way in range(2):
            block = k if way == 0 else block_count - 1 - k
            now = running[way]
            prefix_ref[way, block] = now[:BLOCK]
            start_ref[way, block] = now[BLOCK:]
            after = fine_dot(now, move_ref[way, block], NN)
            running[way] = jnp.concatenate(
                [after[:BLOCK], after[BLOCK:] + carry_ref[way, block]], axis=0
            )
    for way in range(2):
        whole_ref[way] = running[way].astype(bf16)


class Ring:
    def __init__(self, axis, chips):
        self.axis, self.chips = axis, chips
        self.me = lax.axis_index(axis)
        self.chip, self.core = self.me // 2, lax.rem(self.me, 2)
        self.steps = chips - 1
        self.far = chips // 2
        self.next = (self.slot(1, self.core), self.slot(-1, self.core))
        self.twin = self.chip * 2 + 1 - self.core
        self.sent = []

    def chip_at(self, distance):
        return lax.rem(self.chip + distance + self.chips, self.chips)

    def slot(self, distance, which):
        return self.chip_at(distance) * 2 + which

    def copy(self, source, target, send, recv, peer):
        return pltpu.make_async_remote_copy(
            src_ref=source, dst_ref=target, send_sem=send, recv_sem=recv, device_id={self.axis: peer}
        )

    def start(self, copy):
        copy.start()
        self.sent.append(copy)

    def half_of(self, way, step):
        return step % 2 if way == 0 else 1 - step % 2


PARTS = 2


def column_parts(width):
    side = width // LANES // PARTS * LANES
    return [pl.ds(0, side), pl.ds(side, width - side)]


class Gather:
    def __init__(self, ring, own, blocks, sems):
        self.ring, self.own, self.blocks = ring, own, blocks
        self.send, self.recv, self.pass_send, self.pass_recv = sems
        self.half = own.shape[0] // 2
        self.columns = column_parts(own.shape[1])

    def piece(self, way, step):
        return pl.ds(self.ring.half_of(way, step) * self.half, self.half)

    def hop(self, way, step, part):
        ring, piece, columns = self.ring, self.piece(way, step), self.columns[part]
        at = ring.slot((step // 2) * (-1 if way == 0 else 1), ring.core)
        source = self.own.at[piece, columns] if step < 2 else self.blocks.at[at, piece, columns]
        return ring.copy(
            source,
            self.blocks.at[at, piece, columns],
            self.send.at[way, step * PARTS + part],
            self.recv.at[way, step * PARTS + part],
            ring.next[way],
        )

    def hand(self, way, step, part):
        ring, piece, columns = self.ring, self.piece(way, step), self.columns[part]
        at = ring.slot((step // 2 + 1) * (-1 if way == 0 else 1), ring.core)
        return ring.copy(
            self.blocks.at[at, piece, columns],
            self.blocks.at[at, piece, columns],
            self.pass_send.at[way, step * PARTS + part],
            self.pass_recv.at[way, step * PARTS + part],
            ring.twin,
        )

    def hand_own(self):
        ring = self.ring
        return ring.copy(
            self.own,
            self.blocks.at[ring.me],
            self.pass_send.at[0, ring.steps * PARTS],
            self.pass_recv.at[0, ring.steps * PARTS],
            ring.twin,
        )

    def begin(self):
        for step in (0, 1):
            for part in range(PARTS):
                for way in (0, 1):
                    self.ring.start(self.hop(way, step, part))
        self.ring.start(self.hand_own())
        self.blocks[self.ring.me] = self.own[...]

    def advance(self, step):
        for part in range(PARTS):
            for way in (0, 1):
                self.hop(way, step, part).wait_recv()
                if step + 2 < self.ring.steps:
                    self.ring.start(self.hop(way, step + 2, part))
                self.ring.start(self.hand(way, step, part))

    def handed(self, *steps):
        for step in steps:
            for part in range(PARTS):
                for way in (0, 1):
                    self.hand(way, step, part).wait_recv()


class Sum:
    def __init__(self, ring, partial, other, inbox, sems):
        self.ring, self.partial, self.other, self.inbox = ring, partial, other, inbox
        self.pair_send, self.pair_recv, self.send_sem, self.recv_sem = sems
        self.half = partial.shape[1] // 2
        self.columns = column_parts(partial.shape[2])
        self.met = set()

    def pair(self, distance):
        ring = self.ring
        index = ring.chip_at(distance)
        return ring.copy(
            self.partial.at[ring.slot(distance, 1 - ring.core)],
            self.other.at[index],
            self.pair_send.at[index],
            self.pair_recv.at[index],
            ring.twin,
        )

    def give(self, *distances):
        for distance in distances:
            self.ring.start(self.pair(distance))

    def block(self, distance):
        ring = self.ring
        return ring.chip_at(distance) if self.other is None else ring.slot(distance, ring.core)

    def meet(self, distance):
        key = distance % self.ring.chips
        if self.other is not None and key not in self.met:
            self.met.add(key)
            self.pair(distance).wait_recv()

    def place(self, way, step):
        ring = self.ring
        distance = (ring.far - (step + 1) // 2) * (1 if way == 0 else -1)
        return distance, pl.ds(ring.half_of(way, step) * self.half, self.half)

    def hop(self, way, step, part):
        ring = self.ring
        distance, piece = self.place(way, step)
        columns = self.columns[part]
        return ring.copy(
            self.partial.at[self.block(distance), piece, columns],
            self.inbox.at[way, step, :, columns],
            self.send_sem.at[way, step * PARTS + part],
            self.recv_sem.at[way, step * PARTS + part],
            ring.next[way],
        )

    def both_cores(self, distance, piece, columns):
        rows = self.partial[self.block(distance), piece, columns].astype(f32)
        if self.other is None:
            return rows
        return rows + self.other[self.ring.chip_at(distance), piece, columns].astype(f32)

    def advance(self, step):
        ring = self.ring
        for part, columns in enumerate(self.columns):
            for way in (0, 1):
                distance, piece = self.place(way, step)
                self.meet(distance)
                if step >= 2 or self.other is not None:
                    total = self.both_cores(distance, piece, columns)
                    if step >= 2:
                        self.hop(way, step - 2, part).wait_recv()
                        total = total + self.inbox[way, step - 2, :, columns].astype(f32)
                    self.partial[self.block(distance), piece, columns] = total.astype(bf16)
            for way in (0, 1):
                ring.start(self.hop(way, step, part))

    def own_half(self, which):
        ring = self.ring
        self.meet(0)
        totals = []
        for part, columns in enumerate(self.columns):
            total = self.both_cores(0, pl.ds(which * self.half, self.half), columns)
            for way in (0, 1):
                even = ring.half_of(way, ring.steps - 2) == which
                step = ring.steps - 2 if even else ring.steps - 1
                self.hop(way, step, part).wait_recv()
                total = total + self.inbox[way, step, :, columns].astype(f32)
            totals.append(total)
        return jnp.concatenate(totals, axis=1)


class Push:
    def __init__(self, axis, count, source, target, sems, base=0):
        self.axis, self.source, self.target = axis, source, target
        self.send, self.recv = sems
        self.count, self.base = count, base
        self.me = lax.axis_index(axis)
        self.copies = []

    def begin(self):
        for k in range(1, self.count):
            peer = lax.rem(self.me + k, self.count)
            copy = pltpu.make_async_remote_copy(
                src_ref=self.source(peer),
                dst_ref=self.target.at[self.base + self.me],
                send_sem=self.send.at[k],
                recv_sem=self.recv.at[k],
                device_id={self.axis: peer},
            )
            copy.start()
            self.copies.append(copy)
        self.target[self.base + self.me] = self.source(self.me)[...]

    def arrive(self):
        for copy in self.copies:
            copy.wait_recv()

    def leave(self):
        for copy in self.copies:
            copy.wait_send()


def meet_peers(axis, count, others):
    me = lax.axis_index(axis)
    barrier = pltpu.get_barrier_semaphore()
    for k in range(1, count):
        pl.semaphore_signal(barrier, inc=1, device_id={axis: lax.rem(me + k, count)})
    for peer in others:
        pl.semaphore_signal(barrier, inc=1, device_id=peer)
    return barrier, count - 1 + len(others)


def finish_blocks(
    place, await_state, got_ref, local_ref, readout_ref, prefix_ref, start_ref, gain_ref, mixed_ref
):
    last = got_ref.shape[0] - 1
    blocks = range(prefix_ref.shape[1])

    def after(j, entry):
        await_state(j)
        moved = exact_right_dot(entry, both_heads(got_ref[j, :BLOCK, :]), NN)
        return moved + got_ref[j, BLOCK:, :].astype(f32)

    blank = jnp.zeros((BLOCK, LANES), f32)
    entry = [
        lax.fori_loop(0, place, after, blank),
        lax.fori_loop(0, last - place, lambda k, e: after(last - k, e), blank),
    ]
    gain = gain_ref[...].astype(f32)
    states = []
    for way in range(2):
        high, low = halves(entry[way])
        stacked = jnp.concatenate([high, low], axis=0)
        prefixes = [[both_heads(p) for p in halves(prefix_ref[way, b])] for b in blocks]
        boths = [raw_dot(stacked, p[0], NN) for p in prefixes]
        rests = [raw_dot(high, p[1], NN) for p in prefixes]
        states.append(
            [
                [both_heads(p) for p in halves(x[:BLOCK] + x[BLOCK:] + y + start_ref[way, b])]
                for x, y, b in zip(boths, rests, blocks)
            ]
        )
    places = [slice(b * BLOCK, (b + 1) * BLOCK) for b in blocks]
    mixes = []
    for b in blocks:
        state_high, state_low = [
            jnp.concatenate([states[0][b][k], states[1][b][k]], axis=1) for k in (0, 1)
        ]
        read_high, read_low = halves(readout_ref[places[b], :])
        both = raw_dot(jnp.concatenate([read_high, read_low], axis=0), state_high, NT)
        mixes.append(
            local_ref[places[b], :] + both[:BLOCK] + both[BLOCK:] + raw_dot(read_high, state_low, NT)
        )
    centers = [mix - head_sum(mix) * (1.0 / BLOCK) for mix in mixes]
    spreads = [head_sum(center * center) * (1.0 / BLOCK) for center in centers]
    for b in blocks:
        rows = (centers[b] * lax.rsqrt(spreads[b] + GN_EPS) * gain).astype(bf16)
        mixed_ref[b] = rows.reshape(mixed_ref.shape[1:])


def routing(routes_ref, weights_ref):
    rows = routes_ref.shape[1]
    slot = iota((rows, LANES), 1)
    names, values = [], []
    for k in range(2):
        pick = jnp.full((1, LANES), k, jnp.int32)
        names.append(to_columns(routes_ref[...].astype(f32), pick))
        values.append(to_columns(weights_ref[...], pick))
    before = (iota((rows, rows), 0) > iota((rows, rows), 1)).astype(bf16)

    def filled(expert, rank):
        named = [jnp.where(name == expert.astype(f32), 1.0, 0.0) for name in names]
        either = named[0] + named[1]
        taken = raw_dot(before, either.astype(bf16), NN)
        here = jnp.where(taken == rank.astype(f32), 1.0, 0.0)
        return either * here, (named[0] * values[0] + named[1] * values[1]) * here

    placing, weighting = filled(slot // 8 * 2 + slot % 4 // 2, slot % 2)
    late, late_weight = filled(slot % 32, jnp.full_like(slot, 2))
    high, low = halves(late_weight)
    kind = slot // 32
    info = jnp.where(
        kind == 0,
        late,
        jnp.where(kind == 1, high.astype(f32), jnp.where(kind == 2, low.astype(f32), 0.0)),
    )
    per_expert = LANES // 8 * 2
    shape = (2 * per_expert, LANES)
    at = iota(shape, 1)
    target = at % 4 // 2 * per_expert + at // 8 * 2 + at % 2
    column = at % 8 // 4
    packing = [
        jnp.where((iota(shape, 0) == target) & (column == k), 1.0, 0.0).astype(bf16) for k in range(2)
    ]
    return placing, weighting, info, packing


def late_pick(core, peers, blocks):
    row, lane = iota((peers * blocks, LANES), 0), iota((peers * blocks, LANES), 1)
    return jnp.where(lane == row // blocks * 2 + core, 1.0, 0.0).astype(bf16)


def layer_kernel(
    read_ref,
    key_ref,
    value_ref,
    erase_ref,
    decay_ref,
    spike_ref,
    gain_ref,
    mix_weight_ref,
    input_ref,
    norm_gain_ref,
    routes_ref,
    route_weights_ref,
    expert_gate,
    expert_up,
    expert_down,
    shared_gate,
    shared_up,
    shared_down,
    o_ref,
    local_ref,
    readout_ref,
    prefix_ref,
    start_ref,
    move_ref,
    carry_ref,
    whole_ref,
    got_ref,
    mixed,
    residual,
    normed,
    outgoing,
    arrived,
    packed,
    unpacked,
    returned,
    shared_blocks,
    routed_blocks,
    late_out,
    late_blocks,
    late_partial,
    late_other,
    late_back,
    late_returned,
    mix_weight_other,
    mixed_other,
    shared_chip,
    mix_partial,
    shared_partial,
    routed_partial,
    shared_other,
    routed_other,
    mix_inbox,
    shared_inbox,
    routed_inbox,
    gate,
    up,
    down,
    weight_sem,
    *sems,
    devices,
    sp_count,
):
    ring = Ring(TP, devices // 2)
    local_experts = expert_gate.shape[0]
    width = input_ref.shape[1]
    used = packed.shape[0] // local_experts
    weight_copies = []
    for k, (pair, single, into) in enumerate(
        ((expert_gate, shared_gate, gate), (expert_up, shared_up, up), (expert_down, shared_down, down))
    ):
        weight_copies.append(
            pltpu.make_async_copy(pair, into.at[pl.ds(0, local_experts)], weight_sem.at[2 * k])
        )
        weight_copies.append(
            pltpu.make_async_copy(single, into.at[local_experts], weight_sem.at[2 * k + 1])
        )
    for copy in weight_copies:
        copy.start()
    barrier, expected = meet_peers(
        SP,
        sp_count,
        [{TP: ring.next[0]}, {TP: ring.next[1]}, {TP: ring.twin}]
        + [
            {SP: lax.rem(lax.axis_index(SP) + k, sp_count), TP: ring.twin} for k in range(1, sp_count)
        ],
    )

    placing, weighting, info, packing = routing(routes_ref, route_weights_ref)
    slot = iota(placing.shape, 1)
    columns_of = [(slot % 8 // 4 == k).astype(f32) for k in range(2)]
    side = width // 2
    mixer_stage(
        read_ref,
        key_ref,
        value_ref,
        erase_ref,
        decay_ref,
        spike_ref,
        local_ref,
        readout_ref,
        prefix_ref,
        start_ref,
        move_ref,
        carry_ref,
        whole_ref,
        8,
    )
    pl.semaphore_wait(barrier, expected)
    here = lax.axis_index(SP)
    states = Push(
        SP,
        sp_count,
        lambda peer: whole_ref.at[(here + sp_count - peer) // (sp_count + 1)],
        got_ref,
        sems[24:26],
    )
    states.begin()
    twin_weight = ring.copy(
        mix_weight_ref, mix_weight_other, sems[33].at[0], sems[33].at[1], ring.twin
    )
    ring.start(twin_weight)

    def await_state(j):
        k = lax.rem(here + sp_count - j, sp_count)
        pltpu.make_async_remote_copy(
            src_ref=whole_ref.at[0],
            dst_ref=got_ref.at[j],
            send_sem=sems[24].at[k],
            recv_sem=sems[25].at[k],
            device_id={SP: j},
        ).wait_recv()

    finish_blocks(
        here, await_state, got_ref, local_ref, readout_ref, prefix_ref, start_ref, gain_ref, mixed
    )
    twin_mixed = ring.copy(
        mixed.at[:, 1 - ring.core], mixed_other, sems[33].at[2], sems[33].at[3], ring.twin
    )
    ring.start(twin_mixed)
    columns = 512
    own_rows = mix_partial.shape[0] * mix_partial.shape[1]
    twin_weight.wait_recv()
    own_mixed = mixed[:, ring.core].reshape(own_rows, LANES)
    twin_mixed.wait_recv()
    heads = jnp.concatenate([own_mixed, mixed_other[...].reshape(own_rows, LANES)], axis=1)

    def project(k, _):
        at = pl.ds(pl.multiple_of(k * columns, columns), columns)
        weight = jnp.concatenate([mix_weight_ref[:, at], mix_weight_other[:, at]], axis=0)
        product = raw_dot(heads, weight, NN).astype(bf16)
        mix_partial[:, :, at] = product.reshape(mix_partial.shape[0], mix_partial.shape[1], columns)
        return 0

    lax.fori_loop(0, width // columns, project, 0)
    mix_sum = Sum(ring, mix_partial, None, mix_inbox, sems[0:4])
    for step in range(ring.steps):
        mix_sum.advance(step)
    gains = norm_gain_ref[...].astype(f32)
    norm_gain = jnp.concatenate([gains[k : k + 1] for k in range(gains.shape[0])], axis=1)
    half = residual.shape[0] // 2
    for which in (0, 1):
        piece = slice(which * half, (which + 1) * half)
        rows = input_ref[piece, :].astype(f32) + mix_sum.own_half(which)
        residual[piece, :] = rows
        scale = lax.rsqrt(jnp.mean(rows * rows, axis=-1, keepdims=True) + RMS_EPS)
        normed[piece, :width] = (rows * scale * norm_gain).astype(bf16)
        normed[piece, width:] = info[piece, :].astype(bf16)

    shared_in = Gather(ring, normed, shared_blocks, sems[4:8])
    outgoing[...] = (
        raw_dot(
            jnp.concatenate([(placing * c).astype(bf16) for c in columns_of], axis=0),
            jnp.concatenate([normed[:, :side], normed[:, side:width]], axis=0),
            TN,
        )
        .astype(bf16)
        .reshape(outgoing.shape)
    )
    shared_in.begin()
    dispatch = Push(SP, sp_count, lambda peer: outgoing.at[peer], arrived, sems[8:10])
    dispatch.begin()
    for step in range(ring.steps - 2):
        shared_in.advance(step)
    dispatch.arrive()
    arrivals = arrived[...].reshape(LANES, side)
    packed[...] = jnp.concatenate([raw_dot(p, arrivals, NN) for p in packing], axis=1).astype(bf16)
    routed_in = Gather(ring, packed, routed_blocks, sems[10:14])
    routed_in.begin()
    shared_in.advance(ring.steps - 2)
    shared_in.advance(ring.steps - 1)

    def expert_on(blocks, partial, firsts, count, at, which):
        rows = at.size
        x = jnp.concatenate(
            [
                blocks[pl.ds(first, count), at, pl.ds(0, width)].reshape(count * rows, width)
                for first in firsts
            ],
            axis=0,
        )
        gated = raw_dot(x, gate[which], NN)
        lifted = raw_dot(x, up[which], NN)
        inner = (gated / (1.0 + jnp.exp(-gated)) * lifted).astype(bf16)
        outer = raw_dot(inner, down[which], NN).astype(bf16)
        for k, first in enumerate(firsts):
            partial[pl.ds(first, count), at, :] = outer[
                k * count * rows : (k + 1) * count * rows
            ].reshape(count, rows, width)

    def routed_on(*distances):
        firsts = [ring.chip_at(distance) * 2 for distance in distances]

        def one(k, _):
            at = pl.ds(pl.multiple_of(k * used, 16), used)
            expert_on(routed_blocks, routed_partial, firsts, 2, at, k)
            return 0

        lax.fori_loop(0, local_experts, one, 0)

    def shared_half(which):
        count = devices // 2
        at = pl.ds(0, normed.shape[0])
        expert_on(shared_blocks, shared_partial, [which * count], count, at, local_experts)

    routed_sum = Sum(ring, routed_partial, routed_other, routed_inbox, sems[14:18])
    shared_pairs = Sum(ring, shared_partial, shared_other, None, sems[18:20] + (None, None))
    shared_sum = Sum(ring, shared_chip, None, shared_inbox, (None, None) + sems[20:22])
    shared_in.hand_own().wait_recv()
    shared_in.handed(*range(ring.steps))

    block_rows = normed.shape[0]
    group_rows, late_rows = devices * block_rows, sp_count * devices
    infos = shared_blocks[:, :, pl.ds(width, LANES)].reshape(group_rows, LANES)
    order = iota((late_rows, group_rows), 0) % devices
    of_block = (
        order % ring.chips * 2 + order // ring.chips == iota((late_rows, group_rows), 1) // block_rows
    )
    chosen = jnp.where(
        of_block, raw_dot(late_pick(ring.core, sp_count, devices), infos, NT), 0.0
    ).astype(bf16)

    def choose(k, _):
        at = pl.ds(pl.multiple_of(k * columns, columns), columns)
        rows = raw_dot(chosen, shared_blocks[:, :, at].reshape(group_rows, columns), NN)
        late_out[:, :, at] = rows.astype(bf16).reshape(sp_count, devices, columns)
        return 0

    lax.fori_loop(0, width // columns, choose, 0)
    late_in = Push(
        SP, sp_count, lambda peer: late_out.at[peer], late_blocks, sems[26:28], ring.core * sp_count
    )
    late_in.begin()

    def late_hand(which):
        return ring.copy(
            late_blocks.at[which],
            late_blocks.at[which],
            sems[28].at[lax.rem(which, sp_count)],
            sems[29].at[lax.rem(which, sp_count)],
            ring.twin,
        )

    def late_handed(k):
        return late_hand((1 - ring.core) * sp_count + k)

    late_pair = ring.copy(
        late_partial.at[pl.ds((1 - ring.core) * sp_count, sp_count)],
        late_other,
        sems[30].at[0],
        sems[30].at[1],
        ring.twin,
    )
    for copy in weight_copies:
        copy.wait()

    shared_half(0)
    for step in range(ring.steps):
        routed_in.advance(step)
        if step == 0:
            shared_half(1)
        elif step == 1:
            shared_pairs.give(*range(ring.chips))
            routed_in.hand_own().wait_recv()
            routed_in.handed(0, 1)
            routed_on(0, -1, 1)
        elif step == 2:
            routed_sum.give(0, -1, 1)
        elif step % 2 == 1:
            distance = (step + 1) // 2
            routed_in.handed(step - 1, step)
            routed_on(-distance, distance)
        else:
            routed_sum.give(-(step // 2), step // 2)
    ring.start(late_hand(ring.core * sp_count + here))
    for k in range(1, sp_count):
        late_in.copies[k - 1].wait_recv()
        ring.start(late_hand(ring.core * sp_count + lax.rem(here + sp_count - k, sp_count)))
    routed_in.handed(ring.steps - 1)
    routed_on(ring.far)
    routed_sum.give(ring.far)
    routed_sum.advance(0)
    routed_sum.advance(1)
    for k in range(sp_count):
        late_handed(k).wait_recv()

    def late_on(k, _):
        expert_on(late_blocks, late_partial, [k * sp_count], sp_count, pl.ds(0, devices), k)
        return 0

    lax.fori_loop(0, local_experts, late_on, 0)
    routed_sum.advance(2)
    ring.start(late_pair)
    routed_sum.advance(3)
    late_pair.wait_recv()
    late_back[...] = (
        (
            late_partial[pl.ds(ring.core * sp_count, sp_count)].astype(f32)
            + late_other[...].astype(f32)
        )
        .reshape(late_back.shape)
        .astype(bf16)
    )
    at_home = ring.core * sp_count + here
    late_home = []
    for k in range(sp_count):
        for same in (0, 1):
            core = ring.core if same == 0 else 1 - ring.core
            peer = lax.rem(here + k, sp_count)
            if k == 0 and same == 0:
                late_returned[at_home] = late_back[here, core]
                continue
            copy = pltpu.make_async_remote_copy(
                src_ref=late_back.at[peer, core],
                dst_ref=late_returned.at[at_home],
                send_sem=sems[31].at[same, k],
                recv_sem=sems[32].at[same, k],
                device_id={SP: peer, TP: ring.chip * 2 + core},
            )
            ring.start(copy)
            late_home.append(copy)
    for step in range(4, ring.steps):
        routed_sum.advance(step)
    summed = jnp.concatenate([routed_sum.own_half(which).astype(bf16) for which in (0, 1)], axis=0)
    unpacked[...] = (
        (
            raw_dot(packing[0], summed[:, :side], TN) + raw_dot(packing[1], summed[:, side:], TN)
        )
        .astype(bf16)
        .reshape(unpacked.shape)
    )
    back = Push(SP, sp_count, lambda peer: unpacked.at[peer], returned, sems[22:24])
    back.begin()
    own_slots = [2 * k + ring.core for k in range(ring.chips)]
    own_infos = jnp.concatenate([shared_blocks[k, :, pl.ds(width, LANES)] for k in own_slots], axis=0)
    column, lane = iota((late_rows, LANES), 0), iota((late_rows, LANES), 1)
    wanted = column % LANES // ring.chips * 2 + column // LANES
    shape = (own_rows, late_rows)
    by_row = iota(shape, 0) // block_rows == iota(shape, 1) % ring.chips
    late_weights = [
        jnp.where(
            by_row,
            raw_dot(own_infos, jnp.where(lane == 32 * k + wanted, 1.0, 0.0).astype(bf16), NT),
            0.0,
        ).astype(bf16)
        for k in (1, 2)
    ]
    for k in range(ring.chips):
        shared_pairs.meet(k)
    for copy in late_home:
        copy.wait_recv()

    def add_late(k, _):
        at = pl.ds(pl.multiple_of(k * columns, columns), columns)
        rows = late_returned[:, :, at].reshape(late_rows, columns)
        own = jnp.concatenate([shared_partial[slot, :, at] for slot in own_slots], axis=0).astype(f32)
        total = (
            own
            + shared_other[:, :, at].reshape(own_rows, columns).astype(f32)
            + raw_dot(late_weights[0], rows, NN)
            + raw_dot(late_weights[1], rows, NN)
        )
        shared_chip[:, :, at] = total.astype(bf16).reshape(ring.chips, block_rows, columns)
        return 0

    lax.fori_loop(0, width // columns, add_late, 0)
    for step in range(ring.steps):
        shared_sum.advance(step)
    half = residual.shape[0] // 2
    for which in (0, 1):
        piece = slice(which * half, (which + 1) * half)
        residual[piece, :] = residual[piece, :] + shared_sum.own_half(which)
    back.arrive()
    rows = returned[...].reshape(LANES, side)
    routed = jnp.concatenate([exact_right_dot(weighting * c, rows, NN) for c in columns_of], axis=1)
    o_ref[...] = (residual[...] + routed).astype(bf16)
    for copy in ring.sent:
        copy.wait_send()
    dispatch.leave()
    back.leave()
    states.leave()
    late_in.leave()


def layer(arrays, weights, devices, sp_count, capacity, room, number, name):
    tokens = arrays[1].shape[0]
    rows, width = arrays[8].shape
    hidden = weights[3].shape[1]
    local_experts = weights[0].shape[0]
    packed_rows = sp_count * local_experts * capacity
    block_count = tokens // BLOCK
    chips = devices // 2
    steps = chips - 1
    dma = pltpu.SemaphoreType.DMA
    anywhere = pl.BlockSpec(memory_space=pl.ANY)
    buffer = lambda *shape: pltpu.VMEM(shape, bf16)
    hops = steps * PARTS
    gather_sems = [dma((2, hops)), dma((2, hops)), dma((2, hops + 1)), dma((2, hops + 1))]
    sum_sems = [dma((chips,)), dma((chips,)), dma((2, hops)), dma((2, hops))]
    push_sems = [dma((sp_count,)), dma((sp_count,))]
    return pl.pallas_call(
        functools.partial(layer_kernel, devices=devices, sp_count=sp_count),
        name=name,
        out_shape=jax.ShapeDtypeStruct((rows, width), bf16),
        in_specs=[VMEM] * 12 + [anywhere] * 6,
        out_specs=VMEM,
        scratch_shapes=[
            pltpu.VMEM((tokens, LANES), f32),
            pltpu.VMEM((tokens, 2 * LANES), f32),
            pltpu.VMEM((2, block_count, BLOCK, LANES), f32),
            pltpu.VMEM((2, block_count, BLOCK, LANES), f32),
            pltpu.VMEM((2, block_count, LANES, LANES), f32),
            pltpu.VMEM((2, block_count, BLOCK, LANES), f32),
            buffer(2, 2 * BLOCK, LANES),
            buffer(sp_count, 2 * BLOCK, LANES),
            buffer(chips, 2, rows, LANES),
            pltpu.VMEM((rows, width), f32),
            buffer(rows, width + LANES),
            buffer(sp_count, room, width // 2),
            buffer(sp_count, room, width // 2),
            buffer(packed_rows, width),
            buffer(sp_count, room, width // 2),
            buffer(sp_count, room, width // 2),
            buffer(devices, rows, width + LANES),
            buffer(devices, packed_rows, width),
            buffer(sp_count, devices, width),
            buffer(local_experts * sp_count, devices, width),
            buffer(local_experts * sp_count, devices, width),
            buffer(sp_count, devices, width),
            buffer(sp_count, 2, chips, width),
            buffer(2 * sp_count, chips, width),
            buffer(LANES, width),
            buffer(chips, rows, LANES),
            buffer(chips, rows, width),
            buffer(chips, rows, width),
            buffer(devices, rows, width),
            buffer(devices, packed_rows, width),
            buffer(chips, rows, width),
            buffer(chips, packed_rows, width),
            buffer(2, steps, rows // 2, width),
            buffer(2, steps, rows // 2, width),
            buffer(2, steps, packed_rows // 2, width),
            buffer(local_experts + 1, width, hidden),
            buffer(local_experts + 1, width, hidden),
            buffer(local_experts + 1, hidden, width),
            dma((6,)),
        ]
        + sum_sems
        + gather_sems
        + push_sems
        + gather_sems
        + sum_sems
        + sum_sems
        + push_sems
        + push_sems
        + push_sems
        + push_sems
        + [dma((2,)), dma((2, sp_count)), dma((2, sp_count)), dma((4,))],
        compiler_params=pltpu.CompilerParams(
            collective_id=number, has_side_effects=True, vmem_limit_bytes=62 * 1024 * 1024
        ),
    )(*arrays, *weights)


def body(
    layer_input,
    receptance,
    keys,
    values,
    erase_preact,
    decay_preact,
    decay_spike,
    head_norm_gain,
    output_weight,
    expert_norm_gain,
    routes,
    routing_weight,
    expert_gate_weight,
    expert_up_weight,
    expert_down_weight,
    shared_gate_weight,
    shared_up_weight,
    shared_down_weight,
):
    sp_count, tp_count = lax.axis_size(SP), lax.axis_size(TP)
    return layer(
        (
            receptance,
            keys,
            values,
            erase_preact,
            decay_preact,
            decay_spike.T,
            head_norm_gain.reshape(1, -1),
            output_weight,
            layer_input,
            expert_norm_gain.reshape(-1, LANES),
            routes.T,
            routing_weight.T,
        ),
        (
            expert_gate_weight,
            expert_up_weight,
            expert_down_weight,
            shared_gate_weight,
            shared_up_weight,
            shared_down_weight,
        ),
        tp_count,
        sp_count,
        2,
        8,
        0,
        "layer",
    )


def solution(mesh):
    both = (SP, TP)
    in_specs = (
        P(both, None),
        P(SP, TP),
        P(SP, TP),
        P(SP, TP),
        P(SP, TP),
        P(SP, TP),
        P(SP, TP),
        P(TP),
        P(TP, None),
        P(),
        P(both, None),
        P(both, None),
        P(SP, None, TP),
        P(SP, None, TP),
        P(SP, TP, None),
        P(None, TP),
        P(None, TP),
        P(TP, None),
    )
    return jax.shard_map(
        body, mesh=mesh, in_specs=in_specs, out_specs=P(both, None), check_vma=False
    )
```
